32 devices in a mesh: sp: 16 (over z, y, core), tp: 2 (over x).
Axes of the slice: x: 2, y: 2, z: 4, core: 2. Of those that a mesh axis runs over, the one named last changes fastest.
Arguments:
- queries: bfloat16 [16384, 1024], P('sp', 'tp'), may hold values from -8 to 8
- keys: bfloat16 [16384, 256], P('sp', 'tp'), may hold values from -8 to 8
- values: bfloat16 [16384, 256], P('sp', 'tp'), may hold values from -18 to 18
- doc_ids: int32 [16384], P('sp'), may hold values from 0 to 3, never falling along the last dimension, each value on 1 to 8192 neighbouring positions
- sinks: float32 [16], P('tp'), may hold values from 0 to 4
- residual: bfloat16 [16384, 2048], P(('sp', 'tp')), may hold values from -12 to 12
- out_weight: bfloat16 [1024, 2048], P('tp'), may hold values from -0.1875 to 0.1875
- norm_gain: float32 [2048], replicated, may hold values from 0.1 to 1.9
- w_gate: bfloat16 [2048, 5632], P('sp', 'tp'), may hold values from -0.125 to 0.125
- w_value: bfloat16 [2048, 5632], P('sp', 'tp'), may hold values from -0.125 to 0.125
- conv_gate: float32 [3, 5632], P(None, 'tp'), may hold values from -3.5 to 3.5
- conv_value: float32 [3, 5632], P(None, 'tp'), may hold values from -3.5 to 3.5
- w_down: bfloat16 [5632, 2048], P('tp', 'sp'), may hold values from -0.078125 to 0.078125
Outputs:
- layer_out: bfloat16 [16384, 2048], P(('sp', 'tp'))
The draws below stay inside these ranges and needn't reach their ends.
All inputs are finite; a program needn't handle non-finite values.
Results may differ from the reference program's by a relative error of at most 0.012.
Values may be sent and summed in bfloat16 or wider, within the bound.
A program may use at most 128 MiB of HBM per device.

```python
import math
import jax
import jax.numpy as jnp
import numpy as np
from jax import lax

D = 2048
HEAD_DIM = 64
A_HEADS = 16
FF = 5632
WINDOW = 128
TOK_SP = 1024
TOKENS = 16384
A_Q = 1024
KV_W = 256
DOCS = 4
N_SP = 16


def draw_keys(key, part):
    base = jnp.clip(jax.random.normal(jax.random.fold_in(key, 1), (TOKENS, KV_W), jnp.float32), -8.0, 8.0)
    return base.astype(jnp.bfloat16)


def draw_queries(key, part):
    base = jnp.clip(jax.random.normal(jax.random.fold_in(key, 2), (TOKENS, A_Q), jnp.float32), -8.0, 8.0)
    return base.astype(jnp.bfloat16)


def draw_residual(key, part):
    base = jax.random.normal(jax.random.fold_in(key, 3), (TOKENS, D), jnp.float32)
    spread = jax.random.uniform(jax.random.fold_in(key, 4), (TOKENS, 1), jnp.float32, math.log(1.0 / 3.0), math.log(3.0))
    base = base * jnp.exp(spread)
    return jnp.clip(base, -12.0, 12.0).astype(jnp.bfloat16)


def shard_levels(key, shape, shards, least, top_value):
    gain, own = 1.0, jax.random.fold_in(key, 6)
    for dim, shards_of in shards:
        heights = jnp.exp(jax.random.uniform(jax.random.fold_in(own, dim), (shards_of,), jnp.float32, least / len(shards), top_value / len(shards)))
        gain = gain * jnp.repeat(heights, shape[dim] // shards_of).reshape([-1 if axis == dim else 1 for axis in range(len(shape))])
    return gain


def split_up(number_of, total, most, slope):
    portions = [(1 << 20) // math.isqrt(grade ** slope) + 1 for grade in range(2, number_of + 1)]
    rest, counts = total - most - (number_of - 1), [1] * (number_of - 1)
    while rest > 0:
        movable = [i for i in range(number_of - 1) if counts[i] < most]
        whole, left = sum([portions[i] for i in movable]), rest
        for i in movable:
            addition = min(most - counts[i], max(1, left * portions[i] // whole), rest)
            counts[i] = counts[i] + addition
            rest = rest - addition
    return np.array([most] + counts)


def ragged(stream_key, count, total, reach, slope):
    if count == 2:
        one = jax.random.randint(stream_key, (), max(1, total - reach), min(reach, total - 1) + 1)
        return jnp.stack([one, total - one])
    tallies = jnp.asarray(split_up(count, total, reach, slope), jnp.int32)
    couples = (count - 1) // 2
    donor, receiver = tallies[1:1 + 2 * couples:2], tallies[2:2 + 2 * couples:2]
    slack = jnp.minimum(donor - 1, reach - receiver)
    shifted = jax.random.randint(jax.random.fold_in(stream_key, 1), (couples,), 0, 1 << 20) % (slack + 1)
    tallies = tallies.at[1:1 + 2 * couples:2].set(donor - shifted).at[2:2 + 2 * couples:2].set(receiver + shifted)
    return tallies[jax.random.permutation(jax.random.fold_in(stream_key, 2), count)]


def bell_draw(stream_key, shape, deviation, limit, cuts=(), held_as=jnp.bfloat16):
    entries = deviation * jax.random.normal(stream_key, shape, jnp.float32)
    if cuts:
        entries = entries * shard_levels(stream_key, shape, cuts, -0.22, 0.18)
    return jnp.clip(entries, -limit, limit).astype(held_as)


def setup_inputs(seed: int = 0) -> dict:
    streams_of = jax.random.split(jax.random.key(seed), 14)
    queries = draw_queries(jax.random.fold_in(streams_of[13], 71), 0)
    keys = draw_keys(jax.random.fold_in(streams_of[13], 71), 0)
    values = bell_draw(streams_of[2], (TOKENS, KV_W), 3.0, 18.0, ((0, 16), (1, 2)))
    doc_ids = jnp.searchsorted(jnp.cumsum(ragged(streams_of[3], DOCS, TOKENS, TOKENS // 2, 0)), jnp.arange(TOKENS), side="right").astype(jnp.int32)
    sinks = jnp.clip(4.0 * jax.random.uniform(streams_of[4], (A_HEADS,), jnp.float32) ** shard_levels(streams_of[4], (A_HEADS,), ((0, 2),), -0.2, 0.2), 0.0, 4.0)
    residual = draw_residual(jax.random.fold_in(streams_of[13], 71), 0)
    out_weight = bell_draw(streams_of[6], (A_Q, D), A_Q ** -0.5, 0.1875, ((0, 2),))
    norm_gain = jnp.clip(1.0 + 0.18 * jax.random.normal(streams_of[7], (D,), jnp.float32), 0.1, 1.9)
    w_gate = bell_draw(streams_of[8], (D, FF), D ** -0.5, 0.125, ((0, 16), (1, 2)))
    w_value = bell_draw(streams_of[9], (D, FF), D ** -0.5, 0.125, ((0, 16), (1, 2)))
    conv_gate = bell_draw(streams_of[10], (3, FF), 3 ** -0.5, 3.5, ((1, 2),), jnp.float32)
    conv_value = bell_draw(streams_of[11], (3, FF), 3 ** -0.5, 3.5, ((1, 2),), jnp.float32)
    w_down = bell_draw(streams_of[12], (FF, D), FF ** -0.5, 0.078125, ((0, 2), (1, 16)))
    return dict(queries=queries, keys=keys, values=values, doc_ids=doc_ids, sinks=sinks, residual=residual, out_weight=out_weight, norm_gain=norm_gain, w_gate=w_gate, w_value=w_value, conv_gate=conv_gate, conv_value=conv_value, w_down=w_down)


def attend(query_rows, key_ext, value_ext, doc_rows, doc_ext, sinks):
    row_count = query_rows.shape[0]
    block_count = row_count // WINDOW
    kv_heads = key_ext.shape[1] // HEAD_DIM
    group_size = query_rows.shape[1] // (kv_heads * HEAD_DIM)

    def band(t):
        lower = t[:row_count].reshape((block_count, WINDOW) + t.shape[1:])
        upper = t[WINDOW:].reshape((block_count, WINDOW) + t.shape[1:])
        return jnp.concatenate([lower, upper], axis=1)
    query_band = query_rows.astype(jnp.float32).reshape(block_count, WINDOW, kv_heads, group_size, HEAD_DIM)
    key_band = band(key_ext).astype(jnp.float32).reshape(block_count, 2 * WINDOW, kv_heads, HEAD_DIM)
    value_band = band(value_ext).astype(jnp.float32).reshape(block_count, 2 * WINDOW, kv_heads, HEAD_DIM)
    doc_band = band(doc_ext)
    distance = jnp.arange(WINDOW)[:, None] + WINDOW - jnp.arange(2 * WINDOW)[None, :]
    in_window = (distance >= 0) & (distance < WINDOW)
    same_doc = doc_rows.reshape(block_count, WINDOW)[:, :, None] == doc_band[:, None, :]
    keep_mask = in_window[None] & same_doc
    scores = jnp.einsum('nqhgd,nkhd->nhgqk', query_band, key_band) * HEAD_DIM ** (-0.5)
    scores = jnp.where(keep_mask[:, None, None], scores, -jnp.inf)
    sink_logit = sinks.astype(jnp.float32).reshape(kv_heads, group_size)[None, :, :, None, None]
    peak = jnp.maximum(lax.optimization_barrier(jnp.max(scores, axis=-1, keepdims=True)), sink_logit)
    expd = jnp.exp(scores - peak)
    probs = (expd / (lax.optimization_barrier(jnp.sum(expd, axis=-1, keepdims=True)) + jnp.exp(sink_logit - peak))).astype(jnp.bfloat16)
    mixed = jnp.einsum('nhgqk,nkhd->nqhgd', probs.astype(jnp.float32), value_band)
    return mixed.astype(jnp.bfloat16).reshape(row_count, -1)

def convolve(ext_rows, doc_ext, taps):
    center = doc_ext[2:]
    same_one = (doc_ext[1:-1] == center)[:, None]
    same_two = (doc_ext[:-2] == center)[:, None]
    ext32 = ext_rows.astype(jnp.float32)
    result = taps[2] * ext32[2:]
    result = result + jnp.where(same_one, taps[1] * ext32[1:-1], 0.0)
    return result + jnp.where(same_two, taps[0] * ext32[:-2], 0.0)

def reference(queries, keys, values, doc_ids, sinks, residual, out_weight, norm_gain, w_gate, w_value, conv_gate, conv_value, w_down):
    docs_plus = doc_ids + 1
    key_pad = jnp.concatenate([jnp.zeros((WINDOW, KV_W), jnp.bfloat16), keys], axis=0)
    value_pad = jnp.concatenate([jnp.zeros((WINDOW, KV_W), jnp.bfloat16), values], axis=0)
    doc_pad = jnp.concatenate([jnp.zeros((WINDOW,), jnp.int32), docs_plus], axis=0)

    def attend_shard(index):
        start = (index * TOK_SP).astype(jnp.int32)
        return attend(lax.dynamic_slice_in_dim(queries, start, TOK_SP, 0), lax.dynamic_slice_in_dim(key_pad, start, TOK_SP + WINDOW, 0), lax.dynamic_slice_in_dim(value_pad, start, TOK_SP + WINDOW, 0), lax.dynamic_slice_in_dim(docs_plus, start, TOK_SP, 0), lax.dynamic_slice_in_dim(doc_pad, start, TOK_SP + WINDOW, 0), sinks)
    shard_ids = jnp.arange(N_SP, dtype=jnp.int32)
    attn = lax.map(attend_shard, shard_ids).reshape(TOKENS, A_Q)
    proj = jnp.dot(attn, out_weight, preferred_element_type=jnp.float32)
    mid = (residual.astype(jnp.float32) + proj).astype(jnp.bfloat16)
    mid32 = mid.astype(jnp.float32)
    normed = (mid32 * lax.rsqrt(lax.optimization_barrier(jnp.mean(mid32 * mid32, axis=-1, keepdims=True)) + 1e-06) * norm_gain).astype(jnp.bfloat16)
    normed_pad = jnp.concatenate([jnp.zeros((2, D), jnp.bfloat16), normed], axis=0)
    doc_two = jnp.concatenate([jnp.zeros((2,), jnp.int32), docs_plus], axis=0)

    def mlp_shard(index):
        start = (index * TOK_SP).astype(jnp.int32)
        rows_ext = lax.dynamic_slice_in_dim(normed_pad, start, TOK_SP + 2, 0)
        doc_ext = lax.dynamic_slice_in_dim(doc_two, start, TOK_SP + 2, 0)
        gate_pre = jnp.dot(rows_ext, w_gate, preferred_element_type=jnp.float32).astype(jnp.bfloat16)
        value_pre = jnp.dot(rows_ext, w_value, preferred_element_type=jnp.float32).astype(jnp.bfloat16)
        gate_conv = convolve(gate_pre, doc_ext, conv_gate)
        value_conv = convolve(value_pre, doc_ext, conv_value)
        hidden = (jax.nn.silu(gate_conv) * value_conv).astype(jnp.bfloat16)
        return jnp.dot(hidden, w_down, preferred_element_type=jnp.float32)
    mlp = lax.map(mlp_shard, shard_ids).reshape(TOKENS, D)
    return (mid32 + mlp).astype(jnp.bfloat16)
```

```python
import functools

import jax
import jax.numpy as jnp
from jax import lax
from jax.experimental import pallas as pl
from jax.experimental.pallas import tpu as pltpu
from jax.sharding import PartitionSpec as P


HEAD_DIM = 64
WINDOW = 128
ROW_TILE = 128
SUB = 2
HALO = 16
TILE = 256
VMEM_BYTES = 67043328
MESH = pl.DeviceIdType.MESH


def shifted(shard, axis, by):
    size = lax.axis_size(axis)
    pairs = [(i, i + by) for i in range(size) if 0 <= i + by < size]
    return lax.ppermute(shard, axis, pairs)


def turned(t, axis, by):
    size = lax.axis_size(axis)
    return lax.ppermute(t, axis, [(i, (i + by) % size) for i in range(size)])


def core_swap(t):
    size = lax.axis_size("sp")
    return lax.ppermute(t, "sp", [(i, i ^ 1) for i in range(size)])


def parity_gather(t):
    size = lax.axis_size("sp")
    groups = [list(range(0, size, 2)), list(range(1, size, 2))]
    return lax.all_gather(t, "sp", axis=0, tiled=True, axis_index_groups=groups)


def ring_gather(t):
    chips = lax.axis_size("sp") // 2
    order = list(range(0, chips, 2)) + list(range(1, chips, 2))[::-1]
    chip = lax.axis_index("sp") // 2
    place = jnp.where(chip % 2 == 0, chip // 2, chips - 1 - chip // 2)

    def hop(piece, by):
        pairs = [
            (2 * order[k] + c, 2 * order[(k + by) % chips] + c)
            for k in range(chips)
            for c in range(2)
        ]
        return lax.ppermute(piece, "sp", pairs)

    def chip_at(k):
        k = (k + chips) % chips
        return jnp.where(k < chips // 2, 2 * k, 2 * (chips - 1 - k) + 1)

    depth = t.shape[0]
    pieces = [(chip, t)]
    up = down = t
    for step in range(1, chips // 2 + 1):
        up = hop(up, 1)
        pieces.append((chip_at(place - step), up))
        if step < chips - step:
            down = hop(down, -1)
            pieces.append((chip_at(place + step), down))
    whole = jnp.zeros((chips * depth,) + t.shape[1:], t.dtype)
    for at, piece in pieces:
        whole = lax.dynamic_update_slice_in_dim(whole, piece, at * depth, 0)
    return whole


def by_parity(t, depth):
    rows, width = t.shape
    blocks = width // depth
    tile = min(ROW_TILE, rows)

    def kernel(in_ref, out_ref):
        for j in range(blocks):
            to = (j // 2 + (j % 2) * (blocks // 2)) * depth
            out_ref[:, to : to + depth] = in_ref[:, j * depth : (j + 1) * depth]

    return pl.pallas_call(
        kernel,
        out_shape=jax.ShapeDtypeStruct(t.shape, t.dtype),
        grid=(rows // tile,),
        in_specs=[pl.BlockSpec((tile, width), lambda i: (i, 0))],
        out_specs=pl.BlockSpec((tile, width), lambda i: (i, 0)),
        cost_estimate=pl.CostEstimate(
            flops=0, bytes_accessed=2 * t.size * t.dtype.itemsize, transcendentals=0
        ),
    )(t)


def finish(mid, sums, depth):
    rows, width = mid.shape
    blocks = width // depth
    tile = min(ROW_TILE, rows)

    def kernel(mid_ref, even_ref, odd_ref, out_ref):
        for j in range(blocks):
            at = (j // 2) * depth
            held = at + (j % 2) * (width // 2)
            sum_ref = odd_ref if j % 2 else even_ref
            out_ref[:, j * depth : (j + 1) * depth] = (
                mid_ref[:, held : held + depth].astype(jnp.float32)
                + sum_ref[:, at : at + depth]
            ).astype(out_ref.dtype)

    half_spec = pl.BlockSpec((tile, width // 2), lambda i: (i, 0))
    return pl.pallas_call(
        kernel,
        out_shape=jax.ShapeDtypeStruct(mid.shape, mid.dtype),
        grid=(rows // tile,),
        in_specs=[pl.BlockSpec((tile, width), lambda i: (i, 0)), half_spec, half_spec],
        out_specs=pl.BlockSpec((tile, width), lambda i: (i, 0)),
        cost_estimate=pl.CostEstimate(
            flops=mid.size, bytes_accessed=8 * mid.size, transcendentals=0
        ),
    )(mid, *sums)


def attend(query_rows, key_ext, value_ext, doc_rows, doc_ext, sinks):
    row_count = query_rows.shape[0]
    block_count = row_count // WINDOW
    kv_heads = key_ext.shape[1] // HEAD_DIM
    group_size = query_rows.shape[1] // (kv_heads * HEAD_DIM)

    def band(t):
        lower = t[:row_count].reshape((block_count, WINDOW) + t.shape[1:])
        upper = t[WINDOW:].reshape((block_count, WINDOW) + t.shape[1:])
        return jnp.concatenate([lower, upper], axis=1)

    query_band = query_rows.reshape(block_count, WINDOW, kv_heads, group_size, HEAD_DIM)
    key_band = band(key_ext).reshape(block_count, 2 * WINDOW, kv_heads, HEAD_DIM)
    value_band = band(value_ext).reshape(block_count, 2 * WINDOW, kv_heads, HEAD_DIM)
    doc_band = band(doc_ext)
    distance = jnp.arange(WINDOW)[:, None] + WINDOW - jnp.arange(2 * WINDOW)[None, :]
    in_window = (distance >= 0) & (distance < WINDOW)
    same_doc = doc_rows.reshape(block_count, WINDOW)[:, :, None] == doc_band[:, None, :]
    keep_mask = in_window[None] & same_doc
    scores = jnp.einsum(
        "nqhgd,nkhd->nhgqk", query_band, key_band, preferred_element_type=jnp.float32
    ) * HEAD_DIM ** (-0.5)
    scores = jnp.where(keep_mask[:, None, None], scores, -jnp.inf)
    sink_logit = sinks.reshape(kv_heads, group_size)[None, :, :, None, None]
    peak = jnp.maximum(jnp.max(scores, axis=-1, keepdims=True), sink_logit)
    expd = jnp.exp(scores - peak)
    probs = (expd / (jnp.sum(expd, axis=-1, keepdims=True) + jnp.exp(sink_logit - peak))).astype(
        jnp.bfloat16
    )
    mixed = jnp.einsum("nhgqk,nkhd->nqhgd", probs, value_band, preferred_element_type=jnp.float32)
    return mixed.astype(jnp.bfloat16).reshape(row_count, -1)


def convolve(ext_rows, doc_ext, taps):
    center = doc_ext[2:]
    same_one = (doc_ext[1:-1] == center)[:, None]
    same_two = (doc_ext[:-2] == center)[:, None]
    ext32 = ext_rows.astype(jnp.float32)
    result = taps[2] * ext32[2:]
    result = result + jnp.where(same_one, taps[1] * ext32[1:-1], 0.0)
    return result + jnp.where(same_two, taps[0] * ext32[:-2], 0.0)


def per_device(
    queries,
    keys,
    values,
    doc_ids,
    sinks,
    residual,
    out_weight,
    norm_gain,
    w_gate,
    w_value,
    conv_gate,
    conv_value,
    w_down,
):
    core = lax.axis_index("sp") % 2
    tp = lax.axis_index("tp")
    n_tp = lax.axis_size("tp")
    rows = doc_ids.shape[0]
    part_rows = rows // n_tp
    depth = w_gate.shape[0]
    width = residual.shape[1]
    half = width // 2
    part_index = [(tp + n_tp - d) % n_tp for d in range(n_tp)]

    gate_own = parity_gather(w_gate)
    value_own = ring_gather(w_value)
    down_t = w_down.T
    inner = down_t.shape[1] // 2
    low, high = down_t[:, :inner], down_t[:, inner:]
    kept_half = jnp.where(core == 0, low, high)
    came_half = core_swap(jnp.where(core == 0, high, low))
    even_piece = jnp.where(core == 0, kept_half, came_half)
    odd_piece = jnp.where(core == 0, came_half, kept_half)
    down_odd = parity_gather(odd_piece)
    down_even = parity_gather(even_piece)
    gate_far = core_swap(gate_own)
    value_far = core_swap(value_own)

    out_far = [turned(out_weight, "tp", d) for d in range(1, n_tp)]
    out_parts = [by_parity(t, depth) for t in [out_weight] + out_far]
    residual = by_parity(residual, depth)
    norm_gain = norm_gain.reshape(-1, 2, depth).swapaxes(0, 1).reshape(-1)
    docs_plus = doc_ids + 1
    prev_keys, prev_values, prev_docs = shifted(
        (keys[-WINDOW:], values[-WINDOW:], docs_plus[-WINDOW:]), "sp", 1
    )
    key_ext = jnp.concatenate([prev_keys, keys], axis=0)
    value_ext = jnp.concatenate([prev_values, values], axis=0)
    doc_ext = jnp.concatenate([prev_docs, docs_plus], axis=0)
    head_out = attend(queries, key_ext, value_ext, docs_plus, doc_ext, sinks)

    def rows_of(t, index):
        return lax.dynamic_slice_in_dim(t, index * part_rows, part_rows, 0)

    proj = jnp.dot(rows_of(head_out, tp), out_parts[0], preferred_element_type=jnp.float32)
    for d in range(1, n_tp):
        heads_far = turned(rows_of(head_out, (tp + d) % n_tp), "tp", d)
        proj = proj + jnp.dot(heads_far, out_parts[d], preferred_element_type=jnp.float32)
    mid = (residual.astype(jnp.float32) + proj).astype(jnp.bfloat16)
    mid32 = mid.astype(jnp.float32)
    normed = (
        mid32 * lax.rsqrt(jnp.mean(mid32 * mid32, axis=-1, keepdims=True) + 1e-06) * norm_gain
    ).astype(jnp.bfloat16)
    even, odd = normed[:, :half], normed[:, half:]
    own = [jnp.where(core == 0, even, odd)]
    far = [jnp.where(core == 0, odd, even)]
    for d in range(1, n_tp):
        own.append(turned(own[0], "tp", d))
        far.append(turned(far[0], "tp", d))

    def up(own, far, w_own, w_far):
        total = jnp.dot(own, w_own, preferred_element_type=jnp.float32)
        return (total + jnp.dot(far, w_far, preferred_element_type=jnp.float32)).astype(
            jnp.bfloat16
        )

    gate_parts = [up(o, f, gate_own, gate_far) for o, f in zip(own, far)]
    value_parts = [up(o, f, value_own, value_far) for o, f in zip(own, far)]

    conv_docs = jnp.concatenate([prev_docs[-2:], docs_plus], axis=0)
    part_docs = [
        lax.dynamic_slice_in_dim(conv_docs, i * part_rows, part_rows + 2, 0) for i in part_index
    ]

    def conv_parts(parts, taps):
        tails = [p[-2:] for p in parts]
        last = tails[0]
        for d in range(1, n_tp):
            last = jnp.where(part_index[d] == n_tp - 1, tails[d], last)
        prev = shifted(last, "sp", 1)
        result = []
        for d in range(n_tp):
            halo = jnp.where(part_index[d] == 0, prev, tails[(d + 1) % n_tp])
            result.append(
                convolve(jnp.concatenate([halo, parts[d]], axis=0), part_docs[d], taps)
            )
        return result

    gate_conv = conv_parts(gate_parts, conv_gate)
    value_conv = conv_parts(value_parts, conv_value)
    hidden = [
        (jax.nn.silu(g) * v).astype(jnp.bfloat16) for g, v in zip(gate_conv, value_conv)
    ]

    def down(units, w_t):
        return lax.dot_general(
            units, w_t, (((1,), (1,)), ((), ())), preferred_element_type=jnp.float32
        )

    own_units = [jnp.where(core == 0, h[:, :inner], h[:, inner:]) for h in hidden]
    far_units = [jnp.where(core == 0, h[:, inner:], h[:, :inner]) for h in hidden]

    def down_sums(w_own):
        w_far = core_swap(w_own)
        came = []
        for d in range(1, n_tp):
            sent = (down(own_units[d], w_own) + down(far_units[d], w_far)).astype(
                jnp.bfloat16
            )
            came.append(turned(sent, "tp", -d))
        kept = down(own_units[0], w_own) + down(far_units[0], w_far)
        for t in came:
            kept = kept + t.astype(jnp.float32)
        return kept

    odd_sum = down_sums(down_odd)
    even_sum = down_sums(down_even)
    sums = (even_sum, odd_sum)
    return finish(mid, sums, depth)


def mult(x, m):
    return x if isinstance(x, int) else pl.multiple_of(x, m)


def ring_chip(place, chips):
    odd = lax.div(place, chips // 2)
    return (1 - odd) * (2 * place) + odd * (2 * (chips - 1 - place) + 1)


def layer_kernel(
    n_sp,
    n_tp,
    queries,
    keys,
    values,
    docs,
    sinks,
    residual,
    out_weight,
    norm_gain,
    w_gate,
    w_value,
    conv_gate,
    conv_value,
    w_down,
    out,
    wg,
    wv,
    wd,
    nrm,
    hid,
    pre,
    q_v,
    k_v,
    v_v,
    doc_v,
    doc_col,
    same_one,
    same_two,
    att,
    heads,
    ow,
    mid,
    gain_v,
    cg_v,
    cv_v,
    send,
    came,
    own,
    local_sem,
    ring_send,
    ring_recv,
    sib_send,
    sib_recv,
    halo_send,
    halo_recv,
    ow_send,
    ow_recv,
    heads_send,
    heads_recv,
    nrm_send,
    nrm_recv,
    sum_send,
    sum_recv,
    out_sem,
):
    sp = lax.axis_index("sp")
    tp = lax.axis_index("tp")
    chips = n_sp // 2
    core = lax.rem(sp, 2)
    chip = lax.div(sp, 2)
    odd = lax.rem(chip, 2)
    place = (1 - odd) * lax.div(chip, 2) + odd * (chips - 1 - lax.div(chip, 2))
    way = 1 - 2 * core
    down_sp = 2 * ring_chip(lax.rem(place + way + chips, chips), chips) + core
    up_sp = 2 * ring_chip(lax.rem(place - way + chips, chips), chips) + core
    sib_sp = sp + way
    next_sp = lax.rem(sp + 1, n_sp)
    prev_sp = lax.rem(sp + n_sp - 1, n_sp)

    rows, q_width = queries.shape
    part = rows // n_tp
    depth, units = w_gate.shape
    kv_heads = keys.shape[1] // HEAD_DIM
    group = q_width // keys.shape[1]
    blocks = rows // WINDOW
    part_blocks = part // WINDOW
    ow_half = q_width // 2
    unit_tiles = units // TILE
    events = (chips - 1) * SUB

    def peer(d):
        return lax.rem(tp + d, n_tp)

    def held(h):
        return 2 * ring_chip(lax.rem(place - way * h + chips, chips), chips) + core

    def sib_held(h):
        return 2 * ring_chip(lax.rem(place + way * h + chips, chips), chips) + 1 - core

    def piece(w, j, s):
        if w == 2:
            size = units // SUB
            return wd.at[j, pl.ds(mult(s * size, size), size), :]
        size = depth // SUB
        buf = (wg, wv)[w]
        return buf.at[pl.ds(mult(j * depth + s * size, size), size), :]

    def own_piece(w, s):
        ref = (w_gate, w_value, w_down)[w]
        size = ref.shape[0] // SUB
        return ref.at[pl.ds(s * size, size), :]

    def remote(src, dst, send_sem, recv_sem, device):
        return pltpu.make_async_remote_copy(
            src_ref=src,
            dst_ref=dst,
            send_sem=send_sem,
            recv_sem=recv_sem,
            device_id=device,
            device_id_type=MESH,
        )

    def ring_copy(w, h, s, src=None):
        dst = piece(w, held(h - 1), s)
        return remote(
            dst if src is None else src,
            dst,
            ring_send.at[w, h, s],
            ring_recv.at[w, h, s],
            (down_sp, tp),
        )

    def ring_wait(w, h, s):
        dst = piece(w, held(h), s)
        remote(
            dst, dst, ring_send.at[w, h, s], ring_recv.at[w, h, s], (down_sp, tp)
        ).wait_recv()

    def sib_copy(w, h, s, src=None):
        dst = piece(w, held(h), s)
        return remote(
            dst if src is None else src,
            dst,
            sib_send.at[w, h, s],
            sib_recv.at[w, h, s],
            (sib_sp, tp),
        )

    def sib_wait(w, h, s):
        dst = piece(w, sib_held(h), s)
        remote(
            dst, dst, sib_send.at[w, h, s], sib_recv.at[w, h, s], (sib_sp, tp)
        ).wait_recv()

    def start_own(w):
        for s in range(SUB):
            ring_copy(w, 1, s, own_piece(w, s)).start()
        for s in range(SUB):
            sib_copy(w, 0, s, own_piece(w, s)).start()

    def service(w, e):
        h = 1 + (e // SUB if isinstance(e, int) else lax.div(e, SUB))
        s = e % SUB if isinstance(e, int) else lax.rem(e, SUB)
        ring_wait(w, h, s)
        if isinstance(e, int):
            if h < chips - 1:
                ring_copy(w, h + 1, s).start()
        else:

            @pl.when(h < chips - 1)
            def _():
                ring_copy(w, h + 1, s).start()

        sib_copy(w, h, s).start()

    def serve(w, first, last):
        if last > first:

            @pl.loop(first, last)
            def _(e):
                service(w, e)

    local = [
        (keys, k_v.at[pl.ds(WINDOW, rows), :]),
        (values, v_v.at[pl.ds(WINDOW, rows), :]),
        (docs, doc_v.at[pl.ds(8, blocks), :]),
        (queries, q_v),
        (residual, mid),
        (out_weight, ow.at[tp]),
        (norm_gain, gain_v),
        (conv_gate, cg_v),
        (conv_value, cv_v),
        (w_gate, wg.at[pl.ds(mult(sp * depth, depth), depth), :]),
        (w_value, wv.at[pl.ds(mult(sp * depth, depth), depth), :]),
        (w_down, wd.at[sp]),
    ]
    local = [
        pltpu.make_async_copy(src, dst, local_sem.at[i]) for i, (src, dst) in enumerate(local)
    ]
    for copy in local:
        copy.start()

    barrier = pltpu.get_barrier_semaphore()
    greeted = [(down_sp, tp), (up_sp, tp), (sib_sp, tp), (next_sp, tp), (prev_sp, tp)]
    greeted += [(sp, peer(d)) for d in range(1, n_tp)]
    for device in greeted:
        pl.semaphore_signal(barrier, inc=1, device_id=device, device_id_type=MESH)
    pl.semaphore_wait(barrier, len(greeted))

    halos = [
        (keys.at[pl.ds(rows - WINDOW, WINDOW), :], k_v.at[pl.ds(0, WINDOW), :]),
        (values.at[pl.ds(rows - WINDOW, WINDOW), :], v_v.at[pl.ds(0, WINDOW), :]),
        (docs.at[pl.ds(blocks - 1, 1), :], doc_v.at[pl.ds(7, 1), :]),
    ]
    halos = [
        remote(src, dst, halo_send.at[i], halo_recv.at[i], (next_sp, tp))
        for i, (src, dst) in enumerate(halos)
    ]
    for copy in halos:
        copy.start()
    start_own(0)

    def ow_rows(t, c):
        return ow.at[t, pl.ds(mult(c * ow_half, ow_half), ow_half), :]

    ow_src = out_weight.at[pl.ds(mult(core * ow_half, ow_half), ow_half), :]
    ow_out = [
        remote(ow_src, ow_rows(tp, core), ow_send.at[0, d], ow_recv.at[0, d], (sp, peer(n_tp - d)))
        for d in range(1, n_tp)
    ]
    for copy in ow_out:
        copy.start()

    for i in range(3):
        local[i].wait()
    for copy in halos:
        copy.wait_recv()
    local[3].wait()

    lane = lax.broadcasted_iota(jnp.int32, (WINDOW, 2 * HEAD_DIM), 1)
    low_lane = lane < HEAD_DIM
    doc_v[7:8, :] = jnp.where(sp == 0, 0, doc_v[7:8, :])
    for b in range(-1, blocks):
        row = doc_v[8 + b : 9 + b, :]
        column = jnp.broadcast_to(row, (WINDOW, WINDOW)).T
        if b < 0:
            doc_col[0:8, :] = column[WINDOW - 8 :, :]
        else:
            doc_col[8 + b * WINDOW : 8 + (b + 1) * WINDOW, :] = column
    for b in range(blocks):
        at = 8 + b * WINDOW
        here = doc_col[at : at + WINDOW, :]
        back_one = doc_col[at - 1 : at - 1 + WINDOW, :]
        back_two = doc_col[at - 2 : at - 2 + WINDOW, :]
        to = slice(b * WINDOW, (b + 1) * WINDOW)
        same_one[to, :] = jnp.where(here == back_one, 1.0, 0.0)
        same_two[to, :] = jnp.where(here == back_two, 1.0, 0.0)

    q_index = lax.broadcasted_iota(jnp.int32, (WINDOW, 2 * WINDOW), 0)
    k_index = lax.broadcasted_iota(jnp.int32, (WINDOW, 2 * WINDOW), 1)
    first_rows = lax.broadcasted_iota(jnp.int32, (2 * WINDOW, 1), 0) < WINDOW

    def attend_block(b):
        base = mult(b * WINDOW, WINDOW)
        key_docs = jnp.concatenate([doc_v[pl.ds(7 + b, 1), :], doc_v[pl.ds(8 + b, 1), :]], axis=1)
        here = doc_col[pl.ds(mult(8 + base, 8), WINDOW), :]
        keep = (k_index > q_index) & (k_index <= q_index + WINDOW)
        keep = keep & (jnp.concatenate([here, here], axis=1) == key_docs)
        keep = jnp.concatenate([keep, keep], axis=0)
        k_band = k_v[pl.ds(base, 2 * WINDOW), :]
        v_band = v_v[pl.ds(base, 2 * WINDOW), :]
        for g in range(kv_heads):
            at = slice(g * HEAD_DIM, (g + 1) * HEAD_DIM)
            kk = jnp.concatenate([k_band[:, at], k_band[:, at]], axis=1)
            vv = jnp.concatenate([v_band[:, at], v_band[:, at]], axis=1)
            for pair in range(group // 2):
                head = g * group + 2 * pair
                lanes = slice(head * HEAD_DIM, (head + 2) * HEAD_DIM)
                both = q_v[pl.ds(base, WINDOW), lanes]
                zero = jnp.zeros_like(both)
                split = jnp.concatenate(
                    [jnp.where(low_lane, both, zero), jnp.where(low_lane, zero, both)], axis=0
                )
                scores = lax.dot_general(
                    split, kk, (((1,), (1,)), ((), ())), preferred_element_type=jnp.float32
                ) * HEAD_DIM ** (-0.5)
                scores = jnp.where(keep, scores, -1e30)
                sink = jnp.where(first_rows, sinks[head], sinks[head + 1])
                peak = jnp.maximum(jnp.max(scores, axis=1, keepdims=True), sink)
                expd = jnp.exp(scores - peak)
                total = jnp.sum(expd, axis=1, keepdims=True) + jnp.exp(sink - peak)
                probs = (expd * (1.0 / total)).astype(jnp.bfloat16)
                mixed = jnp.dot(probs, vv, preferred_element_type=jnp.float32)
                att[pl.ds(base, WINDOW), lanes] = jnp.where(
                    low_lane, mixed[:WINDOW], mixed[WINDOW:]
                ).astype(jnp.bfloat16)

    early = events // 7
    pl.loop(0, blocks - part_blocks)(
        lambda i: attend_block(lax.rem((tp + 1) * part_blocks + i, blocks))
    )
    serve(0, 0, early // 2)
    pl.loop(0, part_blocks)(lambda i: attend_block(tp * part_blocks + i))
    heads_out = [
        remote(
            att.at[pl.ds(mult(peer(n_tp - d) * part, part), part), :],
            heads.at[d - 1],
            heads_send.at[d],
            heads_recv.at[d],
            (sp, peer(n_tp - d)),
        )
        for d in range(1, n_tp)
    ]
    for copy in heads_out:
        copy.start()
    before_proj = 3 * early
    serve(0, early // 2, before_proj)

    for i in range(4, 9):
        local[i].wait()
    ow_on = []
    for d in range(1, n_tp):
        got = ow_rows(peer(d), core)
        remote(got, got, ow_send.at[0, d], ow_recv.at[0, d], (sp, peer(n_tp - d))).wait_recv()
        copy = remote(got, got, ow_send.at[1, d], ow_recv.at[1, d], (sib_sp, tp))
        copy.start()
        ow_on.append(copy)
    for d in range(1, n_tp):
        got = ow_rows(peer(d), 1 - core)
        remote(got, got, ow_send.at[1, d], ow_recv.at[1, d], (sib_sp, tp)).wait_recv()
        heads_out[d - 1].wait_recv()

    part_base = tp * part

    def nrm_rows(t, i):
        return nrm.at[pl.ds(mult(HALO + t * part + i * WINDOW, HALO), WINDOW), :]

    def nrm_copy(i, d):
        at = nrm_rows(tp, i)
        return remote(at, at, nrm_send.at[i, d], nrm_recv.at[i, d], (sp, peer(n_tp - d)))

    def project(i):
        at = pl.ds(mult(i * WINDOW, WINDOW), WINDOW)
        mine = att[pl.ds(mult(part_base + i * WINDOW, WINDOW), WINDOW), :]
        proj = jnp.dot(mine, ow[tp], preferred_element_type=jnp.float32)
        for d in range(1, n_tp):
            proj = proj + jnp.dot(
                heads[d - 1, at, :], ow[peer(d)], preferred_element_type=jnp.float32
            )
        rounded = (mid[at, :].astype(jnp.float32) + proj).astype(jnp.bfloat16)
        mid[at, :] = rounded
        wide = rounded.astype(jnp.float32)
        scale = lax.rsqrt(jnp.mean(wide * wide, axis=1, keepdims=True) + 1e-06)
        normed = (wide * scale * gain_v[...]).astype(jnp.bfloat16)
        nrm[pl.ds(mult(HALO + part_base + i * WINDOW, HALO), WINDOW), :] = normed

    @pl.loop(0, part_blocks)
    def _(i):
        project(i)
        for d in range(1, n_tp):

            @pl.when(i > 0)
            def _():
                nrm_copy(i - 1, d).start()

        @pl.when(before_proj + i < events)
        def _():
            service(0, before_proj + i)

    for d in range(1, n_tp):
        nrm_copy(part_blocks - 1, d).start()

    after_proj = min(events, before_proj + part_blocks)
    serve(0, after_proj, events)
    start_own(1)
    early_value = 2 * early
    serve(1, 0, early_value)

    @pl.loop(0, part_blocks)
    def _(i):
        for d in range(1, n_tp):
            got = nrm_rows(peer(d), i)
            remote(
                got, got, nrm_send.at[i, d], nrm_recv.at[i, d], (sp, peer(n_tp - d))
            ).wait_recv()

    nrm_halo = remote(
        nrm.at[pl.ds(rows, HALO), :],
        nrm.at[pl.ds(0, HALO), :],
        halo_send.at[3],
        halo_recv.at[3],
        (next_sp, tp),
    )
    nrm_halo.start()
    for i in range(9, 12):
        local[i].wait()

    def all_of_sib(w):
        @pl.loop(0, chips * SUB)
        def _(e):
            sib_wait(w, lax.div(e, SUB), lax.rem(e, SUB))

    all_of_sib(0)
    nrm_halo.wait_recv()

    half_rows = HALO + rows // 2

    def up_tile(w_ref, taps, n):
        cols = pl.ds(mult(n * TILE, TILE), TILE)
        for lo, hi in ((0, half_rows), (half_rows, HALO + rows)):
            pre[lo:hi, :] = (
                jnp.dot(nrm[lo:hi, :], w_ref[:, cols], preferred_element_type=jnp.float32)
                .astype(jnp.bfloat16)
                .astype(jnp.float32)
            )
        tap = taps[:, cols]
        for b in range(blocks):
            at = HALO + b * WINDOW
            to = slice(b * WINDOW, (b + 1) * WINDOW)
            one = jnp.concatenate([same_one[to, :]] * (TILE // WINDOW), axis=1)
            two = jnp.concatenate([same_two[to, :]] * (TILE // WINDOW), axis=1)
            conv = tap[2:3] * pre[at : at + WINDOW, :]
            conv = conv + one * (tap[1:2] * pre[at - 1 : at - 1 + WINDOW, :])
            conv = conv + two * (tap[0:1] * pre[at - 2 : at - 2 + WINDOW, :])
            yield to, cols, conv

    def spread(w, first, count, i):
        before = lax.div(i * count, unit_tiles)
        after = lax.div((i + 1) * count, unit_tiles)

        @pl.when(after > before)
        def _():
            service(w, first + before)

    gate_count = min(unit_tiles, events - early_value)

    @pl.loop(0, unit_tiles)
    def _(n):
        for to, cols, conv in up_tile(wg, cg_v, n):
            hid[to, cols] = (conv / (1.0 + jnp.exp(-conv))).astype(jnp.bfloat16)
        spread(1, early_value, gate_count, n)

    serve(1, early_value + gate_count, events)
    start_own(2)
    all_of_sib(1)
    down_count = min(unit_tiles, 3 * early)

    @pl.loop(0, unit_tiles)
    def _(n):
        for to, cols, conv in up_tile(wv, cv_v, n):
            hid[to, cols] = (hid[to, cols].astype(jnp.float32) * conv).astype(jnp.bfloat16)
        spread(2, 0, down_count, n)

    def sum_copy(h, d):
        return remote(
            send.at[h, d - 1], came.at[h, d - 1], sum_send.at[h, d], sum_recv.at[h, d], (sp, peer(d))
        )

    def out_copy(h, c):
        j = held(h) if c == 0 else sib_held(h)
        cols = pl.ds(mult(j * depth, depth), depth)
        return pltpu.make_async_copy(mid.at[:, cols], out.at[:, cols], out_sem.at[h, c])

    def finish_hop(h):
        for d in range(1, n_tp):
            got = came.at[h, d - 1]
            remote(
                got, got, sum_send.at[h, d], sum_recv.at[h, d], (sp, peer(d))
            ).wait_recv()
        for c in range(2):
            j = held(h) if c == 0 else sib_held(h)
            cols = pl.ds(mult(j * depth, depth), depth)
            from_cols = slice(c * depth, (c + 1) * depth)
            total = own[:, from_cols] + mid[:, cols].astype(jnp.float32)
            for d in range(1, n_tp):
                total = total + came[h, d - 1, :, from_cols].astype(jnp.float32)
            mid[:, cols] = total.astype(jnp.bfloat16)

    def down_rows(h, t):
        lhs = hid[pl.ds(mult(t * part, part), part), :]
        rhs = jnp.concatenate([wd[held(h)], wd[sib_held(h)]], axis=1)
        return jnp.dot(lhs, rhs, preferred_element_type=jnp.float32)

    @pl.loop(0, chips)
    def _(h):
        for s in range(SUB):

            @pl.when((h - 1) * SUB + s >= down_count)
            def _():
                service(2, (h - 1) * SUB + s)

        for s in range(SUB):
            sib_wait(2, h, s)
        for d in range(1, n_tp):
            send[h, d - 1] = down_rows(h, peer(d)).astype(jnp.bfloat16)

        @pl.when(h > 0)
        def _():
            finish_hop(h - 1)
            for c in range(2):
                out_copy(h - 1, c).start()

        own[...] = down_rows(h, tp)
        for d in range(1, n_tp):
            sum_copy(h, d).start()

    finish_hop(chips - 1)
    for c in range(2):
        out_copy(chips - 1, c).start()

    for copy in halos + heads_out + ow_out + ow_on + [nrm_halo]:
        copy.wait_send()

    @pl.loop(0, part_blocks)
    def _(i):
        for d in range(1, n_tp):
            nrm_copy(i, d).wait_send()

    for w in range(3):

        @pl.loop(0, chips)
        def _(h):
            for s in range(SUB):

                @pl.when(h > 0)
                def _():
                    ring_copy(w, h, s).wait_send()

                sib_copy(w, h, s).wait_send()

    @pl.loop(0, chips)
    def _(h):
        for d in range(1, n_tp):
            sum_copy(h, d).wait_send()
        for c in range(2):
            out_copy(h, c).wait()


def whole_layer(n_sp, n_tp, queries, keys, values, doc_ids, sinks, residual, out_weight,
                norm_gain, w_gate, w_value, conv_gate, conv_value, w_down):
    rows, q_width = queries.shape
    kv_width = keys.shape[1]
    part, width = residual.shape
    depth, units = w_gate.shape
    chips = n_sp // 2
    bf16, f32 = jnp.bfloat16, jnp.float32
    dma = pltpu.SemaphoreType.DMA
    part_blocks = part // WINDOW
    scratch = [
        pltpu.VMEM((width, units), bf16),
        pltpu.VMEM((width, units), bf16),
        pltpu.VMEM((n_sp, units, depth), bf16),
        pltpu.VMEM((HALO + rows, width), bf16),
        pltpu.VMEM((rows, units), bf16),
        pltpu.VMEM((HALO + rows, TILE), f32),
        pltpu.VMEM((rows, q_width), bf16),
        pltpu.VMEM((WINDOW + rows, kv_width), bf16),
        pltpu.VMEM((WINDOW + rows, kv_width), bf16),
        pltpu.VMEM((8 + rows // WINDOW, WINDOW), jnp.int32),
        pltpu.VMEM((8 + rows, WINDOW), jnp.int32),
        pltpu.VMEM((rows, WINDOW), f32),
        pltpu.VMEM((rows, WINDOW), f32),
        pltpu.VMEM((rows, q_width), bf16),
        pltpu.VMEM((n_tp - 1, part, q_width), bf16),
        pltpu.VMEM((n_tp, q_width, width), bf16),
        pltpu.VMEM((part, width), bf16),
        pltpu.VMEM((1, width), f32),
        pltpu.VMEM((3, units), f32),
        pltpu.VMEM((3, units), f32),
        pltpu.VMEM((chips, n_tp - 1, part, 2 * depth), bf16),
        pltpu.VMEM((chips, n_tp - 1, part, 2 * depth), bf16),
        pltpu.VMEM((part, 2 * depth), f32),
        dma((12,)),
        dma((3, chips, SUB)),
        dma((3, chips, SUB)),
        dma((3, chips, SUB)),
        dma((3, chips, SUB)),
        dma((4,)),
        dma((4,)),
        dma((2, n_tp)),
        dma((2, n_tp)),
        dma((n_tp,)),
        dma((n_tp,)),
        dma((part_blocks, n_tp)),
        dma((part_blocks, n_tp)),
        dma((chips, n_tp)),
        dma((chips, n_tp)),
        dma((chips, 2)),
    ]
    any_spec = pl.BlockSpec(memory_space=pl.ANY)
    specs = [any_spec] * 13
    specs[4] = pl.BlockSpec(memory_space=pltpu.SMEM)
    return pl.pallas_call(
        functools.partial(layer_kernel, n_sp, n_tp),
        out_shape=jax.ShapeDtypeStruct(residual.shape, residual.dtype),
        in_specs=specs,
        out_specs=any_spec,
        scratch_shapes=scratch,
        compiler_params=pltpu.CompilerParams(
            collective_id=0, has_side_effects=True, vmem_limit_bytes=VMEM_BYTES
        ),
    )(
        queries,
        keys,
        values,
        (doc_ids + 1).reshape(rows // WINDOW, WINDOW),
        sinks,
        residual,
        out_weight,
        norm_gain.reshape(1, width),
        w_gate,
        w_value,
        conv_gate,
        conv_value,
        w_down,
    )


def in_one_kernel(n_sp, n_tp, queries, keys, values, doc_ids, *weights):
    w_gate = weights[4]
    depth, units = w_gate.shape
    aligned = depth % 128 == 0 and keys.shape[1] % 128 == 0 and units % TILE == 0
    return aligned and n_sp % 4 == 0 and n_tp > 1 and doc_ids.shape[0] % (n_tp * WINDOW) == 0


def solution(mesh):
    n_sp, n_tp = mesh.shape["sp"], mesh.shape["tp"]

    def body(*args):
        if in_one_kernel(n_sp, n_tp, *args):
            return whole_layer(n_sp, n_tp, *args)
        return per_device(*args)

    return jax.shard_map(
        body,
        mesh=mesh,
        in_specs=(
            P("sp", "tp"),
            P("sp", "tp"),
            P("sp", "tp"),
            P("sp"),
            P("tp"),
            P(("sp", "tp"), None),
            P("tp", None),
            P(),
            P("sp", "tp"),
            P("sp", "tp"),
            P(None, "tp"),
            P(None, "tp"),
            P("tp", "sp"),
        ),
        out_specs=P(("sp", "tp"), None),
        check_vma=False,
    )
```

```python
import functools

import jax
import jax.numpy as jnp
from jax import lax
from jax.experimental import pallas as pl
from jax.experimental.pallas import tpu as pltpu
from jax.sharding import PartitionSpec as P


HEAD_DIM = 64
WINDOW = 128
ROW_TILE = 128
SUB = 4
EARLY = 2
HALO = 16
TILE = 256
VMEM_BYTES = 67043328
MESH = pl.DeviceIdType.MESH


def shifted(shard, axis, by):
    size = lax.axis_size(axis)
    pairs = [(i, i + by) for i in range(size) if 0 <= i + by < size]
    return lax.ppermute(shard, axis, pairs)


def turned(t, axis, by):
    size = lax.axis_size(axis)
    return lax.ppermute(t, axis, [(i, (i + by) % size) for i in range(size)])


def core_swap(t):
    size = lax.axis_size("sp")
    return lax.ppermute(t, "sp", [(i, i ^ 1) for i in range(size)])


def parity_gather(t):
    size = lax.axis_size("sp")
    groups = [list(range(0, size, 2)), list(range(1, size, 2))]
    return lax.all_gather(t, "sp", axis=0, tiled=True, axis_index_groups=groups)


def ring_gather(t):
    chips = lax.axis_size("sp") // 2
    order = list(range(0, chips, 2)) + list(range(1, chips, 2))[::-1]
    chip = lax.axis_index("sp") // 2
    place = jnp.where(chip % 2 == 0, chip // 2, chips - 1 - chip // 2)

    def hop(piece, by):
        pairs = [
            (2 * order[k] + c, 2 * order[(k + by) % chips] + c)
            for k in range(chips)
            for c in range(2)
        ]
        return lax.ppermute(piece, "sp", pairs)

    def chip_at(k):
        k = (k + chips) % chips
        return jnp.where(k < chips // 2, 2 * k, 2 * (chips - 1 - k) + 1)

    depth = t.shape[0]
    pieces = [(chip, t)]
    up = down = t
    for step in range(1, chips // 2 + 1):
        up = hop(up, 1)
        pieces.append((chip_at(place - step), up))
        if step < chips - step:
            down = hop(down, -1)
            pieces.append((chip_at(place + step), down))
    whole = jnp.zeros((chips * depth,) + t.shape[1:], t.dtype)
    for at, piece in pieces:
        whole = lax.dynamic_update_slice_in_dim(whole, piece, at * depth, 0)
    return whole


def by_parity(t, depth):
    rows, width = t.shape
    blocks = width // depth
    tile = min(ROW_TILE, rows)

    def kernel(in_ref, out_ref):
        for j in range(blocks):
            to = (j // 2 + (j % 2) * (blocks // 2)) * depth
            out_ref[:, to : to + depth] = in_ref[:, j * depth : (j + 1) * depth]

    return pl.pallas_call(
        kernel,
        out_shape=jax.ShapeDtypeStruct(t.shape, t.dtype),
        grid=(rows // tile,),
        in_specs=[pl.BlockSpec((tile, width), lambda i: (i, 0))],
        out_specs=pl.BlockSpec((tile, width), lambda i: (i, 0)),
        cost_estimate=pl.CostEstimate(
            flops=0, bytes_accessed=2 * t.size * t.dtype.itemsize, transcendentals=0
        ),
    )(t)


def finish(mid, sums, depth):
    rows, width = mid.shape
    blocks = width // depth
    tile = min(ROW_TILE, rows)

    def kernel(mid_ref, even_ref, odd_ref, out_ref):
        for j in range(blocks):
            at = (j // 2) * depth
            held = at + (j % 2) * (width // 2)
            sum_ref = odd_ref if j % 2 else even_ref
            out_ref[:, j * depth : (j + 1) * depth] = (
                mid_ref[:, held : held + depth].astype(jnp.float32)
                + sum_ref[:, at : at + depth]
            ).astype(out_ref.dtype)

    half_spec = pl.BlockSpec((tile, width // 2), lambda i: (i, 0))
    return pl.pallas_call(
        kernel,
        out_shape=jax.ShapeDtypeStruct(mid.shape, mid.dtype),
        grid=(rows // tile,),
        in_specs=[pl.BlockSpec((tile, width), lambda i: (i, 0)), half_spec, half_spec],
        out_specs=pl.BlockSpec((tile, width), lambda i: (i, 0)),
        cost_estimate=pl.CostEstimate(
            flops=mid.size, bytes_accessed=8 * mid.size, transcendentals=0
        ),
    )(mid, *sums)


def attend(query_rows, key_ext, value_ext, doc_rows, doc_ext, sinks):
    row_count = query_rows.shape[0]
    block_count = row_count // WINDOW
    kv_heads = key_ext.shape[1] // HEAD_DIM
    group_size = query_rows.shape[1] // (kv_heads * HEAD_DIM)

    def band(t):
        lower = t[:row_count].reshape((block_count, WINDOW) + t.shape[1:])
        upper = t[WINDOW:].reshape((block_count, WINDOW) + t.shape[1:])
        return jnp.concatenate([lower, upper], axis=1)

    query_band = query_rows.reshape(block_count, WINDOW, kv_heads, group_size, HEAD_DIM)
    key_band = band(key_ext).reshape(block_count, 2 * WINDOW, kv_heads, HEAD_DIM)
    value_band = band(value_ext).reshape(block_count, 2 * WINDOW, kv_heads, HEAD_DIM)
    doc_band = band(doc_ext)
    distance = jnp.arange(WINDOW)[:, None] + WINDOW - jnp.arange(2 * WINDOW)[None, :]
    in_window = (distance >= 0) & (distance < WINDOW)
    same_doc = doc_rows.reshape(block_count, WINDOW)[:, :, None] == doc_band[:, None, :]
    keep_mask = in_window[None] & same_doc
    scores = jnp.einsum(
        "nqhgd,nkhd->nhgqk", query_band, key_band, preferred_element_type=jnp.float32
    ) * HEAD_DIM ** (-0.5)
    scores = jnp.where(keep_mask[:, None, None], scores, -jnp.inf)
    sink_logit = sinks.reshape(kv_heads, group_size)[None, :, :, None, None]
    peak = jnp.maximum(jnp.max(scores, axis=-1, keepdims=True), sink_logit)
    expd = jnp.exp(scores - peak)
    probs = (expd / (jnp.sum(expd, axis=-1, keepdims=True) + jnp.exp(sink_logit - peak))).astype(
        jnp.bfloat16
    )
    mixed = jnp.einsum("nhgqk,nkhd->nqhgd", probs, value_band, preferred_element_type=jnp.float32)
    return mixed.astype(jnp.bfloat16).reshape(row_count, -1)


def convolve(ext_rows, doc_ext, taps):
    center = doc_ext[2:]
    same_one = (doc_ext[1:-1] == center)[:, None]
    same_two = (doc_ext[:-2] == center)[:, None]
    ext32 = ext_rows.astype(jnp.float32)
    result = taps[2] * ext32[2:]
    result = result + jnp.where(same_one, taps[1] * ext32[1:-1], 0.0)
    return result + jnp.where(same_two, taps[0] * ext32[:-2], 0.0)


def per_device(
    queries,
    keys,
    values,
    doc_ids,
    sinks,
    residual,
    out_weight,
    norm_gain,
    w_gate,
    w_value,
    conv_gate,
    conv_value,
    w_down,
):
    core = lax.axis_index("sp") % 2
    tp = lax.axis_index("tp")
    n_tp = lax.axis_size("tp")
    rows = doc_ids.shape[0]
    part_rows = rows // n_tp
    depth = w_gate.shape[0]
    width = residual.shape[1]
    half = width // 2
    part_index = [(tp + n_tp - d) % n_tp for d in range(n_tp)]

    gate_own = parity_gather(w_gate)
    value_own = ring_gather(w_value)
    down_t = w_down.T
    inner = down_t.shape[1] // 2
    low, high = down_t[:, :inner], down_t[:, inner:]
    kept_half = jnp.where(core == 0, low, high)
    came_half = core_swap(jnp.where(core == 0, high, low))
    even_piece = jnp.where(core == 0, kept_half, came_half)
    odd_piece = jnp.where(core == 0, came_half, kept_half)
    down_odd = parity_gather(odd_piece)
    down_even = parity_gather(even_piece)
    gate_far = core_swap(gate_own)
    value_far = core_swap(value_own)

    out_far = [turned(out_weight, "tp", d) for d in range(1, n_tp)]
    out_parts = [by_parity(t, depth) for t in [out_weight] + out_far]
    residual = by_parity(residual, depth)
    norm_gain = norm_gain.reshape(-1, 2, depth).swapaxes(0, 1).reshape(-1)
    docs_plus = doc_ids + 1
    prev_keys, prev_values, prev_docs = shifted(
        (keys[-WINDOW:], values[-WINDOW:], docs_plus[-WINDOW:]), "sp", 1
    )
    key_ext = jnp.concatenate([prev_keys, keys], axis=0)
    value_ext = jnp.concatenate([prev_values, values], axis=0)
    doc_ext = jnp.concatenate([prev_docs, docs_plus], axis=0)
    head_out = attend(queries, key_ext, value_ext, docs_plus, doc_ext, sinks)

    def rows_of(t, index):
        return lax.dynamic_slice_in_dim(t, index * part_rows, part_rows, 0)

    proj = jnp.dot(rows_of(head_out, tp), out_parts[0], preferred_element_type=jnp.float32)
    for d in range(1, n_tp):
        heads_far = turned(rows_of(head_out, (tp + d) % n_tp), "tp", d)
        proj = proj + jnp.dot(heads_far, out_parts[d], preferred_element_type=jnp.float32)
    mid = (residual.astype(jnp.float32) + proj).astype(jnp.bfloat16)
    mid32 = mid.astype(jnp.float32)
    normed = (
        mid32 * lax.rsqrt(jnp.mean(mid32 * mid32, axis=-1, keepdims=True) + 1e-06) * norm_gain
    ).astype(jnp.bfloat16)
    even, odd = normed[:, :half], normed[:, half:]
    own = [jnp.where(core == 0, even, odd)]
    far = [jnp.where(core == 0, odd, even)]
    for d in range(1, n_tp):
        own.append(turned(own[0], "tp", d))
        far.append(turned(far[0], "tp", d))

    def up(own, far, w_own, w_far):
        total = jnp.dot(own, w_own, preferred_element_type=jnp.float32)
        return (total + jnp.dot(far, w_far, preferred_element_type=jnp.float32)).astype(
            jnp.bfloat16
        )

    gate_parts = [up(o, f, gate_own, gate_far) for o, f in zip(own, far)]
    value_parts = [up(o, f, value_own, value_far) for o, f in zip(own, far)]

    conv_docs = jnp.concatenate([prev_docs[-2:], docs_plus], axis=0)
    part_docs = [
        lax.dynamic_slice_in_dim(conv_docs, i * part_rows, part_rows + 2, 0) for i in part_index
    ]

    def conv_parts(parts, taps):
        tails = [p[-2:] for p in parts]
        last = tails[0]
        for d in range(1, n_tp):
            last = jnp.where(part_index[d] == n_tp - 1, tails[d], last)
        prev = shifted(last, "sp", 1)
        result = []
        for d in range(n_tp):
            halo = jnp.where(part_index[d] == 0, prev, tails[(d + 1) % n_tp])
            result.append(
                convolve(jnp.concatenate([halo, parts[d]], axis=0), part_docs[d], taps)
            )
        return result

    gate_conv = conv_parts(gate_parts, conv_gate)
    value_conv = conv_parts(value_parts, conv_value)
    hidden = [
        (jax.nn.silu(g) * v).astype(jnp.bfloat16) for g, v in zip(gate_conv, value_conv)
    ]

    def down(units, w_t):
        return lax.dot_general(
            units, w_t, (((1,), (1,)), ((), ())), preferred_element_type=jnp.float32
        )

    own_units = [jnp.where(core == 0, h[:, :inner], h[:, inner:]) for h in hidden]
    far_units = [jnp.where(core == 0, h[:, inner:], h[:, :inner]) for h in hidden]

    def down_sums(w_own):
        w_far = core_swap(w_own)
        came = []
        for d in range(1, n_tp):
            sent = (down(own_units[d], w_own) + down(far_units[d], w_far)).astype(
                jnp.bfloat16
            )
            came.append(turned(sent, "tp", -d))
        kept = down(own_units[0], w_own) + down(far_units[0], w_far)
        for t in came:
            kept = kept + t.astype(jnp.float32)
        return kept

    odd_sum = down_sums(down_odd)
    even_sum = down_sums(down_even)
    sums = (even_sum, odd_sum)
    return finish(mid, sums, depth)


def mult(x, m):
    return x if isinstance(x, int) else pl.multiple_of(x, m)


def ring_chip(place, chips):
    odd = lax.div(place, chips // 2)
    return (1 - odd) * (2 * place) + odd * (2 * (chips - 1 - place) + 1)


def layer_kernel(
    n_sp,
    n_tp,
    queries,
    keys,
    values,
    docs,
    sinks,
    residual,
    out_weight,
    norm_gain,
    w_gate,
    w_value,
    conv_gate,
    conv_value,
    w_down,
    out,
    wg,
    wv,
    wd,
    nrm,
    hid,
    pre,
    q_v,
    k_v,
    v_v,
    doc_v,
    doc_col,
    same_one,
    same_two,
    att,
    heads,
    ow,
    mid,
    gain_v,
    cg_v,
    cv_v,
    send,
    came,
    own,
    local_sem,
    ring_send,
    ring_recv,
    sib_send,
    sib_recv,
    halo_send,
    halo_recv,
    ow_send,
    ow_recv,
    heads_send,
    heads_recv,
    nrm_send,
    nrm_recv,
    sum_send,
    sum_recv,
    out_sem,
):
    sp = lax.axis_index("sp")
    tp = lax.axis_index("tp")
    chips = n_sp // 2
    core = lax.rem(sp, 2)
    chip = lax.div(sp, 2)
    odd = lax.rem(chip, 2)
    place = (1 - odd) * lax.div(chip, 2) + odd * (chips - 1 - lax.div(chip, 2))
    way = 1 - 2 * core
    down_sp = 2 * ring_chip(lax.rem(place + way + chips, chips), chips) + core
    up_sp = 2 * ring_chip(lax.rem(place - way + chips, chips), chips) + core
    sib_sp = sp + way
    next_sp = lax.rem(sp + 1, n_sp)
    prev_sp = lax.rem(sp + n_sp - 1, n_sp)

    rows, q_width = queries.shape
    part = rows // n_tp
    depth, units = w_gate.shape
    kv_heads = keys.shape[1] // HEAD_DIM
    group = q_width // keys.shape[1]
    blocks = rows // WINDOW
    part_blocks = part // WINDOW
    ow_half = q_width // 2
    unit_tiles = units // TILE
    events = (chips - 1) * SUB

    def peer(d):
        return lax.rem(tp + d, n_tp)

    def held(h):
        return 2 * ring_chip(lax.rem(place - way * h + chips, chips), chips) + core

    def sib_held(h):
        return 2 * ring_chip(lax.rem(place + way * h + chips, chips), chips) + 1 - core

    def piece(w, j, s):
        if w == 2:
            size = units // SUB
            return wd.at[j, pl.ds(mult(s * size, size), size), :]
        size = depth // SUB
        buf = (wg, wv)[w]
        return buf.at[pl.ds(mult(j * depth + s * size, size), size), :]

    def own_piece(w, s):
        ref = (w_gate, w_value, w_down)[w]
        size = ref.shape[0] // SUB
        return ref.at[pl.ds(s * size, size), :]

    def remote(src, dst, send_sem, recv_sem, device):
        return pltpu.make_async_remote_copy(
            src_ref=src,
            dst_ref=dst,
            send_sem=send_sem,
            recv_sem=recv_sem,
            device_id=device,
            device_id_type=MESH,
        )

    def ring_copy(w, h, s, src=None):
        dst = piece(w, held(h - 1), s)
        return remote(
            dst if src is None else src,
            dst,
            ring_send.at[w, h, s],
            ring_recv.at[w, h, s],
            (down_sp, tp),
        )

    def ring_wait(w, h, s):
        dst = piece(w, held(h), s)
        remote(
            dst, dst, ring_send.at[w, h, s], ring_recv.at[w, h, s], (down_sp, tp)
        ).wait_recv()

    def sib_copy(w, h, s, src=None):
        dst = piece(w, held(h), s)
        return remote(
            dst if src is None else src,
            dst,
            sib_send.at[w, h, s],
            sib_recv.at[w, h, s],
            (sib_sp, tp),
        )

    def sib_wait(w, h, s):
        dst = piece(w, sib_held(h), s)
        remote(
            dst, dst, sib_send.at[w, h, s], sib_recv.at[w, h, s], (sib_sp, tp)
        ).wait_recv()

    def start_own(w):
        for s in range(SUB):
            ring_copy(w, 1, s, own_piece(w, s)).start()
        for s in range(SUB):
            sib_copy(w, 0, s, own_piece(w, s)).start()

    def service(w, e):
        h = 1 + (e // SUB if isinstance(e, int) else lax.div(e, SUB))
        s = e % SUB if isinstance(e, int) else lax.rem(e, SUB)
        ring_wait(w, h, s)
        if isinstance(e, int):
            if h < chips - 1:
                ring_copy(w, h + 1, s).start()
        else:

            @pl.when(h < chips - 1)
            def _():
                ring_copy(w, h + 1, s).start()

        sib_copy(w, h, s).start()
        if w < 2:

            @pl.when(e == (chips - 2) * SUB - 1)
            def _():
                start_own(w + 1)

    def serve(w, first, last):
        if last > first:

            @pl.loop(first, last)
            def _(e):
                service(w, e)

    local = [
        (keys, k_v.at[pl.ds(WINDOW, rows), :]),
        (values, v_v.at[pl.ds(WINDOW, rows), :]),
        (docs, doc_v.at[pl.ds(8, blocks), :]),
        (queries, q_v),
        (residual, mid),
        (out_weight, ow.at[tp]),
        (norm_gain, gain_v),
        (conv_gate, cg_v),
        (conv_value, cv_v),
        (w_gate, wg.at[pl.ds(mult(sp * depth, depth), depth), :]),
        (w_value, wv.at[pl.ds(mult(sp * depth, depth), depth), :]),
        (w_down, wd.at[sp]),
    ]
    local = [
        pltpu.make_async_copy(src, dst, local_sem.at[i]) for i, (src, dst) in enumerate(local)
    ]
    for copy in local[:4]:
        copy.start()

    barrier = pltpu.get_barrier_semaphore()
    greeted = [(down_sp, tp), (up_sp, tp), (sib_sp, tp), (next_sp, tp), (prev_sp, tp)]
    greeted += [(sp, peer(d)) for d in range(1, n_tp)]
    for device in greeted:
        pl.semaphore_signal(barrier, inc=1, device_id=device, device_id_type=MESH)
    pl.semaphore_wait(barrier, len(greeted))

    halos = [
        (keys.at[pl.ds(rows - WINDOW, WINDOW), :], k_v.at[pl.ds(0, WINDOW), :]),
        (values.at[pl.ds(rows - WINDOW, WINDOW), :], v_v.at[pl.ds(0, WINDOW), :]),
        (docs.at[pl.ds(blocks - 1, 1), :], doc_v.at[pl.ds(7, 1), :]),
    ]
    halos = [
        remote(src, dst, halo_send.at[i], halo_recv.at[i], (next_sp, tp))
        for i, (src, dst) in enumerate(halos)
    ]
    for copy in halos:
        copy.start()
    start_own(0)

    def ow_rows(t, c):
        return ow.at[t, pl.ds(mult(c * ow_half, ow_half), ow_half), :]

    ow_src = out_weight.at[pl.ds(mult(core * ow_half, ow_half), ow_half), :]
    ow_out = [
        remote(ow_src, ow_rows(tp, core), ow_send.at[0, d], ow_recv.at[0, d], (sp, peer(n_tp - d)))
        for d in range(1, n_tp)
    ]
    for copy in ow_out:
        copy.start()
    for copy in local[4:]:
        copy.start()

    for i in range(3):
        local[i].wait()
    for copy in halos:
        copy.wait_recv()
    local[3].wait()

    lane = lax.broadcasted_iota(jnp.int32, (WINDOW, 2 * HEAD_DIM), 1)
    low_lane = lane < HEAD_DIM
    doc_v[7:8, :] = jnp.where(sp == 0, -1, doc_v[7:8, :])
    for b in range(-1, blocks):
        row = doc_v[8 + b : 9 + b, :]
        column = jnp.broadcast_to(row, (WINDOW, WINDOW)).T
        if b < 0:
            doc_col[0:8, :] = column[WINDOW - 8 :, :]
        else:
            doc_col[8 + b * WINDOW : 8 + (b + 1) * WINDOW, :] = column
    for b in range(blocks):
        at = 8 + b * WINDOW
        here = doc_col[at : at + WINDOW, :]
        back_one = doc_col[at - 1 : at - 1 + WINDOW, :]
        back_two = doc_col[at - 2 : at - 2 + WINDOW, :]
        to = slice(b * WINDOW, (b + 1) * WINDOW)
        same_one[to, :] = jnp.where(here == back_one, 1.0, 0.0)
        same_two[to, :] = jnp.where(here == back_two, 1.0, 0.0)

    q_index = lax.broadcasted_iota(jnp.int32, (WINDOW, 2 * WINDOW), 0)
    k_index = lax.broadcasted_iota(jnp.int32, (WINDOW, 2 * WINDOW), 1)
    first_rows = lax.broadcasted_iota(jnp.int32, (2 * WINDOW, 1), 0) < WINDOW

    def attend_block(b):
        base = mult(b * WINDOW, WINDOW)
        key_docs = jnp.concatenate([doc_v[pl.ds(7 + b, 1), :], doc_v[pl.ds(8 + b, 1), :]], axis=1)
        here = doc_col[pl.ds(mult(8 + base, 8), WINDOW), :]
        keep = (k_index > q_index) & (k_index <= q_index + WINDOW)
        keep = keep & (jnp.concatenate([here, here], axis=1) == key_docs)
        keep = jnp.concatenate([keep, keep], axis=0)
        k_band = k_v[pl.ds(base, 2 * WINDOW), :]
        v_band = v_v[pl.ds(base, 2 * WINDOW), :]
        for g in range(kv_heads):
            at = slice(g * HEAD_DIM, (g + 1) * HEAD_DIM)
            kk = jnp.concatenate([k_band[:, at], k_band[:, at]], axis=1)
            vv = jnp.concatenate([v_band[:, at], v_band[:, at]], axis=1)
            for pair in range(group // 2):
                head = g * group + 2 * pair
                lanes = slice(head * HEAD_DIM, (head + 2) * HEAD_DIM)
                both = q_v[pl.ds(base, WINDOW), lanes]
                zero = jnp.zeros_like(both)
                split = jnp.concatenate(
                    [jnp.where(low_lane, both, zero), jnp.where(low_lane, zero, both)], axis=0
                )
                scores = lax.dot_general(
                    split, kk, (((1,), (1,)), ((), ())), preferred_element_type=jnp.float32
                ) * HEAD_DIM ** (-0.5)
                scores = jnp.where(keep, scores, -1e30)
                sink = jnp.where(first_rows, sinks[head], sinks[head + 1])
                peak = jnp.maximum(jnp.max(scores, axis=1, keepdims=True), sink)
                expd = jnp.exp(scores - peak)
                total = jnp.sum(expd, axis=1, keepdims=True) + jnp.exp(sink - peak)
                probs = (expd * (1.0 / total)).astype(jnp.bfloat16)
                mixed = jnp.dot(probs, vv, preferred_element_type=jnp.float32)
                att[pl.ds(base, WINDOW), lanes] = jnp.where(
                    low_lane, mixed[:WINDOW], mixed[WINDOW:]
                ).astype(jnp.bfloat16)

    def due(share):
        return events * share // 28

    pl.loop(0, blocks - part_blocks)(
        lambda i: attend_block(lax.rem((tp + 1) * part_blocks + i, blocks))
    )
    serve(0, 0, due(3))
    pl.loop(0, part_blocks)(lambda i: attend_block(tp * part_blocks + i))
    heads_out = [
        remote(
            att.at[pl.ds(mult(peer(n_tp - d) * part, part), part), :],
            heads.at[d - 1],
            heads_send.at[d],
            heads_recv.at[d],
            (sp, peer(n_tp - d)),
        )
        for d in range(1, n_tp)
    ]
    for copy in heads_out:
        copy.start()
    before_proj = due(14)
    serve(0, due(3), before_proj)

    for i in range(4, 9):
        local[i].wait()
    ow_on = []
    for d in range(1, n_tp):
        got = ow_rows(peer(d), core)
        remote(got, got, ow_send.at[0, d], ow_recv.at[0, d], (sp, peer(n_tp - d))).wait_recv()
        copy = remote(got, got, ow_send.at[1, d], ow_recv.at[1, d], (sib_sp, tp))
        copy.start()
        ow_on.append(copy)
    for d in range(1, n_tp):
        got = ow_rows(peer(d), 1 - core)
        remote(got, got, ow_send.at[1, d], ow_recv.at[1, d], (sib_sp, tp)).wait_recv()
        heads_out[d - 1].wait_recv()

    part_base = tp * part

    def nrm_rows(t, i):
        return nrm.at[pl.ds(mult(HALO + t * part + i * WINDOW, HALO), WINDOW), :]

    def nrm_copy(i, d):
        at = nrm_rows(tp, i)
        return remote(at, at, nrm_send.at[i, d], nrm_recv.at[i, d], (sp, peer(n_tp - d)))

    def project(i):
        at = pl.ds(mult(i * WINDOW, WINDOW), WINDOW)
        mine = att[pl.ds(mult(part_base + i * WINDOW, WINDOW), WINDOW), :]
        proj = jnp.dot(mine, ow[tp], preferred_element_type=jnp.float32)
        for d in range(1, n_tp):
            proj = proj + jnp.dot(
                heads[d - 1, at, :], ow[peer(d)], preferred_element_type=jnp.float32
            )
        rounded = (mid[at, :].astype(jnp.float32) + proj).astype(jnp.bfloat16)
        mid[at, :] = rounded
        wide = rounded.astype(jnp.float32)
        scale = lax.rsqrt(jnp.mean(wide * wide, axis=1, keepdims=True) + 1e-06)
        normed = (wide * scale * gain_v[...]).astype(jnp.bfloat16)
        nrm[pl.ds(mult(HALO + part_base + i * WINDOW, HALO), WINDOW), :] = normed

    @pl.loop(0, part_blocks)
    def _(i):
        project(i)
        for d in range(1, n_tp):

            @pl.when(i > 0)
            def _():
                nrm_copy(i - 1, d).start()

        @pl.when(before_proj + i < events)
        def _():
            service(0, before_proj + i)

    for d in range(1, n_tp):
        nrm_copy(part_blocks - 1, d).start()

    after_proj = min(events, before_proj + part_blocks)
    serve(0, after_proj, events)
    early_value = due(14)
    serve(1, 0, early_value)

    @pl.loop(0, part_blocks)
    def _(i):
        for d in range(1, n_tp):
            got = nrm_rows(peer(d), i)
            remote(
                got, got, nrm_send.at[i, d], nrm_recv.at[i, d], (sp, peer(n_tp - d))
            ).wait_recv()

    nrm_halo = remote(
        nrm.at[pl.ds(rows, HALO), :],
        nrm.at[pl.ds(0, HALO), :],
        halo_send.at[3],
        halo_recv.at[3],
        (next_sp, tp),
    )
    nrm_halo.start()
    for i in range(9, 12):
        local[i].wait()

    def all_of_sib(w):
        @pl.loop(0, chips * SUB)
        def _(e):
            sib_wait(w, lax.div(e, SUB), lax.rem(e, SUB))

    all_of_sib(0)
    nrm_halo.wait_recv()

    def up_tile(w_ref, taps, n, base, lengths):
        cols = pl.ds(mult(n * TILE, TILE), TILE)
        at = 0
        for length in lengths:
            lhs = nrm[pl.ds(mult(base + at, HALO), length), :]
            pre[at : at + length, :] = (
                jnp.dot(lhs, w_ref[:, cols], preferred_element_type=jnp.float32)
                .astype(jnp.bfloat16)
                .astype(jnp.float32)
            )
            at += length
        tap = taps[:, cols]
        for b in range((at - HALO) // WINDOW):
            at = HALO + b * WINDOW
            to = pl.ds(mult(base + b * WINDOW, WINDOW), WINDOW)
            one = jnp.concatenate([same_one[to, :]] * (TILE // WINDOW), axis=1)
            two = jnp.concatenate([same_two[to, :]] * (TILE // WINDOW), axis=1)
            conv = tap[2:3] * pre[at : at + WINDOW, :]
            conv = conv + one * (tap[1:2] * pre[at - 1 : at - 1 + WINDOW, :])
            conv = conv + two * (tap[0:1] * pre[at - 2 : at - 2 + WINDOW, :])
            yield to, cols, conv

    def spread(w, first, count, i):
        before = lax.div(i * count, unit_tiles)
        after = lax.div((i + 1) * count, unit_tiles)

        @pl.when(after > before)
        def _():
            service(w, first + before)

    gate_count = min(unit_tiles, events - early_value)

    @pl.loop(0, unit_tiles)
    def _(n):
        lengths = (HALO + rows // 2, rows // 2)
        for to, cols, conv in up_tile(wg, cg_v, n, 0, lengths):
            hid[to, cols] = (conv / (1.0 + jnp.exp(-conv))).astype(jnp.bfloat16)
        spread(1, early_value, gate_count, n)

    serve(1, early_value + gate_count, events)
    all_of_sib(1)

    def value_part(t, first, count):
        @pl.loop(0, unit_tiles)
        def _(n):
            for to, cols, conv in up_tile(wv, cv_v, n, t * part, (HALO + part,)):
                hid[to, cols] = (hid[to, cols].astype(jnp.float32) * conv).astype(
                    jnp.bfloat16
                )
            spread(2, first, count, n)

    def sum_copy(h, d):
        return remote(
            send.at[h, d - 1],
            came.at[h, d - 1],
            sum_send.at[h, d],
            sum_recv.at[h, d],
            (sp, peer(d)),
        )

    def hop_cols(h, c):
        j = held(h) if c == 0 else sib_held(h)
        return pl.ds(mult(j * depth, depth), depth)

    def out_copy(h, c):
        cols = hop_cols(h, c)
        return pltpu.make_async_copy(mid.at[:, cols], out.at[:, cols], out_sem.at[h, c])

    def finish_hop(h):
        for d in range(1, n_tp):
            got = came.at[h, d - 1]
            remote(
                got, got, sum_send.at[h, d], sum_recv.at[h, d], (sp, peer(d))
            ).wait_recv()
        for c in range(2):
            cols = hop_cols(h, c)
            from_cols = slice(c * depth, (c + 1) * depth)
            total = own[h, :, from_cols] + mid[:, cols].astype(jnp.float32)
            for d in range(1, n_tp):
                total = total + came[h, d - 1, :, from_cols].astype(jnp.float32)
            mid[:, cols] = total.astype(jnp.bfloat16)
        for c in range(2):
            out_copy(h, c).start()

    def down_rows(h, t):
        lhs = hid[pl.ds(mult(t * part, part), part), :]
        rhs = jnp.concatenate([wd[held(h)], wd[sib_held(h)]], axis=1)
        return jnp.dot(lhs, rhs, preferred_element_type=jnp.float32)

    def down_far(h):
        for s in range(SUB):
            sib_wait(2, h, s)
        for d in range(1, n_tp):
            send[h, d - 1] = down_rows(h, peer(d)).astype(jnp.bfloat16)

    def send_sums(h):
        for d in range(1, n_tp):
            sum_copy(h, d).start()

    served = SUB
    for d in range(1, n_tp):
        value_part(peer(d), 0, served if d == 1 else 0)
    for h in range(EARLY):
        down_far(h)
        if h > 0:
            send_sums(h - 1)
    more = due(6)
    value_part(tp, served, more)
    send_sums(EARLY - 1)
    served += more

    @pl.loop(EARLY, chips + EARLY)
    def _(h):
        @pl.when(h < chips)
        def _():
            for s in range(SUB):

                @pl.when((h - 1) * SUB + s >= served)
                def _():
                    service(2, (h - 1) * SUB + s)

            down_far(h)

        own[h - EARLY] = down_rows(h - EARLY, tp)

        @pl.when(h < chips)
        def _():
            send_sums(h)

        @pl.when(h > EARLY)
        def _():
            finish_hop(h - EARLY - 1)

    finish_hop(chips - 1)

    for copy in halos + heads_out + ow_out + ow_on + [nrm_halo]:
        copy.wait_send()

    @pl.loop(0, part_blocks)
    def _(i):
        for d in range(1, n_tp):
            nrm_copy(i, d).wait_send()

    for w in range(3):

        @pl.loop(0, chips)
        def _(h):
            for s in range(SUB):

                @pl.when(h > 0)
                def _():
                    ring_copy(w, h, s).wait_send()

                sib_copy(w, h, s).wait_send()

    @pl.loop(0, chips)
    def _(h):
        for d in range(1, n_tp):
            sum_copy(h, d).wait_send()
        for c in range(2):
            out_copy(h, c).wait()


def whole_layer(n_sp, n_tp, queries, keys, values, doc_ids, sinks, residual, out_weight,
                norm_gain, w_gate, w_value, conv_gate, conv_value, w_down):
    rows, q_width = queries.shape
    kv_width = keys.shape[1]
    part, width = residual.shape
    depth, units = w_gate.shape
    chips = n_sp // 2
    bf16, f32 = jnp.bfloat16, jnp.float32
    dma = pltpu.SemaphoreType.DMA
    part_blocks = part // WINDOW
    scratch = [
        pltpu.VMEM((width, units), bf16),
        pltpu.VMEM((width, units), bf16),
        pltpu.VMEM((n_sp, units, depth), bf16),
        pltpu.VMEM((HALO + rows, width), bf16),
        pltpu.VMEM((rows, units), bf16),
        pltpu.VMEM((HALO + rows, TILE), f32),
        pltpu.VMEM((rows, q_width), bf16),
        pltpu.VMEM((WINDOW + rows, kv_width), bf16),
        pltpu.VMEM((WINDOW + rows, kv_width), bf16),
        pltpu.VMEM((8 + rows // WINDOW, WINDOW), jnp.int32),
        pltpu.VMEM((8 + rows, WINDOW), jnp.int32),
        pltpu.VMEM((rows, WINDOW), f32),
        pltpu.VMEM((rows, WINDOW), f32),
        pltpu.VMEM((rows, q_width), bf16),
        pltpu.VMEM((n_tp - 1, part, q_width), bf16),
        pltpu.VMEM((n_tp, q_width, width), bf16),
        pltpu.VMEM((part, width), bf16),
        pltpu.VMEM((1, width), f32),
        pltpu.VMEM((3, units), f32),
        pltpu.VMEM((3, units), f32),
        pltpu.VMEM((chips, n_tp - 1, part, 2 * depth), bf16),
        pltpu.VMEM((chips, n_tp - 1, part, 2 * depth), bf16),
        pltpu.VMEM((chips, part, 2 * depth), f32),
        dma((12,)),
        dma((3, chips, SUB)),
        dma((3, chips, SUB)),
        dma((3, chips, SUB)),
        dma((3, chips, SUB)),
        dma((4,)),
        dma((4,)),
        dma((2, n_tp)),
        dma((2, n_tp)),
        dma((n_tp,)),
        dma((n_tp,)),
        dma((part_blocks, n_tp)),
        dma((part_blocks, n_tp)),
        dma((chips, n_tp)),
        dma((chips, n_tp)),
        dma((chips, 2)),
    ]
    any_spec = pl.BlockSpec(memory_space=pl.ANY)
    specs = [any_spec] * 13
    specs[4] = pl.BlockSpec(memory_space=pltpu.SMEM)
    return pl.pallas_call(
        functools.partial(layer_kernel, n_sp, n_tp),
        out_shape=jax.ShapeDtypeStruct(residual.shape, residual.dtype),
        in_specs=specs,
        out_specs=any_spec,
        scratch_shapes=scratch,
        compiler_params=pltpu.CompilerParams(
            collective_id=0, has_side_effects=True, vmem_limit_bytes=VMEM_BYTES
        ),
    )(
        queries,
        keys,
        values,
        doc_ids.reshape(rows // WINDOW, WINDOW),
        sinks,
        residual,
        out_weight,
        norm_gain.reshape(1, width),
        w_gate,
        w_value,
        conv_gate,
        conv_value,
        w_down,
    )


def in_one_kernel(n_sp, n_tp, queries, keys, values, doc_ids, *weights):
    w_gate = weights[4]
    depth, units = w_gate.shape
    aligned = depth % 128 == 0 and keys.shape[1] % 128 == 0 and units % TILE == 0
    return aligned and n_sp % 4 == 0 and n_tp > 1 and doc_ids.shape[0] % (n_tp * WINDOW) == 0


def solution(mesh):
    n_sp, n_tp = mesh.shape["sp"], mesh.shape["tp"]

    def body(*args):
        if in_one_kernel(n_sp, n_tp, *args):
            return whole_layer(n_sp, n_tp, *args)
        return per_device(*args)

    return jax.shard_map(
        body,
        mesh=mesh,
        in_specs=(
            P("sp", "tp"),
            P("sp", "tp"),
            P("sp", "tp"),
            P("sp"),
            P("tp"),
            P(("sp", "tp"), None),
            P("tp", None),
            P(),
            P("sp", "tp"),
            P("sp", "tp"),
            P(None, "tp"),
            P(None, "tp"),
            P("tp", "sp"),
        ),
        out_specs=P(("sp", "tp"), None),
        check_vma=False,
    )
```

```python
import functools

import jax
import jax.numpy as jnp
from jax import lax
from jax.experimental import pallas as pl
from jax.experimental.pallas import tpu as pltpu
from jax.sharding import PartitionSpec as P


HEAD_DIM = 64
WINDOW = 128
ROW_TILE = 128
SUB = 4
EARLY = 2
HALO = 16
TILE = 256
VMEM_BYTES = 64800000
MESH = pl.DeviceIdType.MESH


def shifted(shard, axis, by):
    size = lax.axis_size(axis)
    pairs = [(i, i + by) for i in range(size) if 0 <= i + by < size]
    return lax.ppermute(shard, axis, pairs)


def turned(t, axis, by):
    size = lax.axis_size(axis)
    return lax.ppermute(t, axis, [(i, (i + by) % size) for i in range(size)])


def core_swap(t):
    size = lax.axis_size("sp")
    return lax.ppermute(t, "sp", [(i, i ^ 1) for i in range(size)])


def parity_gather(t):
    size = lax.axis_size("sp")
    groups = [list(range(0, size, 2)), list(range(1, size, 2))]
    return lax.all_gather(t, "sp", axis=0, tiled=True, axis_index_groups=groups)


def ring_gather(t):
    chips = lax.axis_size("sp") // 2
    order = list(range(0, chips, 2)) + list(range(1, chips, 2))[::-1]
    chip = lax.axis_index("sp") // 2
    place = jnp.where(chip % 2 == 0, chip // 2, chips - 1 - chip // 2)

    def hop(piece, by):
        pairs = [
            (2 * order[k] + c, 2 * order[(k + by) % chips] + c)
            for k in range(chips)
            for c in range(2)
        ]
        return lax.ppermute(piece, "sp", pairs)

    def chip_at(k):
        k = (k + chips) % chips
        return jnp.where(k < chips // 2, 2 * k, 2 * (chips - 1 - k) + 1)

    depth = t.shape[0]
    pieces = [(chip, t)]
    up = down = t
    for step in range(1, chips // 2 + 1):
        up = hop(up, 1)
        pieces.append((chip_at(place - step), up))
        if step < chips - step:
            down = hop(down, -1)
            pieces.append((chip_at(place + step), down))
    whole = jnp.zeros((chips * depth,) + t.shape[1:], t.dtype)
    for at, piece in pieces:
        whole = lax.dynamic_update_slice_in_dim(whole, piece, at * depth, 0)
    return whole


def by_parity(t, depth):
    rows, width = t.shape
    blocks = width // depth
    tile = min(ROW_TILE, rows)

    def kernel(in_ref, out_ref):
        for j in range(blocks):
            to = (j // 2 + (j % 2) * (blocks // 2)) * depth
            out_ref[:, to : to + depth] = in_ref[:, j * depth : (j + 1) * depth]

    return pl.pallas_call(
        kernel,
        out_shape=jax.ShapeDtypeStruct(t.shape, t.dtype),
        grid=(rows // tile,),
        in_specs=[pl.BlockSpec((tile, width), lambda i: (i, 0))],
        out_specs=pl.BlockSpec((tile, width), lambda i: (i, 0)),
        cost_estimate=pl.CostEstimate(
            flops=0, bytes_accessed=2 * t.size * t.dtype.itemsize, transcendentals=0
        ),
    )(t)


def finish(mid, sums, depth):
    rows, width = mid.shape
    blocks = width // depth
    tile = min(ROW_TILE, rows)

    def kernel(mid_ref, even_ref, odd_ref, out_ref):
        for j in range(blocks):
            at = (j // 2) * depth
            held = at + (j % 2) * (width // 2)
            sum_ref = odd_ref if j % 2 else even_ref
            out_ref[:, j * depth : (j + 1) * depth] = (
                mid_ref[:, held : held + depth].astype(jnp.float32)
                + sum_ref[:, at : at + depth]
            ).astype(out_ref.dtype)

    half_spec = pl.BlockSpec((tile, width // 2), lambda i: (i, 0))
    return pl.pallas_call(
        kernel,
        out_shape=jax.ShapeDtypeStruct(mid.shape, mid.dtype),
        grid=(rows // tile,),
        in_specs=[pl.BlockSpec((tile, width), lambda i: (i, 0)), half_spec, half_spec],
        out_specs=pl.BlockSpec((tile, width), lambda i: (i, 0)),
        cost_estimate=pl.CostEstimate(
            flops=mid.size, bytes_accessed=8 * mid.size, transcendentals=0
        ),
    )(mid, *sums)


def attend(query_rows, key_ext, value_ext, doc_rows, doc_ext, sinks):
    row_count = query_rows.shape[0]
    block_count = row_count // WINDOW
    kv_heads = key_ext.shape[1] // HEAD_DIM
    group_size = query_rows.shape[1] // (kv_heads * HEAD_DIM)

    def band(t):
        lower = t[:row_count].reshape((block_count, WINDOW) + t.shape[1:])
        upper = t[WINDOW:].reshape((block_count, WINDOW) + t.shape[1:])
        return jnp.concatenate([lower, upper], axis=1)

    query_band = query_rows.reshape(block_count, WINDOW, kv_heads, group_size, HEAD_DIM)
    key_band = band(key_ext).reshape(block_count, 2 * WINDOW, kv_heads, HEAD_DIM)
    value_band = band(value_ext).reshape(block_count, 2 * WINDOW, kv_heads, HEAD_DIM)
    doc_band = band(doc_ext)
    distance = jnp.arange(WINDOW)[:, None] + WINDOW - jnp.arange(2 * WINDOW)[None, :]
    in_window = (distance >= 0) & (distance < WINDOW)
    same_doc = doc_rows.reshape(block_count, WINDOW)[:, :, None] == doc_band[:, None, :]
    keep_mask = in_window[None] & same_doc
    scores = jnp.einsum(
        "nqhgd,nkhd->nhgqk", query_band, key_band, preferred_element_type=jnp.float32
    ) * HEAD_DIM ** (-0.5)
    scores = jnp.where(keep_mask[:, None, None], scores, -jnp.inf)
    sink_logit = sinks.reshape(kv_heads, group_size)[None, :, :, None, None]
    peak = jnp.maximum(jnp.max(scores, axis=-1, keepdims=True), sink_logit)
    expd = jnp.exp(scores - peak)
    probs = (expd / (jnp.sum(expd, axis=-1, keepdims=True) + jnp.exp(sink_logit - peak))).astype(
        jnp.bfloat16
    )
    mixed = jnp.einsum("nhgqk,nkhd->nqhgd", probs, value_band, preferred_element_type=jnp.float32)
    return mixed.astype(jnp.bfloat16).reshape(row_count, -1)


def convolve(ext_rows, doc_ext, taps):
    center = doc_ext[2:]
    same_one = (doc_ext[1:-1] == center)[:, None]
    same_two = (doc_ext[:-2] == center)[:, None]
    ext32 = ext_rows.astype(jnp.float32)
    result = taps[2] * ext32[2:]
    result = result + jnp.where(same_one, taps[1] * ext32[1:-1], 0.0)
    return result + jnp.where(same_two, taps[0] * ext32[:-2], 0.0)


def per_device(
    queries,
    keys,
    values,
    doc_ids,
    sinks,
    residual,
    out_weight,
    norm_gain,
    w_gate,
    w_value,
    conv_gate,
    conv_value,
    w_down,
):
    core = lax.axis_index("sp") % 2
    tp = lax.axis_index("tp")
    n_tp = lax.axis_size("tp")
    rows = doc_ids.shape[0]
    part_rows = rows // n_tp
    depth = w_gate.shape[0]
    width = residual.shape[1]
    half = width // 2
    part_index = [(tp + n_tp - d) % n_tp for d in range(n_tp)]

    gate_own = parity_gather(w_gate)
    value_own = ring_gather(w_value)
    down_t = w_down.T
    inner = down_t.shape[1] // 2
    low, high = down_t[:, :inner], down_t[:, inner:]
    kept_half = jnp.where(core == 0, low, high)
    came_half = core_swap(jnp.where(core == 0, high, low))
    even_piece = jnp.where(core == 0, kept_half, came_half)
    odd_piece = jnp.where(core == 0, came_half, kept_half)
    down_odd = parity_gather(odd_piece)
    down_even = parity_gather(even_piece)
    gate_far = core_swap(gate_own)
    value_far = core_swap(value_own)

    out_far = [turned(out_weight, "tp", d) for d in range(1, n_tp)]
    out_parts = [by_parity(t, depth) for t in [out_weight] + out_far]
    residual = by_parity(residual, depth)
    norm_gain = norm_gain.reshape(-1, 2, depth).swapaxes(0, 1).reshape(-1)
    docs_plus = doc_ids + 1
    prev_keys, prev_values, prev_docs = shifted(
        (keys[-WINDOW:], values[-WINDOW:], docs_plus[-WINDOW:]), "sp", 1
    )
    key_ext = jnp.concatenate([prev_keys, keys], axis=0)
    value_ext = jnp.concatenate([prev_values, values], axis=0)
    doc_ext = jnp.concatenate([prev_docs, docs_plus], axis=0)
    head_out = attend(queries, key_ext, value_ext, docs_plus, doc_ext, sinks)

    def rows_of(t, index):
        return lax.dynamic_slice_in_dim(t, index * part_rows, part_rows, 0)

    proj = jnp.dot(rows_of(head_out, tp), out_parts[0], preferred_element_type=jnp.float32)
    for d in range(1, n_tp):
        heads_far = turned(rows_of(head_out, (tp + d) % n_tp), "tp", d)
        proj = proj + jnp.dot(heads_far, out_parts[d], preferred_element_type=jnp.float32)
    mid = (residual.astype(jnp.float32) + proj).astype(jnp.bfloat16)
    mid32 = mid.astype(jnp.float32)
    normed = (
        mid32 * lax.rsqrt(jnp.mean(mid32 * mid32, axis=-1, keepdims=True) + 1e-06) * norm_gain
    ).astype(jnp.bfloat16)
    even, odd = normed[:, :half], normed[:, half:]
    own = [jnp.where(core == 0, even, odd)]
    far = [jnp.where(core == 0, odd, even)]
    for d in range(1, n_tp):
        own.append(turned(own[0], "tp", d))
        far.append(turned(far[0], "tp", d))

    def up(own, far, w_own, w_far):
        total = jnp.dot(own, w_own, preferred_element_type=jnp.float32)
        return (total + jnp.dot(far, w_far, preferred_element_type=jnp.float32)).astype(
            jnp.bfloat16
        )

    gate_parts = [up(o, f, gate_own, gate_far) for o, f in zip(own, far)]
    value_parts = [up(o, f, value_own, value_far) for o, f in zip(own, far)]

    conv_docs = jnp.concatenate([prev_docs[-2:], docs_plus], axis=0)
    part_docs = [
        lax.dynamic_slice_in_dim(conv_docs, i * part_rows, part_rows + 2, 0) for i in part_index
    ]

    def conv_parts(parts, taps):
        tails = [p[-2:] for p in parts]
        last = tails[0]
        for d in range(1, n_tp):
            last = jnp.where(part_index[d] == n_tp - 1, tails[d], last)
        prev = shifted(last, "sp", 1)
        result = []
        for d in range(n_tp):
            halo = jnp.where(part_index[d] == 0, prev, tails[(d + 1) % n_tp])
            result.append(
                convolve(jnp.concatenate([halo, parts[d]], axis=0), part_docs[d], taps)
            )
        return result

    gate_conv = conv_parts(gate_parts, conv_gate)
    value_conv = conv_parts(value_parts, conv_value)
    hidden = [
        (jax.nn.silu(g) * v).astype(jnp.bfloat16) for g, v in zip(gate_conv, value_conv)
    ]

    def down(units, w_t):
        return lax.dot_general(
            units, w_t, (((1,), (1,)), ((), ())), preferred_element_type=jnp.float32
        )

    own_units = [jnp.where(core == 0, h[:, :inner], h[:, inner:]) for h in hidden]
    far_units = [jnp.where(core == 0, h[:, inner:], h[:, :inner]) for h in hidden]

    def down_sums(w_own):
        w_far = core_swap(w_own)
        came = []
        for d in range(1, n_tp):
            sent = (down(own_units[d], w_own) + down(far_units[d], w_far)).astype(
                jnp.bfloat16
            )
            came.append(turned(sent, "tp", -d))
        kept = down(own_units[0], w_own) + down(far_units[0], w_far)
        for t in came:
            kept = kept + t.astype(jnp.float32)
        return kept

    odd_sum = down_sums(down_odd)
    even_sum = down_sums(down_even)
    sums = (even_sum, odd_sum)
    return finish(mid, sums, depth)


def mult(x, m):
    return x if isinstance(x, int) else pl.multiple_of(x, m)


def ring_chip(place, chips):
    odd = lax.div(place, chips // 2)
    return (1 - odd) * (2 * place) + odd * (2 * (chips - 1 - place) + 1)


def layer_kernel(
    n_sp,
    n_tp,
    queries,
    keys,
    values,
    docs,
    sinks,
    residual,
    out_weight,
    norm_gain,
    w_gate,
    w_value,
    conv_gate,
    conv_value,
    w_down,
    mid,
    wg,
    wv,
    wd,
    nrm,
    hid,
    pre,
    q_v,
    k_v,
    v_v,
    doc_v,
    doc_col,
    same_one,
    same_two,
    att,
    heads,
    ow,
    gain_v,
    cg_v,
    cv_v,
    send,
    came,
    own,
    local_sem,
    ring_send,
    ring_recv,
    sib_send,
    sib_recv,
    halo_send,
    halo_recv,
    ow_send,
    ow_recv,
    heads_send,
    heads_recv,
    nrm_send,
    nrm_recv,
    sum_send,
    sum_recv,
):
    sp = lax.axis_index("sp")
    tp = lax.axis_index("tp")
    chips = n_sp // 2
    core = lax.rem(sp, 2)
    chip = lax.div(sp, 2)
    odd = lax.rem(chip, 2)
    place = (1 - odd) * lax.div(chip, 2) + odd * (chips - 1 - lax.div(chip, 2))
    way = 1 - 2 * core
    down_sp = 2 * ring_chip(lax.rem(place + way + chips, chips), chips) + core
    up_sp = 2 * ring_chip(lax.rem(place - way + chips, chips), chips) + core
    sib_sp = sp + way
    next_sp = lax.rem(sp + 1, n_sp)
    prev_sp = lax.rem(sp + n_sp - 1, n_sp)

    rows, q_width = queries.shape
    part = rows // n_tp
    depth, units = w_gate.shape
    kv_heads = keys.shape[1] // HEAD_DIM
    group = q_width // keys.shape[1]
    blocks = rows // WINDOW
    part_blocks = part // WINDOW
    ow_half = q_width // 2
    unit_tiles = units // TILE
    events = (chips - 1) * SUB

    def peer(d):
        return lax.rem(tp + d, n_tp)

    def held(h):
        return 2 * ring_chip(lax.rem(place - way * h + chips, chips), chips) + core

    def sib_held(h):
        return 2 * ring_chip(lax.rem(place + way * h + chips, chips), chips) + 1 - core

    def piece(w, j, s):
        if w == 2:
            size = units // SUB
            return wd.at[j, pl.ds(mult(s * size, size), size), :]
        size = depth // SUB
        buf = (wg, wv)[w]
        return buf.at[pl.ds(mult(j * depth + s * size, size), size), :]

    def own_piece(w, s):
        ref = (w_gate, w_value, w_down)[w]
        size = ref.shape[0] // SUB
        return ref.at[pl.ds(s * size, size), :]

    def remote(src, dst, send_sem, recv_sem, device):
        return pltpu.make_async_remote_copy(
            src_ref=src,
            dst_ref=dst,
            send_sem=send_sem,
            recv_sem=recv_sem,
            device_id=device,
            device_id_type=MESH,
        )

    def ring_copy(w, h, s, src=None):
        dst = piece(w, held(h - 1), s)
        return remote(
            dst if src is None else src,
            dst,
            ring_send.at[w],
            ring_recv.at[w, h, s],
            (down_sp, tp),
        )

    def ring_wait(w, h, s):
        dst = piece(w, held(h), s)
        remote(
            dst, dst, ring_send.at[w], ring_recv.at[w, h, s], (down_sp, tp)
        ).wait_recv()

    def sib_sems(w, h):
        return sib_send.at[w], sib_recv.at[w, h if w == 2 else 0]

    def sib_copy(w, h, s, src=None):
        dst = piece(w, held(h), s)
        return remote(dst if src is None else src, dst, *sib_sems(w, h), (sib_sp, tp))

    def sib_wait(w, h):
        got = wd.at[sib_held(h)] if w == 2 else (wg, wv)[w].at[pl.ds(0, chips * depth), :]
        remote(got, got, *sib_sems(w, h), (sib_sp, tp)).wait_recv()

    def sent_weights(w):
        passed = (chips - 1) * depth
        buf = (wg, wv, wd)[w]
        ring = buf.at[pl.ds(0, chips - 1)] if w == 2 else buf.at[pl.ds(0, passed), :]
        swapped = buf.at[pl.ds(0, chips)] if w == 2 else buf.at[pl.ds(0, chips * depth), :]
        remote(ring, ring, ring_send.at[w], ring_recv.at[w, 0, 0], (down_sp, tp)).wait_send()
        remote(swapped, swapped, *sib_sems(w, 0), (sib_sp, tp)).wait_send()

    def start_own(w):
        for s in range(SUB):
            ring_copy(w, 1, s, own_piece(w, s)).start()
        for s in range(SUB):
            sib_copy(w, 0, s, own_piece(w, s)).start()

    def service(w, e):
        h = 1 + (e // SUB if isinstance(e, int) else lax.div(e, SUB))
        s = e % SUB if isinstance(e, int) else lax.rem(e, SUB)
        ring_wait(w, h, s)
        if isinstance(e, int):
            if h < chips - 1:
                ring_copy(w, h + 1, s).start()
        else:

            @pl.when(h < chips - 1)
            def _():
                ring_copy(w, h + 1, s).start()

        sib_copy(w, h, s).start()
        if w < 2:

            @pl.when(e == (chips - 2) * SUB - 1)
            def _():
                start_own(w + 1)

    def serve(w, first, last):
        if last > first:

            @pl.loop(first, last)
            def _(e):
                service(w, e)

    local = [
        (keys, k_v.at[pl.ds(WINDOW, rows), :]),
        (values, v_v.at[pl.ds(WINDOW, rows), :]),
        (docs, doc_v.at[pl.ds(8, blocks), :]),
        (queries, q_v),
        (residual, mid),
        (out_weight, ow.at[tp]),
        (norm_gain, gain_v),
        (conv_gate, cg_v),
        (conv_value, cv_v),
        (w_gate, wg.at[pl.ds(mult(sp * depth, depth), depth), :]),
        (w_value, wv.at[pl.ds(mult(sp * depth, depth), depth), :]),
        (w_down, wd.at[sp]),
    ]
    local = [
        pltpu.make_async_copy(src, dst, local_sem.at[i]) for i, (src, dst) in enumerate(local)
    ]
    for copy in local[:4]:
        copy.start()

    barrier = pltpu.get_barrier_semaphore()
    greeted = [(down_sp, tp), (up_sp, tp), (sib_sp, tp), (next_sp, tp), (prev_sp, tp)]
    greeted += [(sp, peer(d)) for d in range(1, n_tp)]
    for device in greeted:
        pl.semaphore_signal(barrier, inc=1, device_id=device, device_id_type=MESH)
    pl.semaphore_wait(barrier, len(greeted))

    halos = [
        (keys.at[pl.ds(rows - WINDOW, WINDOW), :], k_v.at[pl.ds(0, WINDOW), :]),
        (values.at[pl.ds(rows - WINDOW, WINDOW), :], v_v.at[pl.ds(0, WINDOW), :]),
        (docs.at[pl.ds(blocks - 1, 1), :], doc_v.at[pl.ds(7, 1), :]),
    ]
    halos = [
        remote(src, dst, halo_send.at[i], halo_recv.at[i], (next_sp, tp))
        for i, (src, dst) in enumerate(halos)
    ]
    for copy in halos:
        copy.start()
    start_own(0)

    def ow_rows(t, c):
        return ow.at[t, pl.ds(mult(c * ow_half, ow_half), ow_half), :]

    ow_src = out_weight.at[pl.ds(mult(core * ow_half, ow_half), ow_half), :]
    ow_out = [
        remote(ow_src, ow_rows(tp, core), ow_send.at[0, d], ow_recv.at[0, d], (sp, peer(n_tp - d)))
        for d in range(1, n_tp)
    ]
    for copy in ow_out:
        copy.start()
    for copy in local[4:]:
        copy.start()

    for i in range(3):
        local[i].wait()
    for copy in halos:
        copy.wait_recv()
    local[3].wait()

    lane = lax.broadcasted_iota(jnp.int32, (WINDOW, 2 * HEAD_DIM), 1)
    low_lane = lane < HEAD_DIM
    doc_v[7:8, :] = jnp.where(sp == 0, -1, doc_v[7:8, :])
    for b in range(-1, blocks):
        row = doc_v[8 + b : 9 + b, :]
        column = jnp.broadcast_to(row, (WINDOW, WINDOW)).T
        if b < 0:
            doc_col[0:8, :] = column[WINDOW - 8 :, :]
        else:
            doc_col[8 + b * WINDOW : 8 + (b + 1) * WINDOW, :] = column
    for b in range(blocks):
        at = 8 + b * WINDOW
        here = doc_col[at : at + WINDOW, :]
        back_one = doc_col[at - 1 : at - 1 + WINDOW, :]
        back_two = doc_col[at - 2 : at - 2 + WINDOW, :]
        to = slice(b * WINDOW, (b + 1) * WINDOW)
        same_one[to, :] = jnp.where(here == back_one, 1.0, 0.0)
        same_two[to, :] = jnp.where(here == back_two, 1.0, 0.0)

    q_index = lax.broadcasted_iota(jnp.int32, (WINDOW, 2 * WINDOW), 0)
    k_index = lax.broadcasted_iota(jnp.int32, (WINDOW, 2 * WINDOW), 1)
    first_rows = lax.broadcasted_iota(jnp.int32, (2 * WINDOW, 1), 0) < WINDOW

    def attend_block(b):
        base = mult(b * WINDOW, WINDOW)
        key_docs = jnp.concatenate([doc_v[pl.ds(7 + b, 1), :], doc_v[pl.ds(8 + b, 1), :]], axis=1)
        here = doc_col[pl.ds(mult(8 + base, 8), WINDOW), :]
        keep = (k_index > q_index) & (k_index <= q_index + WINDOW)
        keep = keep & (jnp.concatenate([here, here], axis=1) == key_docs)
        keep = jnp.concatenate([keep, keep], axis=0)
        k_band = k_v[pl.ds(base, 2 * WINDOW), :]
        v_band = v_v[pl.ds(base, 2 * WINDOW), :]
        for g in range(kv_heads):
            at = slice(g * HEAD_DIM, (g + 1) * HEAD_DIM)
            kk = jnp.concatenate([k_band[:, at], k_band[:, at]], axis=1)
            vv = jnp.concatenate([v_band[:, at], v_band[:, at]], axis=1)
            for pair in range(group // 2):
                head = g * group + 2 * pair
                lanes = slice(head * HEAD_DIM, (head + 2) * HEAD_DIM)
                both = q_v[pl.ds(base, WINDOW), lanes]
                zero = jnp.zeros_like(both)
                split = jnp.concatenate(
                    [jnp.where(low_lane, both, zero), jnp.where(low_lane, zero, both)], axis=0
                )
                scores = lax.dot_general(
                    split, kk, (((1,), (1,)), ((), ())), preferred_element_type=jnp.float32
                ) * HEAD_DIM ** (-0.5)
                scores = jnp.where(keep, scores, -1e30)
                sink = jnp.where(first_rows, sinks[head], sinks[head + 1])
                peak = jnp.maximum(jnp.max(scores, axis=1, keepdims=True), sink)
                expd = jnp.exp(scores - peak)
                total = jnp.sum(expd, axis=1, keepdims=True) + jnp.exp(sink - peak)
                probs = (expd * (1.0 / total)).astype(jnp.bfloat16)
                mixed = jnp.dot(probs, vv, preferred_element_type=jnp.float32)
                att[pl.ds(base, WINDOW), lanes] = jnp.where(
                    low_lane, mixed[:WINDOW], mixed[WINDOW:]
                ).astype(jnp.bfloat16)

    def due(share):
        return events * share // 28

    pl.loop(0, blocks - part_blocks)(
        lambda i: attend_block(lax.rem((tp + 1) * part_blocks + i, blocks))
    )
    serve(0, 0, due(3))
    pl.loop(0, part_blocks)(lambda i: attend_block(tp * part_blocks + i))
    heads_out = [
        remote(
            att.at[pl.ds(mult(peer(n_tp - d) * part, part), part), :],
            heads.at[d - 1],
            heads_send.at[d],
            heads_recv.at[d],
            (sp, peer(n_tp - d)),
        )
        for d in range(1, n_tp)
    ]
    for copy in heads_out:
        copy.start()
    before_proj = due(14)
    serve(0, due(3), before_proj)

    for i in range(4, 9):
        local[i].wait()
    ow_on = []
    for d in range(1, n_tp):
        got = ow_rows(peer(d), core)
        remote(got, got, ow_send.at[0, d], ow_recv.at[0, d], (sp, peer(n_tp - d))).wait_recv()
        copy = remote(got, got, ow_send.at[1, d], ow_recv.at[1, d], (sib_sp, tp))
        copy.start()
        ow_on.append(copy)
    for d in range(1, n_tp):
        got = ow_rows(peer(d), 1 - core)
        remote(got, got, ow_send.at[1, d], ow_recv.at[1, d], (sib_sp, tp)).wait_recv()
        heads_out[d - 1].wait_recv()

    part_base = tp * part

    def nrm_rows(t, i):
        return nrm.at[pl.ds(mult(HALO + t * part + i * WINDOW, HALO), WINDOW), :]

    def nrm_copy(i, d):
        at = nrm_rows(tp, i)
        return remote(at, at, nrm_send.at[0], nrm_recv.at[i, d], (sp, peer(n_tp - d)))

    def project(i):
        at = pl.ds(mult(i * WINDOW, WINDOW), WINDOW)
        mine = att[pl.ds(mult(part_base + i * WINDOW, WINDOW), WINDOW), :]
        proj = jnp.dot(mine, ow[tp], preferred_element_type=jnp.float32)
        for d in range(1, n_tp):
            proj = proj + jnp.dot(
                heads[d - 1, at, :], ow[peer(d)], preferred_element_type=jnp.float32
            )
        rounded = (mid[at, :].astype(jnp.float32) + proj).astype(jnp.bfloat16)
        mid[at, :] = rounded
        wide = rounded.astype(jnp.float32)
        scale = lax.rsqrt(jnp.mean(wide * wide, axis=1, keepdims=True) + 1e-06)
        normed = (wide * scale * gain_v[...]).astype(jnp.bfloat16)
        nrm[pl.ds(mult(HALO + part_base + i * WINDOW, HALO), WINDOW), :] = normed

    @pl.loop(0, part_blocks)
    def _(k):
        i = part_blocks - 1 - k
        project(i)
        for d in range(1, n_tp):

            @pl.when(k > 0)
            def _():
                nrm_copy(i + 1, d).start()

        @pl.when(before_proj + k < events)
        def _():
            service(0, before_proj + k)

    for d in range(1, n_tp):
        nrm_copy(0, d).start()

    after_proj = min(events, before_proj + part_blocks)
    serve(0, after_proj, events)
    early_value = due(14)

    def nrm_wait(i):
        for d in range(1, n_tp):
            got = nrm_rows(peer(d), i)
            remote(
                got, got, nrm_send.at[0], nrm_recv.at[i, d], (sp, peer(n_tp - d))
            ).wait_recv()

    nrm_wait(part_blocks - 1)
    nrm_halo = remote(
        nrm.at[pl.ds(rows, HALO), :],
        nrm.at[pl.ds(0, HALO), :],
        halo_send.at[3],
        halo_recv.at[3],
        (next_sp, tp),
    )
    nrm_halo.start()
    serve(1, 0, early_value)
    pl.loop(0, part_blocks - 1)(nrm_wait)
    for i in range(9, 12):
        local[i].wait()

    sib_wait(0, 0)
    for copy in halos + heads_out + ow_out + ow_on + [nrm_halo]:
        copy.wait_send()

    sent_rows = nrm.at[pl.ds(0, (n_tp - 1) * part), :]
    remote(sent_rows, sent_rows, nrm_send.at[0], nrm_recv.at[0, 1], (sp, peer(1))).wait_send()

    nrm_halo.wait_recv()

    def up_tile(w_ref, taps, n, base, lengths):
        cols = pl.ds(mult(n * TILE, TILE), TILE)
        at = 0
        for length in lengths:
            lhs = nrm[pl.ds(mult(base + at, HALO), length), :]
            pre[at : at + length, :] = (
                jnp.dot(lhs, w_ref[:, cols], preferred_element_type=jnp.float32)
                .astype(jnp.bfloat16)
                .astype(jnp.float32)
            )
            at += length
        tap = taps[:, cols]
        for b in range((at - HALO) // WINDOW):
            at = HALO + b * WINDOW
            to = pl.ds(mult(base + b * WINDOW, WINDOW), WINDOW)
            one = jnp.concatenate([same_one[to, :]] * (TILE // WINDOW), axis=1)
            two = jnp.concatenate([same_two[to, :]] * (TILE // WINDOW), axis=1)
            conv = tap[2:3] * pre[at : at + WINDOW, :]
            conv = conv + one * (tap[1:2] * pre[at - 1 : at - 1 + WINDOW, :])
            conv = conv + two * (tap[0:1] * pre[at - 2 : at - 2 + WINDOW, :])
            yield to, cols, conv

    def spread(w, first, count, i):
        before = lax.div(i * count, unit_tiles)
        after = lax.div((i + 1) * count, unit_tiles)

        @pl.when(after > before)
        def _():
            service(w, first + before)

    gate_count = min(unit_tiles, events - early_value)

    @pl.loop(0, unit_tiles)
    def _(n):
        lengths = (HALO + rows // 2, rows // 2)
        for to, cols, conv in up_tile(wg, cg_v, n, 0, lengths):
            hid[to, cols] = (conv / (1.0 + jnp.exp(-conv))).astype(jnp.bfloat16)
        spread(1, early_value, gate_count, n)

    serve(1, early_value + gate_count, events)
    sib_wait(1, 0)

    def value_part(t, first, count):
        @pl.loop(0, unit_tiles)
        def _(n):
            for to, cols, conv in up_tile(wv, cv_v, n, t * part, (HALO + part,)):
                hid[to, cols] = (hid[to, cols].astype(jnp.float32) * conv).astype(
                    jnp.bfloat16
                )
            spread(2, first, count, n)

    def sum_copy(h, d):
        return remote(
            send.at[h, d - 1],
            came.at[h, d - 1],
            sum_send.at[0],
            sum_recv.at[h, d],
            (sp, peer(d)),
        )

    def hop_cols(h, c):
        j = held(h) if c == 0 else sib_held(h)
        return pl.ds(mult(j * depth, depth), depth)

    def finish_hop(h):
        for d in range(1, n_tp):
            got = came.at[h, d - 1]
            remote(
                got, got, sum_send.at[0], sum_recv.at[h, d], (sp, peer(d))
            ).wait_recv()
        for c in range(2):
            cols = hop_cols(h, c)
            from_cols = slice(c * depth, (c + 1) * depth)
            total = own[h, :, from_cols] + mid[:, cols].astype(jnp.float32)
            for d in range(1, n_tp):
                total = total + came[h, d - 1, :, from_cols].astype(jnp.float32)
            mid[:, cols] = total.astype(jnp.bfloat16)

    def down_rows(h, t):
        lhs = hid[pl.ds(mult(t * part, part), part), :]
        rhs = jnp.concatenate([wd[held(h)], wd[sib_held(h)]], axis=1)
        return jnp.dot(lhs, rhs, preferred_element_type=jnp.float32)

    def down_far(h):
        sib_wait(2, h)
        for d in range(1, n_tp):
            send[h, d - 1] = down_rows(h, peer(d)).astype(jnp.bfloat16)

    def send_sums(h):
        for d in range(1, n_tp):
            sum_copy(h, d).start()

    served = due(5)
    for d in range(1, n_tp):
        value_part(peer(d), 0, served if d == 1 else 0)

    @pl.loop(0, EARLY)
    def _(h):
        down_far(h)
        for i in range(due(1)):
            service(2, served + h * due(1) + i)
        send_sums(h)

    served += EARLY * due(1)
    more = due(6)
    value_part(tp, served, more)
    served += more

    @pl.loop(EARLY, chips + EARLY)
    def _(h):
        @pl.when(h < chips)
        def _():
            for s in range(SUB):

                @pl.when((h - 1) * SUB + s >= served)
                def _():
                    service(2, (h - 1) * SUB + s)

            down_far(h)

        @pl.when(h > EARLY)
        def _():
            finish_hop(h - EARLY - 1)

        for w in range(2):

            @pl.when(h == EARLY + w)
            def _():
                sent_weights(w)

        @pl.when(h < chips)
        def _():
            send_sums(h)

        own[h - EARLY] = down_rows(h - EARLY, tp)

    finish_hop(chips - 1)

    sent_weights(2)

    remote(send, send, sum_send.at[0], sum_recv.at[0, 1], (sp, peer(1))).wait_send()


def whole_layer(n_sp, n_tp, queries, keys, values, doc_ids, sinks, residual, out_weight,
                norm_gain, w_gate, w_value, conv_gate, conv_value, w_down):
    rows, q_width = queries.shape
    kv_width = keys.shape[1]
    part, width = residual.shape
    depth, units = w_gate.shape
    chips = n_sp // 2
    bf16, f32 = jnp.bfloat16, jnp.float32
    dma = pltpu.SemaphoreType.DMA
    part_blocks = part // WINDOW
    scratch = [
        pltpu.VMEM((width, units), bf16),
        pltpu.VMEM((width, units), bf16),
        pltpu.VMEM((n_sp, units, depth), bf16),
        pltpu.VMEM((HALO + rows, width), bf16),
        pltpu.VMEM((rows, units), bf16),
        pltpu.VMEM((HALO + rows, TILE), f32),
        pltpu.VMEM((rows, q_width), bf16),
        pltpu.VMEM((WINDOW + rows, kv_width), bf16),
        pltpu.VMEM((WINDOW + rows, kv_width), bf16),
        pltpu.VMEM((8 + rows // WINDOW, WINDOW), jnp.int32),
        pltpu.VMEM((8 + rows, WINDOW), jnp.int32),
        pltpu.VMEM((rows, WINDOW), f32),
        pltpu.VMEM((rows, WINDOW), f32),
        pltpu.VMEM((rows, q_width), bf16),
        pltpu.VMEM((n_tp - 1, part, q_width), bf16),
        pltpu.VMEM((n_tp, q_width, width), bf16),
        pltpu.VMEM((1, width), f32),
        pltpu.VMEM((3, units), f32),
        pltpu.VMEM((3, units), f32),
        pltpu.VMEM((chips, n_tp - 1, part, 2 * depth), bf16),
        pltpu.VMEM((chips, n_tp - 1, part, 2 * depth), bf16),
        pltpu.VMEM((chips, part, 2 * depth), f32),
        dma((12,)),
        dma((3,)),
        dma((3, chips, SUB)),
        dma((3,)),
        dma((3, chips)),
        dma((4,)),
        dma((4,)),
        dma((2, n_tp)),
        dma((2, n_tp)),
        dma((n_tp,)),
        dma((n_tp,)),
        dma((1,)),
        dma((part_blocks, n_tp)),
        dma((1,)),
        dma((chips, n_tp)),
    ]
    any_spec = pl.BlockSpec(memory_space=pl.ANY)
    specs = [any_spec] * 13
    specs[4] = pl.BlockSpec(memory_space=pltpu.SMEM)
    return pl.pallas_call(
        functools.partial(layer_kernel, n_sp, n_tp),
        out_shape=pltpu.VMEM(residual.shape, residual.dtype),
        in_specs=specs,
        out_specs=pl.BlockSpec(memory_space=pltpu.VMEM),
        scratch_shapes=scratch,
        compiler_params=pltpu.CompilerParams(
            collective_id=0, has_side_effects=True, vmem_limit_bytes=VMEM_BYTES
        ),
    )(
        queries,
        keys,
        values,
        doc_ids.reshape(rows // WINDOW, WINDOW),
        sinks,
        residual,
        out_weight,
        norm_gain.reshape(1, width),
        w_gate,
        w_value,
        conv_gate,
        conv_value,
        w_down,
    )


def in_one_kernel(n_sp, n_tp, queries, keys, values, doc_ids, *weights):
    w_gate = weights[4]
    depth, units = w_gate.shape
    aligned = depth % 128 == 0 and keys.shape[1] % 128 == 0 and units % TILE == 0
    return aligned and n_sp % 4 == 0 and n_tp > 1 and doc_ids.shape[0] % (n_tp * WINDOW) == 0


def solution(mesh):
    n_sp, n_tp = mesh.shape["sp"], mesh.shape["tp"]

    def body(*args):
        if in_one_kernel(n_sp, n_tp, *args):
            return whole_layer(n_sp, n_tp, *args)
        return per_device(*args)

    return jax.shard_map(
        body,
        mesh=mesh,
        in_specs=(
            P("sp", "tp"),
            P("sp", "tp"),
            P("sp", "tp"),
            P("sp"),
            P("tp"),
            P(("sp", "tp"), None),
            P("tp", None),
            P(),
            P("sp", "tp"),
            P("sp", "tp"),
            P(None, "tp"),
            P(None, "tp"),
            P("tp", "sp"),
        ),
        out_specs=P(("sp", "tp"), None),
        check_vma=False,
    )
```

```python
import functools

import jax
import jax.numpy as jnp
from jax import lax
from jax.experimental import pallas as pl
from jax.experimental.pallas import tpu as pltpu
from jax.sharding import PartitionSpec as P


HEAD_DIM = 64
WINDOW = 128
ROW_TILE = 128
SUB = 4
EARLY = 2
HALO = 16
TILE = 256
VMEM_BYTES = 64800000
MESH = pl.DeviceIdType.MESH


def shifted(shard, axis, by):
    size = lax.axis_size(axis)
    pairs = [(i, i + by) for i in range(size) if 0 <= i + by < size]
    return lax.ppermute(shard, axis, pairs)


def turned(t, axis, by):
    size = lax.axis_size(axis)
    return lax.ppermute(t, axis, [(i, (i + by) % size) for i in range(size)])


def core_swap(t):
    size = lax.axis_size("sp")
    return lax.ppermute(t, "sp", [(i, i ^ 1) for i in range(size)])


def parity_gather(t):
    size = lax.axis_size("sp")
    groups = [list(range(0, size, 2)), list(range(1, size, 2))]
    return lax.all_gather(t, "sp", axis=0, tiled=True, axis_index_groups=groups)


def ring_gather(t):
    chips = lax.axis_size("sp") // 2
    order = list(range(0, chips, 2)) + list(range(1, chips, 2))[::-1]
    chip = lax.axis_index("sp") // 2
    place = jnp.where(chip % 2 == 0, chip // 2, chips - 1 - chip // 2)

    def hop(piece, by):
        pairs = [
            (2 * order[k] + c, 2 * order[(k + by) % chips] + c)
            for k in range(chips)
            for c in range(2)
        ]
        return lax.ppermute(piece, "sp", pairs)

    def chip_at(k):
        k = (k + chips) % chips
        return jnp.where(k < chips // 2, 2 * k, 2 * (chips - 1 - k) + 1)

    depth = t.shape[0]
    pieces = [(chip, t)]
    up = down = t
    for step in range(1, chips // 2 + 1):
        up = hop(up, 1)
        pieces.append((chip_at(place - step), up))
        if step < chips - step:
            down = hop(down, -1)
            pieces.append((chip_at(place + step), down))
    whole = jnp.zeros((chips * depth,) + t.shape[1:], t.dtype)
    for at, piece in pieces:
        whole = lax.dynamic_update_slice_in_dim(whole, piece, at * depth, 0)
    return whole


def by_parity(t, depth):
    rows, width = t.shape
    blocks = width // depth
    tile = min(ROW_TILE, rows)

    def kernel(in_ref, out_ref):
        for j in range(blocks):
            to = (j // 2 + (j % 2) * (blocks // 2)) * depth
            out_ref[:, to : to + depth] = in_ref[:, j * depth : (j + 1) * depth]

    return pl.pallas_call(
        kernel,
        out_shape=jax.ShapeDtypeStruct(t.shape, t.dtype),
        grid=(rows // tile,),
        in_specs=[pl.BlockSpec((tile, width), lambda i: (i, 0))],
        out_specs=pl.BlockSpec((tile, width), lambda i: (i, 0)),
        cost_estimate=pl.CostEstimate(
            flops=0, bytes_accessed=2 * t.size * t.dtype.itemsize, transcendentals=0
        ),
    )(t)


def finish(mid, sums, depth):
    rows, width = mid.shape
    blocks = width // depth
    tile = min(ROW_TILE, rows)

    def kernel(mid_ref, even_ref, odd_ref, out_ref):
        for j in range(blocks):
            at = (j // 2) * depth
            held = at + (j % 2) * (width // 2)
            sum_ref = odd_ref if j % 2 else even_ref
            out_ref[:, j * depth : (j + 1) * depth] = (
                mid_ref[:, held : held + depth].astype(jnp.float32)
                + sum_ref[:, at : at + depth]
            ).astype(out_ref.dtype)

    half_spec = pl.BlockSpec((tile, width // 2), lambda i: (i, 0))
    return pl.pallas_call(
        kernel,
        out_shape=jax.ShapeDtypeStruct(mid.shape, mid.dtype),
        grid=(rows // tile,),
        in_specs=[pl.BlockSpec((tile, width), lambda i: (i, 0)), half_spec, half_spec],
        out_specs=pl.BlockSpec((tile, width), lambda i: (i, 0)),
        cost_estimate=pl.CostEstimate(
            flops=mid.size, bytes_accessed=8 * mid.size, transcendentals=0
        ),
    )(mid, *sums)


def attend(query_rows, key_ext, value_ext, doc_rows, doc_ext, sinks):
    row_count = query_rows.shape[0]
    block_count = row_count // WINDOW
    kv_heads = key_ext.shape[1] // HEAD_DIM
    group_size = query_rows.shape[1] // (kv_heads * HEAD_DIM)

    def band(t):
        lower = t[:row_count].reshape((block_count, WINDOW) + t.shape[1:])
        upper = t[WINDOW:].reshape((block_count, WINDOW) + t.shape[1:])
        return jnp.concatenate([lower, upper], axis=1)

    query_band = query_rows.reshape(block_count, WINDOW, kv_heads, group_size, HEAD_DIM)
    key_band = band(key_ext).reshape(block_count, 2 * WINDOW, kv_heads, HEAD_DIM)
    value_band = band(value_ext).reshape(block_count, 2 * WINDOW, kv_heads, HEAD_DIM)
    doc_band = band(doc_ext)
    distance = jnp.arange(WINDOW)[:, None] + WINDOW - jnp.arange(2 * WINDOW)[None, :]
    in_window = (distance >= 0) & (distance < WINDOW)
    same_doc = doc_rows.reshape(block_count, WINDOW)[:, :, None] == doc_band[:, None, :]
    keep_mask = in_window[None] & same_doc
    scores = jnp.einsum(
        "nqhgd,nkhd->nhgqk", query_band, key_band, preferred_element_type=jnp.float32
    ) * HEAD_DIM ** (-0.5)
    scores = jnp.where(keep_mask[:, None, None], scores, -jnp.inf)
    sink_logit = sinks.reshape(kv_heads, group_size)[None, :, :, None, None]
    peak = jnp.maximum(jnp.max(scores, axis=-1, keepdims=True), sink_logit)
    expd = jnp.exp(scores - peak)
    probs = (expd / (jnp.sum(expd, axis=-1, keepdims=True) + jnp.exp(sink_logit - peak))).astype(
        jnp.bfloat16
    )
    mixed = jnp.einsum("nhgqk,nkhd->nqhgd", probs, value_band, preferred_element_type=jnp.float32)
    return mixed.astype(jnp.bfloat16).reshape(row_count, -1)


def convolve(ext_rows, doc_ext, taps):
    center = doc_ext[2:]
    same_one = (doc_ext[1:-1] == center)[:, None]
    same_two = (doc_ext[:-2] == center)[:, None]
    ext32 = ext_rows.astype(jnp.float32)
    result = taps[2] * ext32[2:]
    result = result + jnp.where(same_one, taps[1] * ext32[1:-1], 0.0)
    return result + jnp.where(same_two, taps[0] * ext32[:-2], 0.0)


def per_device(
    queries,
    keys,
    values,
    doc_ids,
    sinks,
    residual,
    out_weight,
    norm_gain,
    w_gate,
    w_value,
    conv_gate,
    conv_value,
    w_down,
):
    core = lax.axis_index("sp") % 2
    tp = lax.axis_index("tp")
    n_tp = lax.axis_size("tp")
    rows = doc_ids.shape[0]
    part_rows = rows // n_tp
    depth = w_gate.shape[0]
    width = residual.shape[1]
    half = width // 2
    part_index = [(tp + n_tp - d) % n_tp for d in range(n_tp)]

    gate_own = parity_gather(w_gate)
    value_own = ring_gather(w_value)
    down_t = w_down.T
    inner = down_t.shape[1] // 2
    low, high = down_t[:, :inner], down_t[:, inner:]
    kept_half = jnp.where(core == 0, low, high)
    came_half = core_swap(jnp.where(core == 0, high, low))
    even_piece = jnp.where(core == 0, kept_half, came_half)
    odd_piece = jnp.where(core == 0, came_half, kept_half)
    down_odd = parity_gather(odd_piece)
    down_even = parity_gather(even_piece)
    gate_far = core_swap(gate_own)
    value_far = core_swap(value_own)

    out_far = [turned(out_weight, "tp", d) for d in range(1, n_tp)]
    out_parts = [by_parity(t, depth) for t in [out_weight] + out_far]
    residual = by_parity(residual, depth)
    norm_gain = norm_gain.reshape(-1, 2, depth).swapaxes(0, 1).reshape(-1)
    docs_plus = doc_ids + 1
    prev_keys, prev_values, prev_docs = shifted(
        (keys[-WINDOW:], values[-WINDOW:], docs_plus[-WINDOW:]), "sp", 1
    )
    key_ext = jnp.concatenate([prev_keys, keys], axis=0)
    value_ext = jnp.concatenate([prev_values, values], axis=0)
    doc_ext = jnp.concatenate([prev_docs, docs_plus], axis=0)
    head_out = attend(queries, key_ext, value_ext, docs_plus, doc_ext, sinks)

    def rows_of(t, index):
        return lax.dynamic_slice_in_dim(t, index * part_rows, part_rows, 0)

    proj = jnp.dot(rows_of(head_out, tp), out_parts[0], preferred_element_type=jnp.float32)
    for d in range(1, n_tp):
        heads_far = turned(rows_of(head_out, (tp + d) % n_tp), "tp", d)
        proj = proj + jnp.dot(heads_far, out_parts[d], preferred_element_type=jnp.float32)
    mid = (residual.astype(jnp.float32) + proj).astype(jnp.bfloat16)
    mid32 = mid.astype(jnp.float32)
    normed = (
        mid32 * lax.rsqrt(jnp.mean(mid32 * mid32, axis=-1, keepdims=True) + 1e-06) * norm_gain
    ).astype(jnp.bfloat16)
    even, odd = normed[:, :half], normed[:, half:]
    own = [jnp.where(core == 0, even, odd)]
    far = [jnp.where(core == 0, odd, even)]
    for d in range(1, n_tp):
        own.append(turned(own[0], "tp", d))
        far.append(turned(far[0], "tp", d))

    def up(own, far, w_own, w_far):
        total = jnp.dot(own, w_own, preferred_element_type=jnp.float32)
        return (total + jnp.dot(far, w_far, preferred_element_type=jnp.float32)).astype(
            jnp.bfloat16
        )

    gate_parts = [up(o, f, gate_own, gate_far) for o, f in zip(own, far)]
    value_parts = [up(o, f, value_own, value_far) for o, f in zip(own, far)]

    conv_docs = jnp.concatenate([prev_docs[-2:], docs_plus], axis=0)
    part_docs = [
        lax.dynamic_slice_in_dim(conv_docs, i * part_rows, part_rows + 2, 0) for i in part_index
    ]

    def conv_parts(parts, taps):
        tails = [p[-2:] for p in parts]
        last = tails[0]
        for d in range(1, n_tp):
            last = jnp.where(part_index[d] == n_tp - 1, tails[d], last)
        prev = shifted(last, "sp", 1)
        result = []
        for d in range(n_tp):
            halo = jnp.where(part_index[d] == 0, prev, tails[(d + 1) % n_tp])
            result.append(
                convolve(jnp.concatenate([halo, parts[d]], axis=0), part_docs[d], taps)
            )
        return result

    gate_conv = conv_parts(gate_parts, conv_gate)
    value_conv = conv_parts(value_parts, conv_value)
    hidden = [
        (jax.nn.silu(g) * v).astype(jnp.bfloat16) for g, v in zip(gate_conv, value_conv)
    ]

    def down(units, w_t):
        return lax.dot_general(
            units, w_t, (((1,), (1,)), ((), ())), preferred_element_type=jnp.float32
        )

    own_units = [jnp.where(core == 0, h[:, :inner], h[:, inner:]) for h in hidden]
    far_units = [jnp.where(core == 0, h[:, inner:], h[:, :inner]) for h in hidden]

    def down_sums(w_own):
        w_far = core_swap(w_own)
        came = []
        for d in range(1, n_tp):
            sent = (down(own_units[d], w_own) + down(far_units[d], w_far)).astype(
                jnp.bfloat16
            )
            came.append(turned(sent, "tp", -d))
        kept = down(own_units[0], w_own) + down(far_units[0], w_far)
        for t in came:
            kept = kept + t.astype(jnp.float32)
        return kept

    odd_sum = down_sums(down_odd)
    even_sum = down_sums(down_even)
    sums = (even_sum, odd_sum)
    return finish(mid, sums, depth)


def mult(x, m):
    return x if isinstance(x, int) else pl.multiple_of(x, m)


def ring_chip(place, chips):
    odd = lax.div(place, chips // 2)
    return (1 - odd) * (2 * place) + odd * (2 * (chips - 1 - place) + 1)


def layer_kernel(
    n_sp,
    n_tp,
    queries,
    keys,
    values,
    docs,
    sinks,
    residual,
    out_weight,
    norm_gain,
    w_gate,
    w_value,
    conv_gate,
    conv_value,
    w_down,
    mid,
    wg,
    wv,
    wd,
    nrm,
    hid,
    pre,
    q_v,
    k_v,
    v_v,
    doc_v,
    doc_col,
    same_one,
    same_two,
    att,
    heads,
    ow,
    gain_v,
    cg_v,
    cv_v,
    send,
    came,
    own,
    local_sem,
    ring_send,
    ring_recv,
    sib_send,
    sib_recv,
    halo_send,
    halo_recv,
    ow_send,
    ow_recv,
    heads_send,
    heads_recv,
    nrm_send,
    nrm_recv,
    sum_send,
    sum_recv,
):
    sp = lax.axis_index("sp")
    tp = lax.axis_index("tp")
    chips = n_sp // 2
    core = lax.rem(sp, 2)
    chip = lax.div(sp, 2)
    odd = lax.rem(chip, 2)
    place = (1 - odd) * lax.div(chip, 2) + odd * (chips - 1 - lax.div(chip, 2))
    way = 1 - 2 * core
    down_sp = 2 * ring_chip(lax.rem(place + way + chips, chips), chips) + core
    up_sp = 2 * ring_chip(lax.rem(place - way + chips, chips), chips) + core
    sib_sp = sp + way
    next_sp = lax.rem(sp + 1, n_sp)
    prev_sp = lax.rem(sp + n_sp - 1, n_sp)

    rows, q_width = queries.shape
    part = rows // n_tp
    depth, units = w_gate.shape
    kv_heads = keys.shape[1] // HEAD_DIM
    group = q_width // keys.shape[1]
    blocks = rows // WINDOW
    part_blocks = part // WINDOW
    ow_half = q_width // 2
    unit_tiles = units // TILE
    events = (chips - 1) * SUB

    def peer(d):
        return lax.rem(tp + d, n_tp)

    def held(h):
        return 2 * ring_chip(lax.rem(place - way * h + chips, chips), chips) + core

    def sib_held(h):
        return 2 * ring_chip(lax.rem(place + way * h + chips, chips), chips) + 1 - core

    def piece(w, j, s):
        size = depth // SUB
        return (wg, wv, wd)[w].at[pl.ds(mult(j * depth + s * size, size), size), :]

    def own_piece(w, s):
        if w == 2:
            return piece(2, sp, s)
        size = depth // SUB
        return (w_gate, w_value)[w].at[pl.ds(s * size, size), :]

    def remote(src, dst, send_sem, recv_sem, device):
        return pltpu.make_async_remote_copy(
            src_ref=src,
            dst_ref=dst,
            send_sem=send_sem,
            recv_sem=recv_sem,
            device_id=device,
            device_id_type=MESH,
        )

    def ring_copy(w, h, s, src=None):
        dst = piece(w, held(h - 1), s)
        return remote(
            dst if src is None else src,
            dst,
            ring_send.at[w],
            ring_recv.at[w, h, s],
            (down_sp, tp),
        )

    def ring_wait(w, h, s):
        dst = piece(w, held(h), s)
        remote(
            dst, dst, ring_send.at[w], ring_recv.at[w, h, s], (down_sp, tp)
        ).wait_recv()

    def sib_sem(w, h, s):
        if w < 2:
            return sib_recv.at[w, 0]
        late = lax.div(h, chips - 1) * (s // (SUB // 2) if isinstance(s, int) else lax.div(s, SUB // 2))
        return sib_recv.at[w, h + late]

    def sib_copy(w, h, s, src=None):
        dst = piece(w, held(h), s)
        return remote(
            dst if src is None else src, dst, sib_send.at[w], sib_sem(w, h, s), (sib_sp, tp)
        )

    def sib_wait(w, h, part_of=None):
        buf = (wg, wv, wd)[w]
        if w < 2:
            got = buf.at[pl.ds(0, chips * depth), :]
        elif part_of is None:
            got = buf.at[pl.ds(mult(sib_held(h) * depth, depth), depth), :]
        else:
            got = last_half(sib_held(h), part_of)
        sem = sib_sem(w, h, 0 if part_of is None else part_of * (SUB // 2))
        remote(got, got, sib_send.at[w], sem, (sib_sp, tp)).wait_recv()

    def last_half(j, part_of):
        return wd.at[pl.ds(mult(j * depth + part_of * (depth // 2), depth // 2), depth // 2), :]

    def sent_weights(w):
        buf = (wg, wv, wd)[w]
        ring = buf.at[pl.ds(0, (chips - 1) * depth), :]
        swapped = buf.at[pl.ds(0, chips * depth), :]
        remote(ring, ring, ring_send.at[w], ring_recv.at[w, 0, 0], (down_sp, tp)).wait_send()
        remote(
            swapped, swapped, sib_send.at[w], sib_recv.at[w, 0], (sib_sp, tp)
        ).wait_send()

    def start_own(w):
        for s in range(SUB):
            ring_copy(w, 1, s, own_piece(w, s)).start()
        for s in range(SUB):
            sib_copy(w, 0, s, own_piece(w, s)).start()

    def service(w, e):
        h = 1 + (e // SUB if isinstance(e, int) else lax.div(e, SUB))
        s = e % SUB if isinstance(e, int) else lax.rem(e, SUB)
        ring_wait(w, h, s)
        if isinstance(e, int):
            if h < chips - 1:
                ring_copy(w, h + 1, s).start()
        else:

            @pl.when(h < chips - 1)
            def _():
                ring_copy(w, h + 1, s).start()

        sib_copy(w, h, s).start()
        if w < 2:

            @pl.when(e == (chips - 2) * SUB - 1)
            def _():
                start_own(w + 1)

    def serve(w, first, last):
        if last > first:

            @pl.loop(first, last)
            def _(e):
                service(w, e)

    local = [
        (keys, k_v.at[pl.ds(WINDOW, rows), :]),
        (values, v_v.at[pl.ds(WINDOW, rows), :]),
        (docs, doc_v.at[pl.ds(8, blocks), :]),
        (queries, q_v),
        (residual, mid),
        (out_weight, ow.at[tp]),
        (norm_gain, gain_v),
        (conv_gate, cg_v),
        (conv_value, cv_v),
        (w_gate, wg.at[pl.ds(mult(sp * depth, depth), depth), :]),
        (w_value, wv.at[pl.ds(mult(sp * depth, depth), depth), :]),
    ]
    strips = [(c, min(rows, units - c * rows)) for c in range(-(-units // rows))]
    local += [
        (
            w_down.at[pl.ds(c * rows, length), :],
            hid.at[pl.ds(0, length), pl.ds(c * depth, depth)],
        )
        for c, length in strips
    ]
    local = [
        pltpu.make_async_copy(src, dst, local_sem.at[i]) for i, (src, dst) in enumerate(local)
    ]
    for copy in local[:4]:
        copy.start()

    barrier = pltpu.get_barrier_semaphore()
    greeted = [(down_sp, tp), (up_sp, tp), (sib_sp, tp), (next_sp, tp), (prev_sp, tp)]
    greeted += [(sp, peer(d)) for d in range(1, n_tp)]
    for device in greeted:
        pl.semaphore_signal(barrier, inc=1, device_id=device, device_id_type=MESH)
    pl.semaphore_wait(barrier, len(greeted))

    halos = [
        (keys.at[pl.ds(rows - WINDOW, WINDOW), :], k_v.at[pl.ds(0, WINDOW), :]),
        (values.at[pl.ds(rows - WINDOW, WINDOW), :], v_v.at[pl.ds(0, WINDOW), :]),
        (docs.at[pl.ds(blocks - 1, 1), :], doc_v.at[pl.ds(7, 1), :]),
    ]
    halos = [
        remote(src, dst, halo_send.at[i], halo_recv.at[i], (next_sp, tp))
        for i, (src, dst) in enumerate(halos)
    ]
    for copy in halos:
        copy.start()
    start_own(0)

    def ow_rows(t, c):
        return ow.at[t, pl.ds(mult(c * ow_half, ow_half), ow_half), :]

    ow_src = out_weight.at[pl.ds(mult(core * ow_half, ow_half), ow_half), :]
    ow_out = [
        remote(ow_src, ow_rows(tp, core), ow_send.at[0, d], ow_recv.at[0, d], (sp, peer(n_tp - d)))
        for d in range(1, n_tp)
    ]
    for copy in ow_out:
        copy.start()
    for copy in local[4:]:
        copy.start()

    for i in range(3):
        local[i].wait()
    for copy in halos:
        copy.wait_recv()
    local[3].wait()

    lane = lax.broadcasted_iota(jnp.int32, (WINDOW, 2 * HEAD_DIM), 1)
    low_lane = lane < HEAD_DIM
    doc_v[7:8, :] = jnp.where(sp == 0, -1, doc_v[7:8, :])
    for b in range(-1, blocks):
        row = doc_v[8 + b : 9 + b, :]
        column = jnp.broadcast_to(row, (WINDOW, WINDOW)).T
        if b < 0:
            doc_col[0:8, :] = column[WINDOW - 8 :, :]
        else:
            doc_col[8 + b * WINDOW : 8 + (b + 1) * WINDOW, :] = column
    for b in range(blocks):
        at = 8 + b * WINDOW
        here = doc_col[at : at + WINDOW, :]
        back_one = doc_col[at - 1 : at - 1 + WINDOW, :]
        back_two = doc_col[at - 2 : at - 2 + WINDOW, :]
        to = slice(b * WINDOW, (b + 1) * WINDOW)
        same_one[to, :] = jnp.where(here == back_one, 1.0, 0.0)
        same_two[to, :] = jnp.where(here == back_two, 1.0, 0.0)

    q_index = lax.broadcasted_iota(jnp.int32, (WINDOW, 2 * WINDOW), 0)
    k_index = lax.broadcasted_iota(jnp.int32, (WINDOW, 2 * WINDOW), 1)
    first_rows = lax.broadcasted_iota(jnp.int32, (2 * WINDOW, 1), 0) < WINDOW

    def attend_block(b):
        base = mult(b * WINDOW, WINDOW)
        key_docs = jnp.concatenate([doc_v[pl.ds(7 + b, 1), :], doc_v[pl.ds(8 + b, 1), :]], axis=1)
        here = doc_col[pl.ds(mult(8 + base, 8), WINDOW), :]
        keep = (k_index > q_index) & (k_index <= q_index + WINDOW)
        keep = keep & (jnp.concatenate([here, here], axis=1) == key_docs)
        keep = jnp.concatenate([keep, keep], axis=0)
        k_band = k_v[pl.ds(base, 2 * WINDOW), :]
        v_band = v_v[pl.ds(base, 2 * WINDOW), :]
        for g in range(kv_heads):
            at = slice(g * HEAD_DIM, (g + 1) * HEAD_DIM)
            kk = jnp.concatenate([k_band[:, at], k_band[:, at]], axis=1)
            vv = jnp.concatenate([v_band[:, at], v_band[:, at]], axis=1)
            for pair in range(group // 2):
                head = g * group + 2 * pair
                lanes = slice(head * HEAD_DIM, (head + 2) * HEAD_DIM)
                both = q_v[pl.ds(base, WINDOW), lanes]
                zero = jnp.zeros_like(both)
                split = jnp.concatenate(
                    [jnp.where(low_lane, both, zero), jnp.where(low_lane, zero, both)], axis=0
                )
                scores = lax.dot_general(
                    split, kk, (((1,), (1,)), ((), ())), preferred_element_type=jnp.float32
                ) * HEAD_DIM ** (-0.5)
                scores = jnp.where(keep, scores, -1e30)
                sink = jnp.where(first_rows, sinks[head], sinks[head + 1])
                peak = jnp.maximum(jnp.max(scores, axis=1, keepdims=True), sink)
                expd = jnp.exp(scores - peak)
                total = jnp.sum(expd, axis=1, keepdims=True) + jnp.exp(sink - peak)
                probs = (expd * (1.0 / total)).astype(jnp.bfloat16)
                mixed = jnp.dot(probs, vv, preferred_element_type=jnp.float32)
                att[pl.ds(base, WINDOW), lanes] = jnp.where(
                    low_lane, mixed[:WINDOW], mixed[WINDOW:]
                ).astype(jnp.bfloat16)

    def due(share):
        return events * share // 28

    pl.loop(0, blocks - part_blocks)(
        lambda i: attend_block(lax.rem((tp + 1) * part_blocks + i, blocks))
    )
    serve(0, 0, due(3))
    pl.loop(0, part_blocks)(lambda i: attend_block(tp * part_blocks + i))
    heads_out = [
        remote(
            att.at[pl.ds(mult(peer(n_tp - d) * part, part), part), :],
            heads.at[d - 1],
            heads_send.at[d],
            heads_recv.at[d],
            (sp, peer(n_tp - d)),
        )
        for d in range(1, n_tp)
    ]
    for copy in heads_out:
        copy.start()
    for copy in local[9:]:
        copy.wait()
    own_rows = pl.ds(mult(sp * depth, depth), depth)
    for c, length in strips:
        for at in range(0, length, TILE):
            turned_piece = hid[at : at + TILE, c * depth : (c + 1) * depth].astype(jnp.float32).T
            to = slice(c * rows + at, c * rows + at + TILE)
            wd[own_rows, to] = turned_piece.astype(jnp.bfloat16)
    before_proj = due(14)
    serve(0, due(3), before_proj)

    for i in range(4, 9):
        local[i].wait()
    ow_on = []
    for d in range(1, n_tp):
        got = ow_rows(peer(d), core)
        remote(got, got, ow_send.at[0, d], ow_recv.at[0, d], (sp, peer(n_tp - d))).wait_recv()
        copy = remote(got, got, ow_send.at[1, d], ow_recv.at[1, d], (sib_sp, tp))
        copy.start()
        ow_on.append(copy)
    for d in range(1, n_tp):
        got = ow_rows(peer(d), 1 - core)
        remote(got, got, ow_send.at[1, d], ow_recv.at[1, d], (sib_sp, tp)).wait_recv()
        heads_out[d - 1].wait_recv()

    part_base = tp * part

    def nrm_rows(t, i):
        return nrm.at[pl.ds(mult(HALO + t * part + i * WINDOW, HALO), WINDOW), :]

    def nrm_copy(i, d):
        at = nrm_rows(tp, i)
        return remote(at, at, nrm_send.at[0], nrm_recv.at[i, d], (sp, peer(n_tp - d)))

    def project(i):
        at = pl.ds(mult(i * WINDOW, WINDOW), WINDOW)
        mine = att[pl.ds(mult(part_base + i * WINDOW, WINDOW), WINDOW), :]
        proj = jnp.dot(mine, ow[tp], preferred_element_type=jnp.float32)
        for d in range(1, n_tp):
            proj = proj + jnp.dot(
                heads[d - 1, at, :], ow[peer(d)], preferred_element_type=jnp.float32
            )
        rounded = (mid[at, :].astype(jnp.float32) + proj).astype(jnp.bfloat16)
        mid[at, :] = rounded
        wide = rounded.astype(jnp.float32)
        scale = lax.rsqrt(jnp.mean(wide * wide, axis=1, keepdims=True) + 1e-06)
        normed = (wide * scale * gain_v[...]).astype(jnp.bfloat16)
        nrm[pl.ds(mult(HALO + part_base + i * WINDOW, HALO), WINDOW), :] = normed

    @pl.loop(0, part_blocks)
    def _(k):
        i = part_blocks - 1 - k
        project(i)
        for d in range(1, n_tp):

            @pl.when(k > 0)
            def _():
                nrm_copy(i + 1, d).start()

        @pl.when(before_proj + k < events)
        def _():
            service(0, before_proj + k)

    for d in range(1, n_tp):
        nrm_copy(0, d).start()

    after_proj = min(events, before_proj + part_blocks)
    serve(0, after_proj, events)
    early_value = due(14)

    def nrm_wait(i):
        for d in range(1, n_tp):
            got = nrm_rows(peer(d), i)
            remote(
                got, got, nrm_send.at[0], nrm_recv.at[i, d], (sp, peer(n_tp - d))
            ).wait_recv()

    nrm_wait(part_blocks - 1)
    nrm_halo = remote(
        nrm.at[pl.ds(rows, HALO), :],
        nrm.at[pl.ds(0, HALO), :],
        halo_send.at[3],
        halo_recv.at[3],
        (next_sp, tp),
    )
    nrm_halo.start()
    serve(1, 0, early_value)
    pl.loop(0, part_blocks - 1)(nrm_wait)

    sib_wait(0, 0)
    for copy in halos + heads_out + ow_out + ow_on + [nrm_halo]:
        copy.wait_send()

    sent_rows = nrm.at[pl.ds(0, (n_tp - 1) * part), :]
    remote(sent_rows, sent_rows, nrm_send.at[0], nrm_recv.at[0, 1], (sp, peer(1))).wait_send()

    nrm_halo.wait_recv()

    def up_tile(w_ref, taps, n, base, lengths):
        cols = pl.ds(mult(n * TILE, TILE), TILE)
        at = 0
        for length in lengths:
            lhs = nrm[pl.ds(mult(base + at, HALO), length), :]
            pre[at : at + length, :] = (
                jnp.dot(lhs, w_ref[:, cols], preferred_element_type=jnp.float32)
                .astype(jnp.bfloat16)
                .astype(jnp.float32)
            )
            at += length
        tap = taps[:, cols]
        for b in range((at - HALO) // WINDOW):
            at = HALO + b * WINDOW
            to = pl.ds(mult(base + b * WINDOW, WINDOW), WINDOW)
            one = jnp.concatenate([same_one[to, :]] * (TILE // WINDOW), axis=1)
            two = jnp.concatenate([same_two[to, :]] * (TILE // WINDOW), axis=1)
            conv = tap[2:3] * pre[at : at + WINDOW, :]
            conv = conv + one * (tap[1:2] * pre[at - 1 : at - 1 + WINDOW, :])
            conv = conv + two * (tap[0:1] * pre[at - 2 : at - 2 + WINDOW, :])
            yield to, cols, conv

    def spread(w, first, count, i):
        before = lax.div(i * count, unit_tiles)
        after = lax.div((i + 1) * count, unit_tiles)

        @pl.when(after > before)
        def _():
            service(w, first + before)

    gate_count = min(unit_tiles, events - early_value)

    @pl.loop(0, unit_tiles)
    def _(n):
        lengths = (HALO + rows // 2, rows // 2)
        for to, cols, conv in up_tile(wg, cg_v, n, 0, lengths):
            hid[to, cols] = (conv / (1.0 + jnp.exp(-conv))).astype(jnp.bfloat16)
        spread(1, early_value, gate_count, n)

    serve(1, early_value + gate_count, events)
    sib_wait(1, 0)

    def value_part(t, first, count):
        @pl.loop(0, unit_tiles)
        def _(n):
            for to, cols, conv in up_tile(wv, cv_v, n, t * part, (HALO + part,)):
                hid[to, cols] = (hid[to, cols].astype(jnp.float32) * conv).astype(
                    jnp.bfloat16
                )
            spread(2, first, count, n)

    def sum_copy(h, d, half=None):
        src, dst, sem = send.at[h, d - 1], came.at[h, d - 1], h
        if half is not None:
            lanes = slice(half * depth, (half + 1) * depth)
            src, dst, sem = src.at[:, lanes], dst.at[:, lanes], h + half
        return remote(src, dst, sum_send.at[0], sum_recv.at[sem, d], (sp, peer(d)))

    def hop_cols(h, c):
        j = held(h) if c == 0 else sib_held(h)
        return pl.ds(mult(j * depth, depth), depth)

    def add_up(h, c, parts):
        cols = hop_cols(h, c)
        total = own[h, :, c * depth : (c + 1) * depth] + mid[:, cols].astype(jnp.float32)
        for t in parts:
            total = total + t.astype(jnp.float32)
        mid[:, cols] = total.astype(jnp.bfloat16)

    def finish_hop(h):
        for d in range(1, n_tp):
            sum_copy(h, d).wait_recv()
        for c in range(2):
            lanes = slice(c * depth, (c + 1) * depth)
            add_up(h, c, [came[h, d - 1, :, lanes] for d in range(1, n_tp)])

    def finish_last():
        h = chips - 1
        for half in range(2):
            for d in range(1, n_tp):
                sum_copy(h, d, half).wait_recv()
        for c in range(2):
            lo = c * (depth // 2)
            pairs = [
                [came[h, d - 1, :, at + lo : at + lo + depth // 2] for at in (0, depth)]
                for d in range(1, n_tp)
            ]
            add_up(h, c, [jnp.concatenate(pair, axis=1) for pair in pairs])

    def apart(step):
        pl.when(sp >= 0)(step)

    def down_rows(rhs, t):
        lhs = hid[pl.ds(mult(t * part, part), part), :]
        return lax.dot_general(
            lhs, rhs, (((1,), (1,)), ((), ())), preferred_element_type=jnp.float32
        )

    def hop_rows(h):
        return jnp.concatenate(
            [wd[pl.ds(mult(j * depth, depth), depth), :] for j in (held(h), sib_held(h))], axis=0
        )

    def down_far(h):
        sib_wait(2, h)
        for d in range(1, n_tp):

            @apart
            def _():
                send[h, d - 1] = down_rows(hop_rows(h), peer(d)).astype(jnp.bfloat16)

    def down_own(h):
        @apart
        def _():
            own[h] = down_rows(hop_rows(h), tp)

    def down_far_half(half):
        h = chips - 1
        sib_wait(2, h, half)

        def rhs():
            return jnp.concatenate(
                [last_half(j, half)[...] for j in (held(h), sib_held(h))], axis=0
            )

        lanes = slice(half * depth, (half + 1) * depth)
        for d in range(1, n_tp):

            @apart
            def _():
                send[h, d - 1, :, lanes] = down_rows(rhs(), peer(d)).astype(jnp.bfloat16)

    def send_sums(h, half=None):
        for d in range(1, n_tp):
            sum_copy(h, d, half).start()

    served = due(5)
    for d in range(1, n_tp):
        value_part(peer(d), 0, served if d == 1 else 0)

    @pl.loop(0, EARLY)
    def _(h):
        down_far(h)
        for i in range(due(1)):
            service(2, served + h * due(1) + i)
        send_sums(h)

    served += EARLY * due(1)
    more = due(6)
    value_part(tp, served, more)
    served += more

    @pl.loop(EARLY, chips - 1)
    def _(h):
        for s in range(SUB):

            @pl.when((h - 1) * SUB + s >= served)
            def _():
                service(2, (h - 1) * SUB + s)

        down_far(h)

        @pl.when(h > EARLY)
        def _():
            finish_hop(h - EARLY - 1)

        for w in range(2):

            @pl.when(h == EARLY + w)
            def _():
                sent_weights(w)

        send_sums(h)
        down_own(h - EARLY)

    last = chips - 1
    for half in range(2):
        for s in range(SUB // 2):
            service(2, (last - 1) * SUB + half * (SUB // 2) + s)
        down_far_half(half)
        finish_hop(last - EARLY - 1 + half)
        send_sums(last, half)
        down_own(last - EARLY + half)
    for h in range(last - EARLY + 2, chips):
        down_own(h)
    for h in range(last - EARLY + 1, last):
        finish_hop(h)
    finish_last()

    sent_weights(2)

    remote(send, send, sum_send.at[0], sum_recv.at[0, 1], (sp, peer(1))).wait_send()


def whole_layer(n_sp, n_tp, queries, keys, values, doc_ids, sinks, residual, out_weight,
                norm_gain, w_gate, w_value, conv_gate, conv_value, w_down):
    rows, q_width = queries.shape
    kv_width = keys.shape[1]
    part, width = residual.shape
    depth, units = w_gate.shape
    chips = n_sp // 2
    bf16, f32 = jnp.bfloat16, jnp.float32
    dma = pltpu.SemaphoreType.DMA
    part_blocks = part // WINDOW
    scratch = [
        pltpu.VMEM((width, units), bf16),
        pltpu.VMEM((width, units), bf16),
        pltpu.VMEM((width, units), bf16),
        pltpu.VMEM((HALO + rows, width), bf16),
        pltpu.VMEM((rows, units), bf16),
        pltpu.VMEM((HALO + rows, TILE), f32),
        pltpu.VMEM((rows, q_width), bf16),
        pltpu.VMEM((WINDOW + rows, kv_width), bf16),
        pltpu.VMEM((WINDOW + rows, kv_width), bf16),
        pltpu.VMEM((8 + rows // WINDOW, WINDOW), jnp.int32),
        pltpu.VMEM((8 + rows, WINDOW), jnp.int32),
        pltpu.VMEM((rows, WINDOW), f32),
        pltpu.VMEM((rows, WINDOW), f32),
        pltpu.VMEM((rows, q_width), bf16),
        pltpu.VMEM((n_tp - 1, part, q_width), bf16),
        pltpu.VMEM((n_tp, q_width, width), bf16),
        pltpu.VMEM((1, width), f32),
        pltpu.VMEM((3, units), f32),
        pltpu.VMEM((3, units), f32),
        pltpu.VMEM((chips, n_tp - 1, part, 2 * depth), bf16),
        pltpu.VMEM((chips, n_tp - 1, part, 2 * depth), bf16),
        pltpu.VMEM((chips, part, 2 * depth), f32),
        dma((11 - (-units // rows),)),
        dma((3,)),
        dma((3, chips, SUB)),
        dma((3,)),
        dma((3, chips + 1)),
        dma((4,)),
        dma((4,)),
        dma((2, n_tp)),
        dma((2, n_tp)),
        dma((n_tp,)),
        dma((n_tp,)),
        dma((1,)),
        dma((part_blocks, n_tp)),
        dma((1,)),
        dma((chips + 1, n_tp)),
    ]
    any_spec = pl.BlockSpec(memory_space=pl.ANY)
    specs = [any_spec] * 13
    specs[4] = pl.BlockSpec(memory_space=pltpu.SMEM)
    return pl.pallas_call(
        functools.partial(layer_kernel, n_sp, n_tp),
        out_shape=pltpu.VMEM(residual.shape, residual.dtype),
        in_specs=specs,
        out_specs=pl.BlockSpec(memory_space=pltpu.VMEM),
        scratch_shapes=scratch,
        compiler_params=pltpu.CompilerParams(
            collective_id=0, has_side_effects=True, vmem_limit_bytes=VMEM_BYTES
        ),
    )(
        queries,
        keys,
        values,
        doc_ids.reshape(rows // WINDOW, WINDOW),
        sinks,
        residual,
        out_weight,
        norm_gain.reshape(1, width),
        w_gate,
        w_value,
        conv_gate,
        conv_value,
        w_down,
    )


def in_one_kernel(n_sp, n_tp, queries, keys, values, doc_ids, *weights):
    w_gate = weights[4]
    depth, units = w_gate.shape
    aligned = depth % 128 == 0 and keys.shape[1] % 128 == 0 and units % TILE == 0
    return aligned and n_sp % 4 == 0 and n_tp > 1 and doc_ids.shape[0] % (n_tp * WINDOW) == 0


def solution(mesh):
    n_sp, n_tp = mesh.shape["sp"], mesh.shape["tp"]

    def body(*args):
        if in_one_kernel(n_sp, n_tp, *args):
            return whole_layer(n_sp, n_tp, *args)
        return per_device(*args)

    return jax.shard_map(
        body,
        mesh=mesh,
        in_specs=(
            P("sp", "tp"),
            P("sp", "tp"),
            P("sp", "tp"),
            P("sp"),
            P("tp"),
            P(("sp", "tp"), None),
            P("tp", None),
            P(),
            P("sp", "tp"),
            P("sp", "tp"),
            P(None, "tp"),
            P(None, "tp"),
            P("tp", "sp"),
        ),
        out_specs=P(("sp", "tp"), None),
        check_vma=False,
    )
```

```python
import functools

import jax
import jax.numpy as jnp
from jax import lax
from jax.experimental import pallas as pl
from jax.experimental.pallas import tpu as pltpu
from jax.sharding import PartitionSpec as P


HEAD_DIM = 64
WINDOW = 128
ROW_TILE = 128
SUB = 4
EARLY = 2
HALO = 16
REACH = 2
TILE = 256
VMEM_BYTES = 64800000
MESH = pl.DeviceIdType.MESH


def shifted(shard, axis, by):
    size = lax.axis_size(axis)
    pairs = [(i, i + by) for i in range(size) if 0 <= i + by < size]
    return lax.ppermute(shard, axis, pairs)


def turned(t, axis, by):
    size = lax.axis_size(axis)
    return lax.ppermute(t, axis, [(i, (i + by) % size) for i in range(size)])


def core_swap(t):
    size = lax.axis_size("sp")
    return lax.ppermute(t, "sp", [(i, i ^ 1) for i in range(size)])


def parity_gather(t):
    size = lax.axis_size("sp")
    groups = [list(range(0, size, 2)), list(range(1, size, 2))]
    return lax.all_gather(t, "sp", axis=0, tiled=True, axis_index_groups=groups)


def ring_gather(t):
    chips = lax.axis_size("sp") // 2
    order = list(range(0, chips, 2)) + list(range(1, chips, 2))[::-1]
    chip = lax.axis_index("sp") // 2
    place = jnp.where(chip % 2 == 0, chip // 2, chips - 1 - chip // 2)

    def hop(piece, by):
        pairs = [
            (2 * order[k] + c, 2 * order[(k + by) % chips] + c)
            for k in range(chips)
            for c in range(2)
        ]
        return lax.ppermute(piece, "sp", pairs)

    def chip_at(k):
        k = (k + chips) % chips
        return jnp.where(k < chips // 2, 2 * k, 2 * (chips - 1 - k) + 1)

    depth = t.shape[0]
    pieces = [(chip, t)]
    up = down = t
    for step in range(1, chips // 2 + 1):
        up = hop(up, 1)
        pieces.append((chip_at(place - step), up))
        if step < chips - step:
            down = hop(down, -1)
            pieces.append((chip_at(place + step), down))
    whole = jnp.zeros((chips * depth,) + t.shape[1:], t.dtype)
    for at, piece in pieces:
        whole = lax.dynamic_update_slice_in_dim(whole, piece, at * depth, 0)
    return whole


def by_parity(t, depth):
    rows, width = t.shape
    blocks = width // depth
    tile = min(ROW_TILE, rows)

    def kernel(in_ref, out_ref):
        for j in range(blocks):
            to = (j // 2 + (j % 2) * (blocks // 2)) * depth
            out_ref[:, to : to + depth] = in_ref[:, j * depth : (j + 1) * depth]

    return pl.pallas_call(
        kernel,
        out_shape=jax.ShapeDtypeStruct(t.shape, t.dtype),
        grid=(rows // tile,),
        in_specs=[pl.BlockSpec((tile, width), lambda i: (i, 0))],
        out_specs=pl.BlockSpec((tile, width), lambda i: (i, 0)),
        cost_estimate=pl.CostEstimate(
            flops=0, bytes_accessed=2 * t.size * t.dtype.itemsize, transcendentals=0
        ),
    )(t)


def finish(mid, sums, depth):
    rows, width = mid.shape
    blocks = width // depth
    tile = min(ROW_TILE, rows)

    def kernel(mid_ref, even_ref, odd_ref, out_ref):
        for j in range(blocks):
            at = (j // 2) * depth
            held = at + (j % 2) * (width // 2)
            sum_ref = odd_ref if j % 2 else even_ref
            out_ref[:, j * depth : (j + 1) * depth] = (
                mid_ref[:, held : held + depth].astype(jnp.float32)
                + sum_ref[:, at : at + depth]
            ).astype(out_ref.dtype)

    half_spec = pl.BlockSpec((tile, width // 2), lambda i: (i, 0))
    return pl.pallas_call(
        kernel,
        out_shape=jax.ShapeDtypeStruct(mid.shape, mid.dtype),
        grid=(rows // tile,),
        in_specs=[pl.BlockSpec((tile, width), lambda i: (i, 0)), half_spec, half_spec],
        out_specs=pl.BlockSpec((tile, width), lambda i: (i, 0)),
        cost_estimate=pl.CostEstimate(
            flops=mid.size, bytes_accessed=8 * mid.size, transcendentals=0
        ),
    )(mid, *sums)


def attend(query_rows, key_ext, value_ext, doc_rows, doc_ext, sinks):
    row_count = query_rows.shape[0]
    block_count = row_count // WINDOW
    kv_heads = key_ext.shape[1] // HEAD_DIM
    group_size = query_rows.shape[1] // (kv_heads * HEAD_DIM)

    def band(t):
        lower = t[:row_count].reshape((block_count, WINDOW) + t.shape[1:])
        upper = t[WINDOW:].reshape((block_count, WINDOW) + t.shape[1:])
        return jnp.concatenate([lower, upper], axis=1)

    query_band = query_rows.reshape(block_count, WINDOW, kv_heads, group_size, HEAD_DIM)
    key_band = band(key_ext).reshape(block_count, 2 * WINDOW, kv_heads, HEAD_DIM)
    value_band = band(value_ext).reshape(block_count, 2 * WINDOW, kv_heads, HEAD_DIM)
    doc_band = band(doc_ext)
    distance = jnp.arange(WINDOW)[:, None] + WINDOW - jnp.arange(2 * WINDOW)[None, :]
    in_window = (distance >= 0) & (distance < WINDOW)
    same_doc = doc_rows.reshape(block_count, WINDOW)[:, :, None] == doc_band[:, None, :]
    keep_mask = in_window[None] & same_doc
    scores = jnp.einsum(
        "nqhgd,nkhd->nhgqk", query_band, key_band, preferred_element_type=jnp.float32
    ) * HEAD_DIM ** (-0.5)
    scores = jnp.where(keep_mask[:, None, None], scores, -jnp.inf)
    sink_logit = sinks.reshape(kv_heads, group_size)[None, :, :, None, None]
    peak = jnp.maximum(jnp.max(scores, axis=-1, keepdims=True), sink_logit)
    expd = jnp.exp(scores - peak)
    probs = (expd / (jnp.sum(expd, axis=-1, keepdims=True) + jnp.exp(sink_logit - peak))).astype(
        jnp.bfloat16
    )
    mixed = jnp.einsum("nhgqk,nkhd->nqhgd", probs, value_band, preferred_element_type=jnp.float32)
    return mixed.astype(jnp.bfloat16).reshape(row_count, -1)


def convolve(ext_rows, doc_ext, taps):
    center = doc_ext[2:]
    same_one = (doc_ext[1:-1] == center)[:, None]
    same_two = (doc_ext[:-2] == center)[:, None]
    ext32 = ext_rows.astype(jnp.float32)
    result = taps[2] * ext32[2:]
    result = result + jnp.where(same_one, taps[1] * ext32[1:-1], 0.0)
    return result + jnp.where(same_two, taps[0] * ext32[:-2], 0.0)


def per_device(
    queries,
    keys,
    values,
    doc_ids,
    sinks,
    residual,
    out_weight,
    norm_gain,
    w_gate,
    w_value,
    conv_gate,
    conv_value,
    w_down,
):
    core = lax.axis_index("sp") % 2
    tp = lax.axis_index("tp")
    n_tp = lax.axis_size("tp")
    rows = doc_ids.shape[0]
    part_rows = rows // n_tp
    depth = w_gate.shape[0]
    width = residual.shape[1]
    half = width // 2
    part_index = [(tp + n_tp - d) % n_tp for d in range(n_tp)]

    gate_own = parity_gather(w_gate)
    value_own = ring_gather(w_value)
    down_t = w_down.T
    inner = down_t.shape[1] // 2
    low, high = down_t[:, :inner], down_t[:, inner:]
    kept_half = jnp.where(core == 0, low, high)
    came_half = core_swap(jnp.where(core == 0, high, low))
    even_piece = jnp.where(core == 0, kept_half, came_half)
    odd_piece = jnp.where(core == 0, came_half, kept_half)
    down_odd = parity_gather(odd_piece)
    down_even = parity_gather(even_piece)
    gate_far = core_swap(gate_own)
    value_far = core_swap(value_own)

    out_far = [turned(out_weight, "tp", d) for d in range(1, n_tp)]
    out_parts = [by_parity(t, depth) for t in [out_weight] + out_far]
    residual = by_parity(residual, depth)
    norm_gain = norm_gain.reshape(-1, 2, depth).swapaxes(0, 1).reshape(-1)
    docs_plus = doc_ids + 1
    prev_keys, prev_values, prev_docs = shifted(
        (keys[-WINDOW:], values[-WINDOW:], docs_plus[-WINDOW:]), "sp", 1
    )
    key_ext = jnp.concatenate([prev_keys, keys], axis=0)
    value_ext = jnp.concatenate([prev_values, values], axis=0)
    doc_ext = jnp.concatenate([prev_docs, docs_plus], axis=0)
    head_out = attend(queries, key_ext, value_ext, docs_plus, doc_ext, sinks)

    def rows_of(t, index):
        return lax.dynamic_slice_in_dim(t, index * part_rows, part_rows, 0)

    proj = jnp.dot(rows_of(head_out, tp), out_parts[0], preferred_element_type=jnp.float32)
    for d in range(1, n_tp):
        heads_far = turned(rows_of(head_out, (tp + d) % n_tp), "tp", d)
        proj = proj + jnp.dot(heads_far, out_parts[d], preferred_element_type=jnp.float32)
    mid = (residual.astype(jnp.float32) + proj).astype(jnp.bfloat16)
    mid32 = mid.astype(jnp.float32)
    normed = (
        mid32 * lax.rsqrt(jnp.mean(mid32 * mid32, axis=-1, keepdims=True) + 1e-06) * norm_gain
    ).astype(jnp.bfloat16)
    even, odd = normed[:, :half], normed[:, half:]
    own = [jnp.where(core == 0, even, odd)]
    far = [jnp.where(core == 0, odd, even)]
    for d in range(1, n_tp):
        own.append(turned(own[0], "tp", d))
        far.append(turned(far[0], "tp", d))

    def up(own, far, w_own, w_far):
        total = jnp.dot(own, w_own, preferred_element_type=jnp.float32)
        return (total + jnp.dot(far, w_far, preferred_element_type=jnp.float32)).astype(
            jnp.bfloat16
        )

    gate_parts = [up(o, f, gate_own, gate_far) for o, f in zip(own, far)]
    value_parts = [up(o, f, value_own, value_far) for o, f in zip(own, far)]

    conv_docs = jnp.concatenate([prev_docs[-2:], docs_plus], axis=0)
    part_docs = [
        lax.dynamic_slice_in_dim(conv_docs, i * part_rows, part_rows + 2, 0) for i in part_index
    ]

    def conv_parts(parts, taps):
        tails = [p[-2:] for p in parts]
        last = tails[0]
        for d in range(1, n_tp):
            last = jnp.where(part_index[d] == n_tp - 1, tails[d], last)
        prev = shifted(last, "sp", 1)
        result = []
        for d in range(n_tp):
            halo = jnp.where(part_index[d] == 0, prev, tails[(d + 1) % n_tp])
            result.append(
                convolve(jnp.concatenate([halo, parts[d]], axis=0), part_docs[d], taps)
            )
        return result

    gate_conv = conv_parts(gate_parts, conv_gate)
    value_conv = conv_parts(value_parts, conv_value)
    hidden = [
        (jax.nn.silu(g) * v).astype(jnp.bfloat16) for g, v in zip(gate_conv, value_conv)
    ]

    def down(units, w_t):
        return lax.dot_general(
            units, w_t, (((1,), (1,)), ((), ())), preferred_element_type=jnp.float32
        )

    own_units = [jnp.where(core == 0, h[:, :inner], h[:, inner:]) for h in hidden]
    far_units = [jnp.where(core == 0, h[:, inner:], h[:, :inner]) for h in hidden]

    def down_sums(w_own):
        w_far = core_swap(w_own)
        came = []
        for d in range(1, n_tp):
            sent = (down(own_units[d], w_own) + down(far_units[d], w_far)).astype(
                jnp.bfloat16
            )
            came.append(turned(sent, "tp", -d))
        kept = down(own_units[0], w_own) + down(far_units[0], w_far)
        for t in came:
            kept = kept + t.astype(jnp.float32)
        return kept

    odd_sum = down_sums(down_odd)
    even_sum = down_sums(down_even)
    sums = (even_sum, odd_sum)
    return finish(mid, sums, depth)


def mult(x, m):
    return x if isinstance(x, int) else pl.multiple_of(x, m)


def ring_chip(place, chips):
    odd = lax.div(place, chips // 2)
    return (1 - odd) * (2 * place) + odd * (2 * (chips - 1 - place) + 1)


def layer_kernel(
    n_sp,
    n_tp,
    queries,
    keys,
    values,
    docs,
    sinks,
    residual,
    out_weight,
    norm_gain,
    w_gate,
    w_value,
    conv_gate,
    conv_value,
    w_down,
    mid,
    wg,
    wv,
    wd,
    nrm,
    hid,
    pre,
    q_v,
    k_v,
    v_v,
    doc_v,
    doc_col,
    same_one,
    same_two,
    att,
    heads,
    ow,
    gain_v,
    cg_v,
    cv_v,
    send,
    came,
    own,
    local_sem,
    ring_send,
    ring_recv,
    sib_send,
    sib_recv,
    halo_send,
    halo_recv,
    ow_send,
    ow_recv,
    heads_send,
    heads_recv,
    nrm_send,
    nrm_recv,
    sum_send,
    sum_recv,
):
    sp = lax.axis_index("sp")
    tp = lax.axis_index("tp")
    chips = n_sp // 2
    core = lax.rem(sp, 2)
    chip = lax.div(sp, 2)
    odd = lax.rem(chip, 2)
    place = (1 - odd) * lax.div(chip, 2) + odd * (chips - 1 - lax.div(chip, 2))
    way = 1 - 2 * core
    down_sp = 2 * ring_chip(lax.rem(place + way + chips, chips), chips) + core
    up_sp = 2 * ring_chip(lax.rem(place - way + chips, chips), chips) + core
    sib_sp = sp + way
    next_sp = lax.rem(sp + 1, n_sp)
    prev_sp = lax.rem(sp + n_sp - 1, n_sp)

    rows, q_width = queries.shape
    part = rows // n_tp
    depth, units = w_gate.shape
    width = residual.shape[1]
    kv_heads = keys.shape[1] // HEAD_DIM
    group = q_width // keys.shape[1]
    blocks = rows // WINDOW
    part_blocks = part // WINDOW
    ow_half = q_width // 2
    unit_tiles = units // TILE
    events = (chips - 1) * SUB

    def peer(d):
        return lax.rem(tp + d, n_tp)

    def held(h):
        return 2 * ring_chip(lax.rem(place - way * h + chips, chips), chips) + core

    def sib_held(h):
        return 2 * ring_chip(lax.rem(place + way * h + chips, chips), chips) + 1 - core

    def piece(w, j, s):
        size = depth // SUB
        return (wg, wv, wd)[w].at[pl.ds(mult(j * depth + s * size, size), size), :]

    def own_piece(w, s):
        if w == 2:
            return piece(2, sp, s)
        size = depth // SUB
        return (w_gate, w_value)[w].at[pl.ds(s * size, size), :]

    def remote(src, dst, send_sem, recv_sem, device):
        return pltpu.make_async_remote_copy(
            src_ref=src,
            dst_ref=dst,
            send_sem=send_sem,
            recv_sem=recv_sem,
            device_id=device,
            device_id_type=MESH,
        )

    def ring_copy(w, h, s, src=None):
        dst = piece(w, held(h - 1), s)
        return remote(
            dst if src is None else src,
            dst,
            ring_send.at[w],
            ring_recv.at[w, h - 1, s],
            (down_sp, tp),
        )

    def ring_wait(w, h, s):
        dst = piece(w, held(h), s)
        remote(
            dst, dst, ring_send.at[w], ring_recv.at[w, h - 1, s], (down_sp, tp)
        ).wait_recv()

    def sib_sem(w, h, s):
        if w < 2:
            return sib_recv.at[w]
        late = lax.div(h, chips - 1) * (s // (SUB // 2) if isinstance(s, int) else lax.div(s, SUB // 2))
        return sib_recv.at[2 + h + late]

    def sib_copy(w, h, s, src=None):
        dst = piece(w, held(h), s)
        return remote(
            dst if src is None else src, dst, sib_send.at[w], sib_sem(w, h, s), (sib_sp, tp)
        )

    def sib_wait(w, h, part_of=None):
        buf = (wg, wv, wd)[w]
        if w < 2:
            got = buf.at[pl.ds(0, chips * depth), :]
        elif part_of is None:
            got = buf.at[pl.ds(mult(sib_held(h) * depth, depth), depth), :]
        else:
            got = last_half(sib_held(h), part_of)
        sem = sib_sem(w, h, 0 if part_of is None else part_of * (SUB // 2))
        remote(got, got, sib_send.at[w], sem, (sib_sp, tp)).wait_recv()

    def last_half(j, part_of):
        return wd.at[pl.ds(mult(j * depth + part_of * (depth // 2), depth // 2), depth // 2), :]

    def sent_weights(w):
        buf = (wg, wv, wd)[w]
        ring = buf.at[pl.ds(0, (chips - 1) * depth), :]
        swapped = buf.at[pl.ds(0, chips * depth), :]
        remote(ring, ring, ring_send.at[w], ring_recv.at[w, 0, 0], (down_sp, tp)).wait_send()
        remote(swapped, swapped, sib_send.at[w], sib_recv.at[w], (sib_sp, tp)).wait_send()

    def start_own(w):
        for s in range(SUB):
            ring_copy(w, 1, s, own_piece(w, s)).start()
        for s in range(SUB):
            sib_copy(w, 0, s, own_piece(w, s)).start()

    def service(w, e):
        h = 1 + (e // SUB if isinstance(e, int) else lax.div(e, SUB))
        s = e % SUB if isinstance(e, int) else lax.rem(e, SUB)
        ring_wait(w, h, s)
        if isinstance(e, int):
            if h < chips - 1:
                ring_copy(w, h + 1, s).start()
        else:

            @pl.when(h < chips - 1)
            def _():
                ring_copy(w, h + 1, s).start()

        sib_copy(w, h, s).start()
        if w < 2:

            @pl.when(e == (chips - 2) * SUB - 1)
            def _():
                start_own(w + 1)

    def serve(w, first, last):
        if last > first:

            @pl.loop(first, last)
            def _(e):
                service(w, e)

    local = [
        (keys, k_v.at[pl.ds(WINDOW, rows), :]),
        (values, v_v.at[pl.ds(WINDOW, rows), :]),
        (docs, doc_v.at[pl.ds(8, blocks), :]),
        (queries, q_v),
        (residual, mid),
        (out_weight, ow.at[tp]),
        (norm_gain, gain_v),
        (conv_gate, cg_v),
        (conv_value, cv_v),
        (w_gate, wg.at[pl.ds(mult(sp * depth, depth), depth), :]),
        (w_value, wv.at[pl.ds(mult(sp * depth, depth), depth), :]),
    ]
    strips = [(c, min(rows, units - c * rows)) for c in range(-(-units // rows))]
    local += [
        (
            w_down.at[pl.ds(c * rows, length), :],
            hid.at[pl.ds(0, length), pl.ds(c * depth, depth)],
        )
        for c, length in strips
    ]
    local = [
        pltpu.make_async_copy(src, dst, local_sem.at[i]) for i, (src, dst) in enumerate(local)
    ]
    for copy in local[:4]:
        copy.start()

    nrm[0:HALO, :] = jnp.zeros((HALO, width), jnp.bfloat16)
    barrier = pltpu.get_barrier_semaphore()
    greeted = [(down_sp, tp), (up_sp, tp), (sib_sp, tp), (next_sp, tp), (prev_sp, tp)]
    greeted += [(sp, peer(d)) for d in range(1, n_tp)]
    for device in greeted:
        pl.semaphore_signal(barrier, inc=1, device_id=device, device_id_type=MESH)
    pl.semaphore_wait(barrier, len(greeted))

    halos = [
        (keys.at[pl.ds(rows - WINDOW, WINDOW), :], k_v.at[pl.ds(0, WINDOW), :]),
        (values.at[pl.ds(rows - WINDOW, WINDOW), :], v_v.at[pl.ds(0, WINDOW), :]),
        (docs.at[pl.ds(blocks - 1, 1), :], doc_v.at[pl.ds(7, 1), :]),
    ]
    halos = [
        remote(src, dst, halo_send.at[i], halo_recv.at[i], (next_sp, tp))
        for i, (src, dst) in enumerate(halos)
    ]
    for copy in halos:
        copy.start()
    start_own(0)

    def ow_rows(t, c):
        return ow.at[t, pl.ds(mult(c * ow_half, ow_half), ow_half), :]

    ow_src = out_weight.at[pl.ds(mult(core * ow_half, ow_half), ow_half), :]
    ow_out = [
        remote(ow_src, ow_rows(tp, core), ow_send.at[0, d - 1], ow_recv.at[0, d - 1], (sp, peer(n_tp - d)))
        for d in range(1, n_tp)
    ]
    for copy in ow_out:
        copy.start()
    for copy in local[4:]:
        copy.start()

    for i in range(3):
        local[i].wait()
    for copy in halos:
        copy.wait_recv()
    local[3].wait()

    lane = lax.broadcasted_iota(jnp.int32, (WINDOW, 2 * HEAD_DIM), 1)
    low_lane = lane < HEAD_DIM
    doc_v[7:8, :] = jnp.where(sp == 0, -1, doc_v[7:8, :])
    for b in range(-1, blocks):
        row = doc_v[8 + b : 9 + b, :]
        column = jnp.broadcast_to(row, (WINDOW, WINDOW)).T
        if b < 0:
            doc_col[0:8, :] = column[WINDOW - 8 :, :]
        else:
            doc_col[8 + b * WINDOW : 8 + (b + 1) * WINDOW, :] = column
    for b in range(blocks):
        at = 8 + b * WINDOW
        here = doc_col[at : at + WINDOW, :]
        back_one = doc_col[at - 1 : at - 1 + WINDOW, :]
        back_two = doc_col[at - 2 : at - 2 + WINDOW, :]
        to = slice(b * WINDOW, (b + 1) * WINDOW)
        same_one[to, :] = jnp.where(here == back_one, 1.0, 0.0)
        same_two[to, :] = jnp.where(here == back_two, 1.0, 0.0)

    q_index = lax.broadcasted_iota(jnp.int32, (WINDOW, 2 * WINDOW), 0)
    k_index = lax.broadcasted_iota(jnp.int32, (WINDOW, 2 * WINDOW), 1)
    first_rows = lax.broadcasted_iota(jnp.int32, (2 * WINDOW, 1), 0) < WINDOW

    def attend_block(b):
        base = mult(b * WINDOW, WINDOW)
        key_docs = jnp.concatenate([doc_v[pl.ds(7 + b, 1), :], doc_v[pl.ds(8 + b, 1), :]], axis=1)
        here = doc_col[pl.ds(mult(8 + base, 8), WINDOW), :]
        keep = (k_index > q_index) & (k_index <= q_index + WINDOW)
        keep = keep & (jnp.concatenate([here, here], axis=1) == key_docs)
        keep = jnp.concatenate([keep, keep], axis=0)
        k_band = k_v[pl.ds(base, 2 * WINDOW), :]
        v_band = v_v[pl.ds(base, 2 * WINDOW), :]
        for g in range(kv_heads):
            at = slice(g * HEAD_DIM, (g + 1) * HEAD_DIM)
            kk = jnp.concatenate([k_band[:, at], k_band[:, at]], axis=1)
            vv = jnp.concatenate([v_band[:, at], v_band[:, at]], axis=1)
            for pair in range(group // 2):
                head = g * group + 2 * pair
                lanes = slice(head * HEAD_DIM, (head + 2) * HEAD_DIM)
                both = q_v[pl.ds(base, WINDOW), lanes]
                zero = jnp.zeros_like(both)
                split = jnp.concatenate(
                    [jnp.where(low_lane, both, zero), jnp.where(low_lane, zero, both)], axis=0
                )
                scores = lax.dot_general(
                    split, kk, (((1,), (1,)), ((), ())), preferred_element_type=jnp.float32
                ) * HEAD_DIM ** (-0.5)
                scores = jnp.where(keep, scores, -1e30)
                sink = jnp.where(first_rows, sinks[head], sinks[head + 1])
                peak = jnp.maximum(jnp.max(scores, axis=1, keepdims=True), sink)
                expd = jnp.exp(scores - peak)
                total = jnp.sum(expd, axis=1, keepdims=True) + jnp.exp(sink - peak)
                probs = (expd * (1.0 / total)).astype(jnp.bfloat16)
                mixed = jnp.dot(probs, vv, preferred_element_type=jnp.float32)
                att[pl.ds(base, WINDOW), lanes] = jnp.where(
                    low_lane, mixed[:WINDOW], mixed[WINDOW:]
                ).astype(jnp.bfloat16)

    def due(share):
        return events * share // 28

    def attend_blocks(first, count, e, share):
        @pl.loop(0, count)
        def _(i):
            attend_block(lax.rem(first + i, blocks))
            before = lax.div(i * share, count)

            @pl.when(lax.div((i + 1) * share, count) > before)
            def _():
                service(0, e + before)

    far_share = min(due(2), blocks - part_blocks)
    own_share = min(due(3), part_blocks)
    attend_blocks((tp + 1) * part_blocks, blocks - part_blocks, 0, far_share)
    attend_blocks(tp * part_blocks, part_blocks, far_share, own_share)
    heads_out = [
        remote(
            att.at[pl.ds(mult(peer(n_tp - d) * part, part), part), :],
            heads.at[d - 1],
            heads_send.at[d - 1],
            heads_recv.at[d - 1],
            (sp, peer(n_tp - d)),
        )
        for d in range(1, n_tp)
    ]
    for copy in heads_out:
        copy.start()
    for copy in local[9:]:
        copy.wait()
    own_rows = pl.ds(mult(sp * depth, depth), depth)
    for c, length in strips:
        for at in range(0, length, TILE):
            turned_piece = hid[at : at + TILE, c * depth : (c + 1) * depth].astype(jnp.float32).T
            to = slice(c * rows + at, c * rows + at + TILE)
            wd[own_rows, to] = turned_piece.astype(jnp.bfloat16)
    before_proj = due(16)
    serve(0, far_share + own_share, before_proj)

    for i in range(4, 9):
        local[i].wait()
    ow_on = []
    for d in range(1, n_tp):
        got = ow_rows(peer(d), core)
        remote(got, got, ow_send.at[0, d - 1], ow_recv.at[0, d - 1], (sp, peer(n_tp - d))).wait_recv()
        copy = remote(got, got, ow_send.at[1, d - 1], ow_recv.at[1, d - 1], (sib_sp, tp))
        copy.start()
        ow_on.append(copy)
    for d in range(1, n_tp):
        got = ow_rows(peer(d), 1 - core)
        remote(got, got, ow_send.at[1, d - 1], ow_recv.at[1, d - 1], (sib_sp, tp)).wait_recv()
        heads_out[d - 1].wait_recv()

    part_base = tp * part

    def nrm_rows(t, i):
        return nrm.at[pl.ds(mult(HALO + t * part + i * WINDOW, HALO), WINDOW), :]

    def nrm_copy(i, d):
        at = nrm_rows(tp, i)
        return remote(at, at, nrm_send.at[0], nrm_recv.at[i, d - 1], (sp, peer(n_tp - d)))

    def project(i):
        at = pl.ds(mult(i * WINDOW, WINDOW), WINDOW)
        mine = att[pl.ds(mult(part_base + i * WINDOW, WINDOW), WINDOW), :]
        proj = jnp.dot(mine, ow[tp], preferred_element_type=jnp.float32)
        for d in range(1, n_tp):
            proj = proj + jnp.dot(
                heads[d - 1, at, :], ow[peer(d)], preferred_element_type=jnp.float32
            )
        rounded = (mid[at, :].astype(jnp.float32) + proj).astype(jnp.bfloat16)
        mid[at, :] = rounded
        wide = rounded.astype(jnp.float32)
        scale = lax.rsqrt(jnp.mean(wide * wide, axis=1, keepdims=True) + 1e-06)
        normed = (wide * scale * gain_v[...]).astype(jnp.bfloat16)
        nrm[pl.ds(mult(HALO + part_base + i * WINDOW, HALO), WINDOW), :] = normed

    @pl.loop(0, part_blocks)
    def _(k):
        i = part_blocks - 1 - k
        project(i)
        for d in range(1, n_tp):

            @pl.when(k > 0)
            def _():
                nrm_copy(i + 1, d).start()

        @pl.when(before_proj + k < events)
        def _():
            service(0, before_proj + k)

    for d in range(1, n_tp):
        nrm_copy(0, d).start()

    after_proj = min(events, before_proj + part_blocks)
    serve(0, after_proj, events)
    early_value = due(14)

    def nrm_wait(i):
        for d in range(1, n_tp):
            got = nrm_rows(peer(d), i)
            remote(
                got, got, nrm_send.at[0], nrm_recv.at[i, d - 1], (sp, peer(n_tp - d))
            ).wait_recv()

    nrm_wait(part_blocks - 1)
    nrm_halo = remote(
        nrm.at[pl.ds(HALO + rows - REACH, REACH), :],
        nrm.at[pl.ds(HALO - REACH, REACH), :],
        halo_send.at[3],
        halo_recv.at[3],
        (next_sp, tp),
    )
    nrm_halo.start()
    serve(1, 0, early_value)
    pl.loop(0, part_blocks - 1)(nrm_wait)

    sib_wait(0, 0)
    for copy in halos + heads_out + ow_out + ow_on + [nrm_halo]:
        copy.wait_send()

    sent_rows = nrm.at[pl.ds(0, (n_tp - 1) * part), :]
    remote(sent_rows, sent_rows, nrm_send.at[0], nrm_recv.at[0, 0], (sp, peer(1))).wait_send()

    nrm_halo.wait_recv()

    def up_tile(w_ref, taps, n, base, lengths):
        cols = pl.ds(mult(n * TILE, TILE), TILE)
        at = 0
        for length in lengths:
            lhs = nrm[pl.ds(mult(base + at, HALO), length), :]
            pre[at : at + length, :] = (
                jnp.dot(lhs, w_ref[:, cols], preferred_element_type=jnp.float32)
                .astype(jnp.bfloat16)
                .astype(jnp.float32)
            )
            at += length
        tap = taps[:, cols]
        for b in range((at - HALO) // WINDOW):
            at = HALO + b * WINDOW
            to = pl.ds(mult(base + b * WINDOW, WINDOW), WINDOW)
            one = jnp.concatenate([same_one[to, :]] * (TILE // WINDOW), axis=1)
            two = jnp.concatenate([same_two[to, :]] * (TILE // WINDOW), axis=1)
            conv = tap[2:3] * pre[at : at + WINDOW, :]
            conv = conv + one * (tap[1:2] * pre[at - 1 : at - 1 + WINDOW, :])
            conv = conv + two * (tap[0:1] * pre[at - 2 : at - 2 + WINDOW, :])
            yield to, cols, conv

    def spread(w, first, count, i):
        before = lax.div(i * count, unit_tiles)
        after = lax.div((i + 1) * count, unit_tiles)

        @pl.when(after > before)
        def _():
            service(w, first + before)

    gate_count = min(unit_tiles, events - early_value)

    @pl.loop(0, unit_tiles)
    def _(n):
        lengths = (HALO + rows // 2, rows // 2)
        for to, cols, conv in up_tile(wg, cg_v, n, 0, lengths):
            hid[to, cols] = (conv / (1.0 + jnp.exp(-conv))).astype(jnp.bfloat16)
        spread(1, early_value, gate_count, n)

    serve(1, early_value + gate_count, events)
    sib_wait(1, 0)

    def value_part(t, first, count):
        @pl.loop(0, unit_tiles)
        def _(n):
            for to, cols, conv in up_tile(wv, cv_v, n, t * part, (HALO + part,)):
                hid[to, cols] = (hid[to, cols].astype(jnp.float32) * conv).astype(
                    jnp.bfloat16
                )
            spread(2, first, count, n)

    def sum_copy(h, d, half=None):
        src, dst, sem = send.at[h, d - 1], came.at[h, d - 1], h
        if half is not None:
            lanes = slice(half * depth, (half + 1) * depth)
            src, dst, sem = src.at[:, lanes], dst.at[:, lanes], h + half
        return remote(src, dst, sum_send.at[0], sum_recv.at[sem, d - 1], (sp, peer(d)))

    def hop_cols(h, c):
        j = held(h) if c == 0 else sib_held(h)
        return pl.ds(mult(j * depth, depth), depth)

    def add_up(h, c, parts):
        cols = hop_cols(h, c)
        total = own[h, :, c * depth : (c + 1) * depth] + mid[:, cols].astype(jnp.float32)
        for t in parts:
            total = total + t.astype(jnp.float32)
        mid[:, cols] = total.astype(jnp.bfloat16)

    def finish_hop(h):
        for d in range(1, n_tp):
            sum_copy(h, d).wait_recv()
        for c in range(2):
            lanes = slice(c * depth, (c + 1) * depth)
            add_up(h, c, [came[h, d - 1, :, lanes] for d in range(1, n_tp)])

    def finish_last():
        h = chips - 1
        for half in range(2):
            for d in range(1, n_tp):
                sum_copy(h, d, half).wait_recv()
        for c in range(2):
            lo = c * (depth // 2)
            pairs = [
                [came[h, d - 1, :, at + lo : at + lo + depth // 2] for at in (0, depth)]
                for d in range(1, n_tp)
            ]
            add_up(h, c, [jnp.concatenate(pair, axis=1) for pair in pairs])

    def apart(step):
        pl.when(sp >= 0)(step)

    def down_rows(rhs, t):
        lhs = hid[pl.ds(mult(t * part, part), part), :]
        return lax.dot_general(
            lhs, rhs, (((1,), (1,)), ((), ())), preferred_element_type=jnp.float32
        )

    def hop_rows(h):
        return jnp.concatenate(
            [wd[pl.ds(mult(j * depth, depth), depth), :] for j in (held(h), sib_held(h))], axis=0
        )

    def down_far(h):
        sib_wait(2, h)
        for d in range(1, n_tp):

            @apart
            def _():
                send[h, d - 1] = down_rows(hop_rows(h), peer(d)).astype(jnp.bfloat16)

    def down_own(h):
        @apart
        def _():
            own[h] = down_rows(hop_rows(h), tp)

    def down_far_half(half):
        h = chips - 1
        sib_wait(2, h, half)

        def rhs():
            return jnp.concatenate(
                [last_half(j, half)[...] for j in (held(h), sib_held(h))], axis=0
            )

        lanes = slice(half * depth, (half + 1) * depth)
        for d in range(1, n_tp):

            @apart
            def _():
                send[h, d - 1, :, lanes] = down_rows(rhs(), peer(d)).astype(jnp.bfloat16)

    def send_sums(h, half=None):
        for d in range(1, n_tp):
            sum_copy(h, d, half).start()

    served = due(5)
    for d in range(1, n_tp):
        value_part(peer(d), 0, served if d == 1 else 0)

    @pl.loop(0, EARLY)
    def _(h):
        down_far(h)
        for i in range(due(1)):
            service(2, served + h * due(1) + i)
        send_sums(h)

    served += EARLY * due(1)
    more = due(6)
    value_part(tp, served, more)
    served += more

    @pl.loop(EARLY, chips - 1)
    def _(h):
        for s in range(SUB):

            @pl.when((h - 1) * SUB + s >= served)
            def _():
                service(2, (h - 1) * SUB + s)

        down_far(h)

        @pl.when(h > EARLY)
        def _():
            finish_hop(h - EARLY - 1)

        for w in range(2):

            @pl.when(h == EARLY + w)
            def _():
                sent_weights(w)

        send_sums(h)
        down_own(h - EARLY)

    last = chips - 1
    for half in range(2):
        for s in range(SUB // 2):
            service(2, (last - 1) * SUB + half * (SUB // 2) + s)
        down_far_half(half)
        finish_hop(last - EARLY - 1 + half)
        send_sums(last, half)
        down_own(last - EARLY + half)
    for h in range(last - EARLY + 2, chips):
        down_own(h)
    for h in range(last - EARLY + 1, last):
        finish_hop(h)
    finish_last()

    sent_weights(2)

    remote(send, send, sum_send.at[0], sum_recv.at[0, 0], (sp, peer(1))).wait_send()


def whole_layer(n_sp, n_tp, queries, keys, values, doc_ids, sinks, residual, out_weight,
                norm_gain, w_gate, w_value, conv_gate, conv_value, w_down):
    rows, q_width = queries.shape
    kv_width = keys.shape[1]
    part, width = residual.shape
    depth, units = w_gate.shape
    chips = n_sp // 2
    bf16, f32 = jnp.bfloat16, jnp.float32
    dma = pltpu.SemaphoreType.DMA
    part_blocks = part // WINDOW
    scratch = [
        pltpu.VMEM((width, units), bf16),
        pltpu.VMEM((width, units), bf16),
        pltpu.VMEM((width, units), bf16),
        pltpu.VMEM((HALO + rows, width), bf16),
        pltpu.VMEM((rows, units), bf16),
        pltpu.VMEM((HALO + rows, TILE), f32),
        pltpu.VMEM((rows, q_width), bf16),
        pltpu.VMEM((WINDOW + rows, kv_width), bf16),
        pltpu.VMEM((WINDOW + rows, kv_width), bf16),
        pltpu.VMEM((8 + rows // WINDOW, WINDOW), jnp.int32),
        pltpu.VMEM((8 + rows, WINDOW), jnp.int32),
        pltpu.VMEM((rows, WINDOW), f32),
        pltpu.VMEM((rows, WINDOW), f32),
        pltpu.VMEM((rows, q_width), bf16),
        pltpu.VMEM((n_tp - 1, part, q_width), bf16),
        pltpu.VMEM((n_tp, q_width, width), bf16),
        pltpu.VMEM((1, width), f32),
        pltpu.VMEM((3, units), f32),
        pltpu.VMEM((3, units), f32),
        pltpu.VMEM((chips, n_tp - 1, part, 2 * depth), bf16),
        pltpu.VMEM((chips, n_tp - 1, part, 2 * depth), bf16),
        pltpu.VMEM((chips, part, 2 * depth), f32),
        dma((11 - (-units // rows),)),
        dma((3,)),
        dma((3, chips - 1, SUB)),
        dma((3,)),
        dma((chips + 3,)),
        dma((4,)),
        dma((4,)),
        dma((2, n_tp - 1)),
        dma((2, n_tp - 1)),
        dma((n_tp - 1,)),
        dma((n_tp - 1,)),
        dma((1,)),
        dma((part_blocks, n_tp - 1)),
        dma((1,)),
        dma((chips + 1, n_tp - 1)),
    ]
    any_spec = pl.BlockSpec(memory_space=pl.ANY)
    specs = [any_spec] * 13
    specs[4] = pl.BlockSpec(memory_space=pltpu.SMEM)
    return pl.pallas_call(
        functools.partial(layer_kernel, n_sp, n_tp),
        out_shape=pltpu.VMEM(residual.shape, residual.dtype),
        in_specs=specs,
        out_specs=pl.BlockSpec(memory_space=pltpu.VMEM),
        scratch_shapes=scratch,
        compiler_params=pltpu.CompilerParams(
            collective_id=0, has_side_effects=True, vmem_limit_bytes=VMEM_BYTES
        ),
    )(
        queries,
        keys,
        values,
        doc_ids.reshape(rows // WINDOW, WINDOW),
        sinks,
        residual,
        out_weight,
        norm_gain.reshape(1, width),
        w_gate,
        w_value,
        conv_gate,
        conv_value,
        w_down,
    )


def in_one_kernel(n_sp, n_tp, queries, keys, values, doc_ids, *weights):
    w_gate = weights[4]
    depth, units = w_gate.shape
    aligned = depth % 128 == 0 and keys.shape[1] % 128 == 0 and units % TILE == 0
    return aligned and n_sp % 4 == 0 and n_tp > 1 and doc_ids.shape[0] % (n_tp * WINDOW) == 0


def solution(mesh):
    n_sp, n_tp = mesh.shape["sp"], mesh.shape["tp"]

    def body(*args):
        if in_one_kernel(n_sp, n_tp, *args):
            return whole_layer(n_sp, n_tp, *args)
        return per_device(*args)

    return jax.shard_map(
        body,
        mesh=mesh,
        in_specs=(
            P("sp", "tp"),
            P("sp", "tp"),
            P("sp", "tp"),
            P("sp"),
            P("tp"),
            P(("sp", "tp"), None),
            P("tp", None),
            P(),
            P("sp", "tp"),
            P("sp", "tp"),
            P(None, "tp"),
            P(None, "tp"),
            P("tp", "sp"),
        ),
        out_specs=P(("sp", "tp"), None),
        check_vma=False,
    )
```

```python
import functools

import jax
import jax.numpy as jnp
from jax import lax
from jax.experimental import pallas as pl
from jax.experimental.pallas import tpu as pltpu
from jax.sharding import PartitionSpec as P


HEAD_DIM = 64
WINDOW = 128
ROW_TILE = 128
SUB = 4
EARLY = 2
HALO = 16
REACH = 2
TILE = 256
VMEM_BYTES = 67043328
MESH = pl.DeviceIdType.MESH


def shifted(shard, axis, by):
    size = lax.axis_size(axis)
    pairs = [(i, i + by) for i in range(size) if 0 <= i + by < size]
    return lax.ppermute(shard, axis, pairs)


def turned(t, axis, by):
    size = lax.axis_size(axis)
    return lax.ppermute(t, axis, [(i, (i + by) % size) for i in range(size)])


def core_swap(t):
    size = lax.axis_size("sp")
    return lax.ppermute(t, "sp", [(i, i ^ 1) for i in range(size)])


def parity_gather(t):
    size = lax.axis_size("sp")
    groups = [list(range(0, size, 2)), list(range(1, size, 2))]
    return lax.all_gather(t, "sp", axis=0, tiled=True, axis_index_groups=groups)


def ring_gather(t):
    chips = lax.axis_size("sp") // 2
    order = list(range(0, chips, 2)) + list(range(1, chips, 2))[::-1]
    chip = lax.axis_index("sp") // 2
    place = jnp.where(chip % 2 == 0, chip // 2, chips - 1 - chip // 2)

    def hop(piece, by):
        pairs = [
            (2 * order[k] + c, 2 * order[(k + by) % chips] + c)
            for k in range(chips)
            for c in range(2)
        ]
        return lax.ppermute(piece, "sp", pairs)

    def chip_at(k):
        k = (k + chips) % chips
        return jnp.where(k < chips // 2, 2 * k, 2 * (chips - 1 - k) + 1)

    depth = t.shape[0]
    pieces = [(chip, t)]
    up = down = t
    for step in range(1, chips // 2 + 1):
        up = hop(up, 1)
        pieces.append((chip_at(place - step), up))
        if step < chips - step:
            down = hop(down, -1)
            pieces.append((chip_at(place + step), down))
    whole = jnp.zeros((chips * depth,) + t.shape[1:], t.dtype)
    for at, piece in pieces:
        whole = lax.dynamic_update_slice_in_dim(whole, piece, at * depth, 0)
    return whole


def by_parity(t, depth):
    rows, width = t.shape
    blocks = width // depth
    tile = min(ROW_TILE, rows)

    def kernel(in_ref, out_ref):
        for j in range(blocks):
            to = (j // 2 + (j % 2) * (blocks // 2)) * depth
            out_ref[:, to : to + depth] = in_ref[:, j * depth : (j + 1) * depth]

    return pl.pallas_call(
        kernel,
        out_shape=jax.ShapeDtypeStruct(t.shape, t.dtype),
        grid=(rows // tile,),
        in_specs=[pl.BlockSpec((tile, width), lambda i: (i, 0))],
        out_specs=pl.BlockSpec((tile, width), lambda i: (i, 0)),
        cost_estimate=pl.CostEstimate(
            flops=0, bytes_accessed=2 * t.size * t.dtype.itemsize, transcendentals=0
        ),
    )(t)


def finish(mid, sums, depth):
    rows, width = mid.shape
    blocks = width // depth
    tile = min(ROW_TILE, rows)

    def kernel(mid_ref, even_ref, odd_ref, out_ref):
        for j in range(blocks):
            at = (j // 2) * depth
            held = at + (j % 2) * (width // 2)
            sum_ref = odd_ref if j % 2 else even_ref
            out_ref[:, j * depth : (j + 1) * depth] = (
                mid_ref[:, held : held + depth].astype(jnp.float32)
                + sum_ref[:, at : at + depth]
            ).astype(out_ref.dtype)

    half_spec = pl.BlockSpec((tile, width // 2), lambda i: (i, 0))
    return pl.pallas_call(
        kernel,
        out_shape=jax.ShapeDtypeStruct(mid.shape, mid.dtype),
        grid=(rows // tile,),
        in_specs=[pl.BlockSpec((tile, width), lambda i: (i, 0)), half_spec, half_spec],
        out_specs=pl.BlockSpec((tile, width), lambda i: (i, 0)),
        cost_estimate=pl.CostEstimate(
            flops=mid.size, bytes_accessed=8 * mid.size, transcendentals=0
        ),
    )(mid, *sums)


def attend(query_rows, key_ext, value_ext, doc_rows, doc_ext, sinks):
    row_count = query_rows.shape[0]
    block_count = row_count // WINDOW
    kv_heads = key_ext.shape[1] // HEAD_DIM
    group_size = query_rows.shape[1] // (kv_heads * HEAD_DIM)

    def band(t):
        lower = t[:row_count].reshape((block_count, WINDOW) + t.shape[1:])
        upper = t[WINDOW:].reshape((block_count, WINDOW) + t.shape[1:])
        return jnp.concatenate([lower, upper], axis=1)

    query_band = query_rows.reshape(block_count, WINDOW, kv_heads, group_size, HEAD_DIM)
    key_band = band(key_ext).reshape(block_count, 2 * WINDOW, kv_heads, HEAD_DIM)
    value_band = band(value_ext).reshape(block_count, 2 * WINDOW, kv_heads, HEAD_DIM)
    doc_band = band(doc_ext)
    distance = jnp.arange(WINDOW)[:, None] + WINDOW - jnp.arange(2 * WINDOW)[None, :]
    in_window = (distance >= 0) & (distance < WINDOW)
    same_doc = doc_rows.reshape(block_count, WINDOW)[:, :, None] == doc_band[:, None, :]
    keep_mask = in_window[None] & same_doc
    scores = jnp.einsum(
        "nqhgd,nkhd->nhgqk", query_band, key_band, preferred_element_type=jnp.float32
    ) * HEAD_DIM ** (-0.5)
    scores = jnp.where(keep_mask[:, None, None], scores, -jnp.inf)
    sink_logit = sinks.reshape(kv_heads, group_size)[None, :, :, None, None]
    peak = jnp.maximum(jnp.max(scores, axis=-1, keepdims=True), sink_logit)
    expd = jnp.exp(scores - peak)
    probs = (expd / (jnp.sum(expd, axis=-1, keepdims=True) + jnp.exp(sink_logit - peak))).astype(
        jnp.bfloat16
    )
    mixed = jnp.einsum("nhgqk,nkhd->nqhgd", probs, value_band, preferred_element_type=jnp.float32)
    return mixed.astype(jnp.bfloat16).reshape(row_count, -1)


def convolve(ext_rows, doc_ext, taps):
    center = doc_ext[2:]
    same_one = (doc_ext[1:-1] == center)[:, None]
    same_two = (doc_ext[:-2] == center)[:, None]
    ext32 = ext_rows.astype(jnp.float32)
    result = taps[2] * ext32[2:]
    result = result + jnp.where(same_one, taps[1] * ext32[1:-1], 0.0)
    return result + jnp.where(same_two, taps[0] * ext32[:-2], 0.0)


def per_device(
    queries,
    keys,
    values,
    doc_ids,
    sinks,
    residual,
    out_weight,
    norm_gain,
    w_gate,
    w_value,
    conv_gate,
    conv_value,
    w_down,
):
    core = lax.axis_index("sp") % 2
    tp = lax.axis_index("tp")
    n_tp = lax.axis_size("tp")
    rows = doc_ids.shape[0]
    part_rows = rows // n_tp
    depth = w_gate.shape[0]
    width = residual.shape[1]
    half = width // 2
    part_index = [(tp + n_tp - d) % n_tp for d in range(n_tp)]

    gate_own = parity_gather(w_gate)
    value_own = ring_gather(w_value)
    down_t = w_down.T
    inner = down_t.shape[1] // 2
    low, high = down_t[:, :inner], down_t[:, inner:]
    kept_half = jnp.where(core == 0, low, high)
    came_half = core_swap(jnp.where(core == 0, high, low))
    even_piece = jnp.where(core == 0, kept_half, came_half)
    odd_piece = jnp.where(core == 0, came_half, kept_half)
    down_odd = parity_gather(odd_piece)
    down_even = parity_gather(even_piece)
    gate_far = core_swap(gate_own)
    value_far = core_swap(value_own)

    out_far = [turned(out_weight, "tp", d) for d in range(1, n_tp)]
    out_parts = [by_parity(t, depth) for t in [out_weight] + out_far]
    residual = by_parity(residual, depth)
    norm_gain = norm_gain.reshape(-1, 2, depth).swapaxes(0, 1).reshape(-1)
    docs_plus = doc_ids + 1
    prev_keys, prev_values, prev_docs = shifted(
        (keys[-WINDOW:], values[-WINDOW:], docs_plus[-WINDOW:]), "sp", 1
    )
    key_ext = jnp.concatenate([prev_keys, keys], axis=0)
    value_ext = jnp.concatenate([prev_values, values], axis=0)
    doc_ext = jnp.concatenate([prev_docs, docs_plus], axis=0)
    head_out = attend(queries, key_ext, value_ext, docs_plus, doc_ext, sinks)

    def rows_of(t, index):
        return lax.dynamic_slice_in_dim(t, index * part_rows, part_rows, 0)

    proj = jnp.dot(rows_of(head_out, tp), out_parts[0], preferred_element_type=jnp.float32)
    for d in range(1, n_tp):
        heads_far = turned(rows_of(head_out, (tp + d) % n_tp), "tp", d)
        proj = proj + jnp.dot(heads_far, out_parts[d], preferred_element_type=jnp.float32)
    mid = (residual.astype(jnp.float32) + proj).astype(jnp.bfloat16)
    mid32 = mid.astype(jnp.float32)
    normed = (
        mid32 * lax.rsqrt(jnp.mean(mid32 * mid32, axis=-1, keepdims=True) + 1e-06) * norm_gain
    ).astype(jnp.bfloat16)
    even, odd = normed[:, :half], normed[:, half:]
    own = [jnp.where(core == 0, even, odd)]
    far = [jnp.where(core == 0, odd, even)]
    for d in range(1, n_tp):
        own.append(turned(own[0], "tp", d))
        far.append(turned(far[0], "tp", d))

    def up(own, far, w_own, w_far):
        total = jnp.dot(own, w_own, preferred_element_type=jnp.float32)
        return (total + jnp.dot(far, w_far, preferred_element_type=jnp.float32)).astype(
            jnp.bfloat16
        )

    gate_parts = [up(o, f, gate_own, gate_far) for o, f in zip(own, far)]
    value_parts = [up(o, f, value_own, value_far) for o, f in zip(own, far)]

    conv_docs = jnp.concatenate([prev_docs[-2:], docs_plus], axis=0)
    part_docs = [
        lax.dynamic_slice_in_dim(conv_docs, i * part_rows, part_rows + 2, 0) for i in part_index
    ]

    def conv_parts(parts, taps):
        tails = [p[-2:] for p in parts]
        last = tails[0]
        for d in range(1, n_tp):
            last = jnp.where(part_index[d] == n_tp - 1, tails[d], last)
        prev = shifted(last, "sp", 1)
        result = []
        for d in range(n_tp):
            halo = jnp.where(part_index[d] == 0, prev, tails[(d + 1) % n_tp])
            result.append(
                convolve(jnp.concatenate([halo, parts[d]], axis=0), part_docs[d], taps)
            )
        return result

    gate_conv = conv_parts(gate_parts, conv_gate)
    value_conv = conv_parts(value_parts, conv_value)
    hidden = [
        (jax.nn.silu(g) * v).astype(jnp.bfloat16) for g, v in zip(gate_conv, value_conv)
    ]

    def down(units, w_t):
        return lax.dot_general(
            units, w_t, (((1,), (1,)), ((), ())), preferred_element_type=jnp.float32
        )

    own_units = [jnp.where(core == 0, h[:, :inner], h[:, inner:]) for h in hidden]
    far_units = [jnp.where(core == 0, h[:, inner:], h[:, :inner]) for h in hidden]

    def down_sums(w_own):
        w_far = core_swap(w_own)
        came = []
        for d in range(1, n_tp):
            sent = (down(own_units[d], w_own) + down(far_units[d], w_far)).astype(
                jnp.bfloat16
            )
            came.append(turned(sent, "tp", -d))
        kept = down(own_units[0], w_own) + down(far_units[0], w_far)
        for t in came:
            kept = kept + t.astype(jnp.float32)
        return kept

    odd_sum = down_sums(down_odd)
    even_sum = down_sums(down_even)
    sums = (even_sum, odd_sum)
    return finish(mid, sums, depth)


def mult(x, m):
    return x if isinstance(x, int) else pl.multiple_of(x, m)


def ring_chip(place, chips):
    odd = lax.div(place, chips // 2)
    return (1 - odd) * (2 * place) + odd * (2 * (chips - 1 - place) + 1)


def layer_kernel(
    n_sp,
    n_tp,
    queries,
    keys,
    values,
    docs,
    sinks,
    residual,
    out_weight,
    norm_gain,
    w_gate,
    w_value,
    conv_gate,
    conv_value,
    w_down,
    mid,
    wg,
    wv,
    wd,
    nrm,
    hid,
    pre,
    q_v,
    k_v,
    v_v,
    doc_v,
    doc_col,
    same_one,
    same_two,
    att,
    heads,
    ow,
    sink_v,
    gain_v,
    cg_v,
    cv_v,
    send,
    came,
    own,
    local_sem,
    ring_send,
    ring_recv,
    sib_send,
    sib_recv,
    halo_send,
    halo_recv,
    ow_send,
    ow_recv,
    heads_send,
    heads_recv,
    nrm_send,
    nrm_recv,
    sum_send,
    sum_recv,
):
    sp = lax.axis_index("sp")
    tp = lax.axis_index("tp")
    chips = n_sp // 2
    core = lax.rem(sp, 2)
    chip = lax.div(sp, 2)
    odd = lax.rem(chip, 2)
    place = (1 - odd) * lax.div(chip, 2) + odd * (chips - 1 - lax.div(chip, 2))
    way = 1 - 2 * core
    down_sp = 2 * ring_chip(lax.rem(place + way + chips, chips), chips) + core
    up_sp = 2 * ring_chip(lax.rem(place - way + chips, chips), chips) + core
    sib_sp = sp + way
    next_sp = lax.rem(sp + 1, n_sp)
    prev_sp = lax.rem(sp + n_sp - 1, n_sp)

    rows, q_width = queries.shape
    part = rows // n_tp
    depth, units = w_gate.shape
    width = residual.shape[1]
    kv_heads = keys.shape[1] // HEAD_DIM
    group = q_width // keys.shape[1]
    blocks = rows // WINDOW
    part_blocks = part // WINDOW
    ow_half = q_width // 2
    unit_tiles = units // TILE
    events = (chips - 1) * SUB

    def peer(d):
        return lax.rem(tp + d, n_tp)

    def held(h):
        return 2 * ring_chip(lax.rem(place - way * h + chips, chips), chips) + core

    def sib_held(h):
        return 2 * ring_chip(lax.rem(place + way * h + chips, chips), chips) + 1 - core

    def piece(w, j, s):
        size = depth // SUB
        return (wg, wv, wd)[w].at[pl.ds(mult(j * depth + s * size, size), size), :]

    def remote(src, dst, send_sem, recv_sem, device):
        return pltpu.make_async_remote_copy(
            src_ref=src,
            dst_ref=dst,
            send_sem=send_sem,
            recv_sem=recv_sem,
            device_id=device,
            device_id_type=MESH,
        )

    def ring_copy(w, h, s):
        at = piece(w, held(h - 1), s)
        return remote(at, at, ring_send.at[w], ring_recv.at[w, h - 1, s], (down_sp, tp))

    def ring_wait(w, h, s):
        dst = piece(w, held(h), s)
        remote(
            dst, dst, ring_send.at[w], ring_recv.at[w, h - 1, s], (down_sp, tp)
        ).wait_recv()

    def sib_sem(w, h, s):
        if w < 2:
            return sib_recv.at[w]
        late = lax.div(h, chips - 1) * (s // (SUB // 2) if isinstance(s, int) else lax.div(s, SUB // 2))
        return sib_recv.at[2 + h + late]

    def sib_copy(w, h, s):
        at = piece(w, held(h), s)
        return remote(at, at, sib_send.at[w], sib_sem(w, h, s), (sib_sp, tp))

    def sib_wait(w, h, part_of=None):
        buf = (wg, wv, wd)[w]
        if w < 2:
            got = buf.at[pl.ds(0, chips * depth), :]
        elif part_of is None:
            got = buf.at[pl.ds(mult(sib_held(h) * depth, depth), depth), :]
        else:
            got = last_half(sib_held(h), part_of)
        sem = sib_sem(w, h, 0 if part_of is None else part_of * (SUB // 2))
        remote(got, got, sib_send.at[w], sem, (sib_sp, tp)).wait_recv()

    def last_half(j, part_of):
        return wd.at[pl.ds(mult(j * depth + part_of * (depth // 2), depth // 2), depth // 2), :]

    def sent_weights(w):
        buf = (wg, wv, wd)[w]
        ring = buf.at[pl.ds(0, (chips - 1) * depth), :]
        swapped = buf.at[pl.ds(0, chips * depth), :]
        remote(ring, ring, ring_send.at[w], ring_recv.at[w, 0, 0], (down_sp, tp)).wait_send()
        remote(swapped, swapped, sib_send.at[w], sib_recv.at[w], (sib_sp, tp)).wait_send()

    def start_own(w):
        for s in range(SUB):
            ring_copy(w, 1, s).start()
        for s in range(SUB):
            sib_copy(w, 0, s).start()

    def service(w, e):
        h = 1 + (e // SUB if isinstance(e, int) else lax.div(e, SUB))
        s = e % SUB if isinstance(e, int) else lax.rem(e, SUB)
        ring_wait(w, h, s)
        if isinstance(e, int):
            if h < chips - 1:
                ring_copy(w, h + 1, s).start()
        else:

            @pl.when(h < chips - 1)
            def _():
                ring_copy(w, h + 1, s).start()

        sib_copy(w, h, s).start()
        if w < 2:

            @pl.when(e == (chips - 2) * SUB - 1)
            def _():
                start_own(w + 1)

    def serve(w, first, last):
        if last > first:

            @pl.loop(first, last)
            def _(e):
                service(w, e)

    own_rows = pl.ds(mult(sp * depth, depth), depth)
    strips = [(c, min(rows, units - c * rows)) for c in range(-(-units // rows))]
    local = [
        (w_gate, wg.at[own_rows, :]),
        (keys, k_v.at[pl.ds(WINDOW, rows), :]),
        (values, v_v.at[pl.ds(WINDOW, rows), :]),
        (docs, doc_v.at[pl.ds(8, blocks), :]),
        (queries, q_v),
        (sinks, sink_v),
        (residual, mid),
        (out_weight, ow.at[tp]),
        (norm_gain, gain_v),
        (conv_gate, cg_v),
        (conv_value, cv_v),
        (w_value, wv.at[own_rows, :]),
    ]
    local += [
        (
            w_down.at[pl.ds(c * rows, length), :],
            hid.at[pl.ds(0, length), pl.ds(c * depth, depth)],
        )
        for c, length in strips
    ]
    local = [
        pltpu.make_async_copy(src, dst, local_sem.at[i]) for i, (src, dst) in enumerate(local)
    ]
    for copy in local[:6]:
        copy.start()

    nrm[0:HALO, :] = jnp.zeros((HALO, width), jnp.bfloat16)
    barrier = pltpu.get_barrier_semaphore()
    greeted = [(down_sp, tp), (up_sp, tp), (sib_sp, tp), (next_sp, tp), (prev_sp, tp)]
    greeted += [(sp, peer(d)) for d in range(1, n_tp)]
    for device in greeted:
        pl.semaphore_signal(barrier, inc=1, device_id=device, device_id_type=MESH)
    pl.semaphore_wait(barrier, len(greeted))

    halos = [
        (keys.at[pl.ds(rows - WINDOW, WINDOW), :], k_v.at[pl.ds(0, WINDOW), :]),
        (values.at[pl.ds(rows - WINDOW, WINDOW), :], v_v.at[pl.ds(0, WINDOW), :]),
        (docs.at[pl.ds(blocks - 1, 1), :], doc_v.at[pl.ds(7, 1), :]),
    ]
    halos = [
        remote(src, dst, halo_send.at[i], halo_recv.at[i], (next_sp, tp))
        for i, (src, dst) in enumerate(halos)
    ]
    for copy in halos:
        copy.start()
    local[0].wait()
    start_own(0)

    def ow_rows(t, c):
        return ow.at[t, pl.ds(mult(c * ow_half, ow_half), ow_half), :]

    ow_src = out_weight.at[pl.ds(mult(core * ow_half, ow_half), ow_half), :]
    ow_out = [
        remote(ow_src, ow_rows(tp, core), ow_send.at[0, d - 1], ow_recv.at[0, d - 1], (sp, peer(n_tp - d)))
        for d in range(1, n_tp)
    ]
    for copy in ow_out:
        copy.start()
    for copy in local[6:]:
        copy.start()

    for copy in local[1:6]:
        copy.wait()
    for copy in halos:
        copy.wait_recv()

    lane = lax.broadcasted_iota(jnp.int32, (WINDOW, 2 * HEAD_DIM), 1)
    low_lane = lane < HEAD_DIM
    doc_v[7:8, :] = jnp.where(sp == 0, -1, doc_v[7:8, :])
    for b in range(-1, blocks):
        row = doc_v[8 + b : 9 + b, :]
        column = jnp.broadcast_to(row, (WINDOW, WINDOW)).T
        if b < 0:
            doc_col[0:8, :] = column[WINDOW - 8 :, :]
        else:
            doc_col[8 + b * WINDOW : 8 + (b + 1) * WINDOW, :] = column
    for b in range(blocks):
        at = 8 + b * WINDOW
        here = doc_col[at : at + WINDOW, :]
        back_one = doc_col[at - 1 : at - 1 + WINDOW, :]
        back_two = doc_col[at - 2 : at - 2 + WINDOW, :]
        to = slice(b * WINDOW, (b + 1) * WINDOW)
        same_one[to, :] = jnp.where(here == back_one, 1.0, 0.0)
        same_two[to, :] = jnp.where(here == back_two, 1.0, 0.0)

    q_index = lax.broadcasted_iota(jnp.int32, (WINDOW, 2 * WINDOW), 0)
    k_index = lax.broadcasted_iota(jnp.int32, (WINDOW, 2 * WINDOW), 1)
    first_rows = lax.broadcasted_iota(jnp.int32, (2 * WINDOW, 1), 0) < WINDOW

    def attend_block(b):
        base = mult(b * WINDOW, WINDOW)
        key_docs = jnp.concatenate([doc_v[pl.ds(7 + b, 1), :], doc_v[pl.ds(8 + b, 1), :]], axis=1)
        here = doc_col[pl.ds(mult(8 + base, 8), WINDOW), :]
        keep = (k_index > q_index) & (k_index <= q_index + WINDOW)
        keep = keep & (jnp.concatenate([here, here], axis=1) == key_docs)
        keep = jnp.concatenate([keep, keep], axis=0)
        k_band = k_v[pl.ds(base, 2 * WINDOW), :]
        v_band = v_v[pl.ds(base, 2 * WINDOW), :]
        for g in range(kv_heads):
            at = slice(g * HEAD_DIM, (g + 1) * HEAD_DIM)
            kk = jnp.concatenate([k_band[:, at], k_band[:, at]], axis=1)
            vv = jnp.concatenate([v_band[:, at], v_band[:, at]], axis=1)
            for pair in range(group // 2):
                head = g * group + 2 * pair
                lanes = slice(head * HEAD_DIM, (head + 2) * HEAD_DIM)
                both = q_v[pl.ds(base, WINDOW), lanes]
                zero = jnp.zeros_like(both)
                split = jnp.concatenate(
                    [jnp.where(low_lane, both, zero), jnp.where(low_lane, zero, both)], axis=0
                )
                scores = lax.dot_general(
                    split, kk, (((1,), (1,)), ((), ())), preferred_element_type=jnp.float32
                ) * HEAD_DIM ** (-0.5)
                scores = jnp.where(keep, scores, -1e30)
                sink = jnp.where(first_rows, sink_v[head], sink_v[head + 1])
                peak = jnp.maximum(jnp.max(scores, axis=1, keepdims=True), sink)
                expd = jnp.exp(scores - peak)
                total = jnp.sum(expd, axis=1, keepdims=True) + jnp.exp(sink - peak)
                probs = (expd * (1.0 / total)).astype(jnp.bfloat16)
                mixed = jnp.dot(probs, vv, preferred_element_type=jnp.float32)
                att[pl.ds(base, WINDOW), lanes] = jnp.where(
                    low_lane, mixed[:WINDOW], mixed[WINDOW:]
                ).astype(jnp.bfloat16)

    def due(share):
        return events * share // 28

    def attend_blocks(first, count, e, share):
        @pl.loop(0, count)
        def _(i):
            attend_block(lax.rem(first + i, blocks))
            before = lax.div(i * share, count)

            @pl.when(lax.div((i + 1) * share, count) > before)
            def _():
                service(0, e + before)

    far_share = min(due(2), blocks - part_blocks)
    own_share = min(due(3), part_blocks)
    attend_blocks((tp + 1) * part_blocks, blocks - part_blocks, 0, far_share)
    attend_blocks(tp * part_blocks, part_blocks, far_share, own_share)
    heads_out = [
        remote(
            att.at[pl.ds(mult(peer(n_tp - d) * part, part), part), :],
            heads.at[d - 1],
            heads_send.at[d - 1],
            heads_recv.at[d - 1],
            (sp, peer(n_tp - d)),
        )
        for d in range(1, n_tp)
    ]
    for copy in heads_out:
        copy.start()
    for copy in local[6:]:
        copy.wait()
    for c, length in strips:
        for at in range(0, length, TILE):
            turned_piece = hid[at : at + TILE, c * depth : (c + 1) * depth].astype(jnp.float32).T
            to = slice(c * rows + at, c * rows + at + TILE)
            wd[own_rows, to] = turned_piece.astype(jnp.bfloat16)
    before_proj = due(16)
    serve(0, far_share + own_share, before_proj)

    ow_on = []
    for d in range(1, n_tp):
        got = ow_rows(peer(d), core)
        remote(got, got, ow_send.at[0, d - 1], ow_recv.at[0, d - 1], (sp, peer(n_tp - d))).wait_recv()
        copy = remote(got, got, ow_send.at[1, d - 1], ow_recv.at[1, d - 1], (sib_sp, tp))
        copy.start()
        ow_on.append(copy)
    for d in range(1, n_tp):
        got = ow_rows(peer(d), 1 - core)
        remote(got, got, ow_send.at[1, d - 1], ow_recv.at[1, d - 1], (sib_sp, tp)).wait_recv()
        heads_out[d - 1].wait_recv()

    part_base = tp * part

    def nrm_rows(t, i):
        return nrm.at[pl.ds(mult(HALO + t * part + i * WINDOW, HALO), WINDOW), :]

    def nrm_copy(i, d):
        at = nrm_rows(tp, i)
        return remote(at, at, nrm_send.at[0], nrm_recv.at[i, d - 1], (sp, peer(n_tp - d)))

    def project(i):
        at = pl.ds(mult(i * WINDOW, WINDOW), WINDOW)
        mine = att[pl.ds(mult(part_base + i * WINDOW, WINDOW), WINDOW), :]
        proj = jnp.dot(mine, ow[tp], preferred_element_type=jnp.float32)
        for d in range(1, n_tp):
            proj = proj + jnp.dot(
                heads[d - 1, at, :], ow[peer(d)], preferred_element_type=jnp.float32
            )
        rounded = (mid[at, :].astype(jnp.float32) + proj).astype(jnp.bfloat16)
        mid[at, :] = rounded
        wide = rounded.astype(jnp.float32)
        scale = lax.rsqrt(jnp.mean(wide * wide, axis=1, keepdims=True) + 1e-06)
        normed = (wide * scale * gain_v[...]).astype(jnp.bfloat16)
        nrm[pl.ds(mult(HALO + part_base + i * WINDOW, HALO), WINDOW), :] = normed

    @pl.loop(0, part_blocks)
    def _(k):
        i = part_blocks - 1 - k
        project(i)
        for d in range(1, n_tp):

            @pl.when(k > 0)
            def _():
                nrm_copy(i + 1, d).start()

        @pl.when(before_proj + k < events)
        def _():
            service(0, before_proj + k)

    for d in range(1, n_tp):
        nrm_copy(0, d).start()

    after_proj = min(events, before_proj + part_blocks)
    serve(0, after_proj, events)
    early_value = due(14)

    def nrm_wait(i):
        for d in range(1, n_tp):
            got = nrm_rows(peer(d), i)
            remote(
                got, got, nrm_send.at[0], nrm_recv.at[i, d - 1], (sp, peer(n_tp - d))
            ).wait_recv()

    nrm_wait(part_blocks - 1)
    nrm_halo = remote(
        nrm.at[pl.ds(HALO + rows - REACH, REACH), :],
        nrm.at[pl.ds(HALO - REACH, REACH), :],
        halo_send.at[3],
        halo_recv.at[3],
        (next_sp, tp),
    )
    nrm_halo.start()
    serve(1, 0, early_value)
    pl.loop(0, part_blocks - 1)(nrm_wait)

    sib_wait(0, 0)
    for copy in halos + heads_out + ow_out + ow_on + [nrm_halo]:
        copy.wait_send()

    sent_rows = nrm.at[pl.ds(0, (n_tp - 1) * part), :]
    remote(sent_rows, sent_rows, nrm_send.at[0], nrm_recv.at[0, 0], (sp, peer(1))).wait_send()

    nrm_halo.wait_recv()

    def up_tile(w_ref, taps, n, base, lengths):
        cols = pl.ds(mult(n * TILE, TILE), TILE)
        at = 0
        for length in lengths:
            lhs = nrm[pl.ds(mult(base + at, HALO), length), :]
            pre[at : at + length, :] = (
                jnp.dot(lhs, w_ref[:, cols], preferred_element_type=jnp.float32)
                .astype(jnp.bfloat16)
                .astype(jnp.float32)
            )
            at += length
        tap = taps[:, cols]
        for b in range((at - HALO) // WINDOW):
            at = HALO + b * WINDOW
            to = pl.ds(mult(base + b * WINDOW, WINDOW), WINDOW)
            one = jnp.concatenate([same_one[to, :]] * (TILE // WINDOW), axis=1)
            two = jnp.concatenate([same_two[to, :]] * (TILE // WINDOW), axis=1)
            conv = tap[2:3] * pre[at : at + WINDOW, :]
            conv = conv + one * (tap[1:2] * pre[at - 1 : at - 1 + WINDOW, :])
            conv = conv + two * (tap[0:1] * pre[at - 2 : at - 2 + WINDOW, :])
            yield to, cols, conv

    def spread(w, first, count, i):
        before = lax.div(i * count, unit_tiles)
        after = lax.div((i + 1) * count, unit_tiles)

        @pl.when(after > before)
        def _():
            service(w, first + before)

    gate_count = min(unit_tiles, events - early_value)

    @pl.loop(0, unit_tiles)
    def _(n):
        lengths = (HALO + rows // 2, rows // 2)
        for to, cols, conv in up_tile(wg, cg_v, n, 0, lengths):
            hid[to, cols] = (conv / (1.0 + jnp.exp(-conv))).astype(jnp.bfloat16)
        spread(1, early_value, gate_count, n)

    serve(1, early_value + gate_count, events)
    sib_wait(1, 0)

    def value_part(t, first, count):
        @pl.loop(0, unit_tiles)
        def _(n):
            for to, cols, conv in up_tile(wv, cv_v, n, t * part, (HALO + part,)):
                hid[to, cols] = (hid[to, cols].astype(jnp.float32) * conv).astype(
                    jnp.bfloat16
                )
            spread(2, first, count, n)

    def sum_copy(h, d, strip=None):
        src, dst, sem = send.at[h, d - 1], came.at[h, d - 1], h
        if strip is not None:
            at, lanes = last_strips[strip]
            src, dst, sem = src.at[at, lanes], dst.at[at, lanes], h + strip
        return remote(src, dst, sum_send.at[0], sum_recv.at[sem, d - 1], (sp, peer(d)))

    low_cols, high_cols = slice(0, depth), slice(depth, 2 * depth)
    last_strips = [
        (slice(0, part), low_cols),
        (slice(0, part // 2), high_cols),
        (slice(part // 2, part), high_cols),
    ]

    def hop_cols(h, c):
        j = held(h) if c == 0 else sib_held(h)
        return pl.ds(mult(j * depth, depth), depth)

    def add_up(h, c, parts):
        cols = hop_cols(h, c)
        total = own[h, :, c * depth : (c + 1) * depth] + mid[:, cols].astype(jnp.float32)
        for t in parts:
            total = total + t.astype(jnp.float32)
        mid[:, cols] = total.astype(jnp.bfloat16)

    def finish_hop(h):
        for d in range(1, n_tp):
            sum_copy(h, d).wait_recv()
        for c in range(2):
            lanes = slice(c * depth, (c + 1) * depth)
            add_up(h, c, [came[h, d - 1, :, lanes] for d in range(1, n_tp)])

    def finish_last():
        h = chips - 1
        for strip in range(3):
            for d in range(1, n_tp):
                sum_copy(h, d, strip).wait_recv()
        for c in range(2):
            lo = c * (depth // 2)
            pairs = [
                [came[h, d - 1, :, at + lo : at + lo + depth // 2] for at in (0, depth)]
                for d in range(1, n_tp)
            ]
            add_up(h, c, [jnp.concatenate(pair, axis=1) for pair in pairs])

    def apart(step):
        pl.when(sp >= 0)(step)

    def down_rows(rhs, t, at=0, length=part):
        lhs = hid[pl.ds(mult(t * part + at, length), length), :]
        return lax.dot_general(
            lhs, rhs, (((1,), (1,)), ((), ())), preferred_element_type=jnp.float32
        )

    def hop_rows(h):
        return jnp.concatenate(
            [wd[pl.ds(mult(j * depth, depth), depth), :] for j in (held(h), sib_held(h))], axis=0
        )

    def down_far(h):
        sib_wait(2, h)
        for d in range(1, n_tp):

            @apart
            def _():
                send[h, d - 1] = down_rows(hop_rows(h), peer(d)).astype(jnp.bfloat16)

    def down_own(h):
        @apart
        def _():
            own[h] = down_rows(hop_rows(h), tp)

    def down_far_strip(strip):
        h = chips - 1
        at, lanes = last_strips[strip]
        half = min(strip, 1)

        def rhs():
            return jnp.concatenate(
                [last_half(j, half)[...] for j in (held(h), sib_held(h))], axis=0
            )

        for d in range(1, n_tp):

            @apart
            def _():
                send[h, d - 1, at, lanes] = down_rows(
                    rhs(), peer(d), at.start, at.stop - at.start
                ).astype(jnp.bfloat16)

    def send_sums(h, strip=None):
        for d in range(1, n_tp):
            sum_copy(h, d, strip).start()

    served = due(5)
    for d in range(1, n_tp):
        value_part(peer(d), 0, served if d == 1 else 0)

    @pl.loop(0, EARLY)
    def _(h):
        down_far(h)
        for i in range(due(1)):
            service(2, served + h * due(1) + i)
        send_sums(h)

    served += EARLY * due(1)
    more = due(6)
    value_part(tp, served, more)
    served += more

    @pl.loop(EARLY, chips - 1)
    def _(h):
        for s in range(SUB):

            @pl.when((h - 1) * SUB + s >= served)
            def _():
                service(2, (h - 1) * SUB + s)

        down_far(h)

        @pl.when(h > EARLY)
        def _():
            finish_hop(h - EARLY - 1)

        for w in range(2):

            @pl.when(h == EARLY + w)
            def _():
                sent_weights(w)

        send_sums(h)
        down_own(h - EARLY)

    last = chips - 1

    def serve_last(half):
        for s in range(SUB // 2):
            service(2, (last - 1) * SUB + half * (SUB // 2) + s)
        sib_wait(2, last, half)

    def finish_range(first, stop):
        for h in range(first, stop):
            finish_hop(h)

    serve_last(0)
    down_far_strip(0)
    finish_range(last - EARLY - 1, last - EARLY)
    send_sums(last, 0)
    pl.loop(last - EARLY, last)(down_own)
    serve_last(1)
    down_far_strip(1)
    finish_range(last - EARLY, last - 1)
    send_sums(last, 1)
    down_far_strip(2)
    finish_range(last - 1, last)
    send_sums(last, 2)
    down_own(last)
    finish_last()

    sent_weights(2)

    remote(send, send, sum_send.at[0], sum_recv.at[0, 0], (sp, peer(1))).wait_send()


def whole_layer(n_sp, n_tp, queries, keys, values, doc_ids, sinks, residual, out_weight,
                norm_gain, w_gate, w_value, conv_gate, conv_value, w_down):
    rows, q_width = queries.shape
    kv_width = keys.shape[1]
    part, width = residual.shape
    depth, units = w_gate.shape
    chips = n_sp // 2
    bf16, f32 = jnp.bfloat16, jnp.float32
    dma = pltpu.SemaphoreType.DMA
    part_blocks = part // WINDOW
    scratch = [
        pltpu.VMEM((width, units), bf16),
        pltpu.VMEM((width, units), bf16),
        pltpu.VMEM((width, units), bf16),
        pltpu.VMEM((HALO + rows, width), bf16),
        pltpu.VMEM((rows, units), bf16),
        pltpu.VMEM((HALO + rows, TILE), f32),
        pltpu.VMEM((rows, q_width), bf16),
        pltpu.VMEM((WINDOW + rows, kv_width), bf16),
        pltpu.VMEM((WINDOW + rows, kv_width), bf16),
        pltpu.VMEM((8 + rows // WINDOW, WINDOW), jnp.int32),
        pltpu.VMEM((8 + rows, WINDOW), jnp.int32),
        pltpu.VMEM((rows, WINDOW), f32),
        pltpu.VMEM((rows, WINDOW), f32),
        pltpu.VMEM((rows, q_width), bf16),
        pltpu.VMEM((n_tp - 1, part, q_width), bf16),
        pltpu.VMEM((n_tp, q_width, width), bf16),
        pltpu.SMEM((q_width // HEAD_DIM,), f32),
        pltpu.VMEM((1, width), f32),
        pltpu.VMEM((3, units), f32),
        pltpu.VMEM((3, units), f32),
        pltpu.VMEM((chips, n_tp - 1, part, 2 * depth), bf16),
        pltpu.VMEM((chips, n_tp - 1, part, 2 * depth), bf16),
        pltpu.VMEM((chips, part, 2 * depth), f32),
        dma((12 - (-units // rows),)),
        dma((3,)),
        dma((3, chips - 1, SUB)),
        dma((3,)),
        dma((chips + 3,)),
        dma((4,)),
        dma((4,)),
        dma((2, n_tp - 1)),
        dma((2, n_tp - 1)),
        dma((n_tp - 1,)),
        dma((n_tp - 1,)),
        dma((1,)),
        dma((part_blocks, n_tp - 1)),
        dma((1,)),
        dma((chips + 2, n_tp - 1)),
    ]
    any_spec = pl.BlockSpec(memory_space=pl.ANY)
    return pl.pallas_call(
        functools.partial(layer_kernel, n_sp, n_tp),
        out_shape=pltpu.VMEM(residual.shape, residual.dtype),
        in_specs=[any_spec] * 13,
        out_specs=pl.BlockSpec(memory_space=pltpu.VMEM),
        scratch_shapes=scratch,
        compiler_params=pltpu.CompilerParams(
            collective_id=0, has_side_effects=True, vmem_limit_bytes=VMEM_BYTES - 2 * residual.size
        ),
    )(
        queries,
        keys,
        values,
        doc_ids.reshape(rows // WINDOW, WINDOW),
        sinks,
        residual,
        out_weight,
        norm_gain.reshape(1, width),
        w_gate,
        w_value,
        conv_gate,
        conv_value,
        w_down,
    )


def in_one_kernel(n_sp, n_tp, queries, keys, values, doc_ids, *weights):
    w_gate = weights[4]
    depth, units = w_gate.shape
    aligned = depth % 128 == 0 and keys.shape[1] % 128 == 0 and units % TILE == 0
    return aligned and n_sp % 4 == 0 and n_tp > 1 and doc_ids.shape[0] % (n_tp * WINDOW) == 0


def solution(mesh):
    n_sp, n_tp = mesh.shape["sp"], mesh.shape["tp"]

    def body(*args):
        if in_one_kernel(n_sp, n_tp, *args):
            return whole_layer(n_sp, n_tp, *args)
        return per_device(*args)

    return jax.shard_map(
        body,
        mesh=mesh,
        in_specs=(
            P("sp", "tp"),
            P("sp", "tp"),
            P("sp", "tp"),
            P("sp"),
            P("tp"),
            P(("sp", "tp"), None),
            P("tp", None),
            P(),
            P("sp", "tp"),
            P("sp", "tp"),
            P(None, "tp"),
            P(None, "tp"),
            P("tp", "sp"),
        ),
        out_specs=P(("sp", "tp"), None),
        check_vma=False,
    )
```

```python
import functools

import jax
import jax.numpy as jnp
from jax import lax
from jax.experimental import pallas as pl
from jax.experimental.pallas import tpu as pltpu
from jax.sharding import PartitionSpec as P


HEAD_DIM = 64
WINDOW = 128
ROW_TILE = 128
SUB = 4
EARLY = 2
HALO = 16
REACH = 2
TILE = 256
VMEM_BYTES = 67043328
MESH = pl.DeviceIdType.MESH


def shifted(shard, axis, by):
    size = lax.axis_size(axis)
    pairs = [(i, i + by) for i in range(size) if 0 <= i + by < size]
    return lax.ppermute(shard, axis, pairs)


def turned(t, axis, by):
    size = lax.axis_size(axis)
    return lax.ppermute(t, axis, [(i, (i + by) % size) for i in range(size)])


def core_swap(t):
    size = lax.axis_size("sp")
    return lax.ppermute(t, "sp", [(i, i ^ 1) for i in range(size)])


def parity_gather(t):
    size = lax.axis_size("sp")
    groups = [list(range(0, size, 2)), list(range(1, size, 2))]
    return lax.all_gather(t, "sp", axis=0, tiled=True, axis_index_groups=groups)


def ring_gather(t):
    chips = lax.axis_size("sp") // 2
    order = list(range(0, chips, 2)) + list(range(1, chips, 2))[::-1]
    chip = lax.axis_index("sp") // 2
    place = jnp.where(chip % 2 == 0, chip // 2, chips - 1 - chip // 2)

    def hop(piece, by):
        pairs = [
            (2 * order[k] + c, 2 * order[(k + by) % chips] + c)
            for k in range(chips)
            for c in range(2)
        ]
        return lax.ppermute(piece, "sp", pairs)

    def chip_at(k):
        k = (k + chips) % chips
        return jnp.where(k < chips // 2, 2 * k, 2 * (chips - 1 - k) + 1)

    depth = t.shape[0]
    pieces = [(chip, t)]
    up = down = t
    for step in range(1, chips // 2 + 1):
        up = hop(up, 1)
        pieces.append((chip_at(place - step), up))
        if step < chips - step:
            down = hop(down, -1)
            pieces.append((chip_at(place + step), down))
    whole = jnp.zeros((chips * depth,) + t.shape[1:], t.dtype)
    for at, piece in pieces:
        whole = lax.dynamic_update_slice_in_dim(whole, piece, at * depth, 0)
    return whole


def by_parity(t, depth):
    rows, width = t.shape
    blocks = width // depth
    tile = min(ROW_TILE, rows)

    def kernel(in_ref, out_ref):
        for j in range(blocks):
            to = (j // 2 + (j % 2) * (blocks // 2)) * depth
            out_ref[:, to : to + depth] = in_ref[:, j * depth : (j + 1) * depth]

    return pl.pallas_call(
        kernel,
        out_shape=jax.ShapeDtypeStruct(t.shape, t.dtype),
        grid=(rows // tile,),
        in_specs=[pl.BlockSpec((tile, width), lambda i: (i, 0))],
        out_specs=pl.BlockSpec((tile, width), lambda i: (i, 0)),
        cost_estimate=pl.CostEstimate(
            flops=0, bytes_accessed=2 * t.size * t.dtype.itemsize, transcendentals=0
        ),
    )(t)


def finish(mid, sums, depth):
    rows, width = mid.shape
    blocks = width // depth
    tile = min(ROW_TILE, rows)

    def kernel(mid_ref, even_ref, odd_ref, out_ref):
        for j in range(blocks):
            at = (j // 2) * depth
            held = at + (j % 2) * (width // 2)
            sum_ref = odd_ref if j % 2 else even_ref
            out_ref[:, j * depth : (j + 1) * depth] = (
                mid_ref[:, held : held + depth].astype(jnp.float32)
                + sum_ref[:, at : at + depth]
            ).astype(out_ref.dtype)

    half_spec = pl.BlockSpec((tile, width // 2), lambda i: (i, 0))
    return pl.pallas_call(
        kernel,
        out_shape=jax.ShapeDtypeStruct(mid.shape, mid.dtype),
        grid=(rows // tile,),
        in_specs=[pl.BlockSpec((tile, width), lambda i: (i, 0)), half_spec, half_spec],
        out_specs=pl.BlockSpec((tile, width), lambda i: (i, 0)),
        cost_estimate=pl.CostEstimate(
            flops=mid.size, bytes_accessed=8 * mid.size, transcendentals=0
        ),
    )(mid, *sums)


def attend(query_rows, key_ext, value_ext, doc_rows, doc_ext, sinks):
    row_count = query_rows.shape[0]
    block_count = row_count // WINDOW
    kv_heads = key_ext.shape[1] // HEAD_DIM
    group_size = query_rows.shape[1] // (kv_heads * HEAD_DIM)

    def band(t):
        lower = t[:row_count].reshape((block_count, WINDOW) + t.shape[1:])
        upper = t[WINDOW:].reshape((block_count, WINDOW) + t.shape[1:])
        return jnp.concatenate([lower, upper], axis=1)

    query_band = query_rows.reshape(block_count, WINDOW, kv_heads, group_size, HEAD_DIM)
    key_band = band(key_ext).reshape(block_count, 2 * WINDOW, kv_heads, HEAD_DIM)
    value_band = band(value_ext).reshape(block_count, 2 * WINDOW, kv_heads, HEAD_DIM)
    doc_band = band(doc_ext)
    distance = jnp.arange(WINDOW)[:, None] + WINDOW - jnp.arange(2 * WINDOW)[None, :]
    in_window = (distance >= 0) & (distance < WINDOW)
    same_doc = doc_rows.reshape(block_count, WINDOW)[:, :, None] == doc_band[:, None, :]
    keep_mask = in_window[None] & same_doc
    scores = jnp.einsum(
        "nqhgd,nkhd->nhgqk", query_band, key_band, preferred_element_type=jnp.float32
    ) * HEAD_DIM ** (-0.5)
    scores = jnp.where(keep_mask[:, None, None], scores, -jnp.inf)
    sink_logit = sinks.reshape(kv_heads, group_size)[None, :, :, None, None]
    peak = jnp.maximum(jnp.max(scores, axis=-1, keepdims=True), sink_logit)
    expd = jnp.exp(scores - peak)
    probs = (expd / (jnp.sum(expd, axis=-1, keepdims=True) + jnp.exp(sink_logit - peak))).astype(
        jnp.bfloat16
    )
    mixed = jnp.einsum("nhgqk,nkhd->nqhgd", probs, value_band, preferred_element_type=jnp.float32)
    return mixed.astype(jnp.bfloat16).reshape(row_count, -1)


def convolve(ext_rows, doc_ext, taps):
    center = doc_ext[2:]
    same_one = (doc_ext[1:-1] == center)[:, None]
    same_two = (doc_ext[:-2] == center)[:, None]
    ext32 = ext_rows.astype(jnp.float32)
    result = taps[2] * ext32[2:]
    result = result + jnp.where(same_one, taps[1] * ext32[1:-1], 0.0)
    return result + jnp.where(same_two, taps[0] * ext32[:-2], 0.0)


def per_device(
    queries,
    keys,
    values,
    doc_ids,
    sinks,
    residual,
    out_weight,
    norm_gain,
    w_gate,
    w_value,
    conv_gate,
    conv_value,
    w_down,
):
    core = lax.axis_index("sp") % 2
    tp = lax.axis_index("tp")
    n_tp = lax.axis_size("tp")
    rows = doc_ids.shape[0]
    part_rows = rows // n_tp
    depth = w_gate.shape[0]
    width = residual.shape[1]
    half = width // 2
    part_index = [(tp + n_tp - d) % n_tp for d in range(n_tp)]

    gate_own = parity_gather(w_gate)
    value_own = ring_gather(w_value)
    down_t = w_down.T
    inner = down_t.shape[1] // 2
    low, high = down_t[:, :inner], down_t[:, inner:]
    kept_half = jnp.where(core == 0, low, high)
    came_half = core_swap(jnp.where(core == 0, high, low))
    even_piece = jnp.where(core == 0, kept_half, came_half)
    odd_piece = jnp.where(core == 0, came_half, kept_half)
    down_odd = parity_gather(odd_piece)
    down_even = parity_gather(even_piece)
    gate_far = core_swap(gate_own)
    value_far = core_swap(value_own)

    out_far = [turned(out_weight, "tp", d) for d in range(1, n_tp)]
    out_parts = [by_parity(t, depth) for t in [out_weight] + out_far]
    residual = by_parity(residual, depth)
    norm_gain = norm_gain.reshape(-1, 2, depth).swapaxes(0, 1).reshape(-1)
    docs_plus = doc_ids + 1
    prev_keys, prev_values, prev_docs = shifted(
        (keys[-WINDOW:], values[-WINDOW:], docs_plus[-WINDOW:]), "sp", 1
    )
    key_ext = jnp.concatenate([prev_keys, keys], axis=0)
    value_ext = jnp.concatenate([prev_values, values], axis=0)
    doc_ext = jnp.concatenate([prev_docs, docs_plus], axis=0)
    head_out = attend(queries, key_ext, value_ext, docs_plus, doc_ext, sinks)

    def rows_of(t, index):
        return lax.dynamic_slice_in_dim(t, index * part_rows, part_rows, 0)

    proj = jnp.dot(rows_of(head_out, tp), out_parts[0], preferred_element_type=jnp.float32)
    for d in range(1, n_tp):
        heads_far = turned(rows_of(head_out, (tp + d) % n_tp), "tp", d)
        proj = proj + jnp.dot(heads_far, out_parts[d], preferred_element_type=jnp.float32)
    mid = (residual.astype(jnp.float32) + proj).astype(jnp.bfloat16)
    mid32 = mid.astype(jnp.float32)
    normed = (
        mid32 * lax.rsqrt(jnp.mean(mid32 * mid32, axis=-1, keepdims=True) + 1e-06) * norm_gain
    ).astype(jnp.bfloat16)
    even, odd = normed[:, :half], normed[:, half:]
    own = [jnp.where(core == 0, even, odd)]
    far = [jnp.where(core == 0, odd, even)]
    for d in range(1, n_tp):
        own.append(turned(own[0], "tp", d))
        far.append(turned(far[0], "tp", d))

    def up(own, far, w_own, w_far):
        total = jnp.dot(own, w_own, preferred_element_type=jnp.float32)
        return (total + jnp.dot(far, w_far, preferred_element_type=jnp.float32)).astype(
            jnp.bfloat16
        )

    gate_parts = [up(o, f, gate_own, gate_far) for o, f in zip(own, far)]
    value_parts = [up(o, f, value_own, value_far) for o, f in zip(own, far)]

    conv_docs = jnp.concatenate([prev_docs[-2:], docs_plus], axis=0)
    part_docs = [
        lax.dynamic_slice_in_dim(conv_docs, i * part_rows, part_rows + 2, 0) for i in part_index
    ]

    def conv_parts(parts, taps):
        tails = [p[-2:] for p in parts]
        last = tails[0]
        for d in range(1, n_tp):
            last = jnp.where(part_index[d] == n_tp - 1, tails[d], last)
        prev = shifted(last, "sp", 1)
        result = []
        for d in range(n_tp):
            halo = jnp.where(part_index[d] == 0, prev, tails[(d + 1) % n_tp])
            result.append(
                convolve(jnp.concatenate([halo, parts[d]], axis=0), part_docs[d], taps)
            )
        return result

    gate_conv = conv_parts(gate_parts, conv_gate)
    value_conv = conv_parts(value_parts, conv_value)
    hidden = [
        (jax.nn.silu(g) * v).astype(jnp.bfloat16) for g, v in zip(gate_conv, value_conv)
    ]

    def down(units, w_t):
        return lax.dot_general(
            units, w_t, (((1,), (1,)), ((), ())), preferred_element_type=jnp.float32
        )

    own_units = [jnp.where(core == 0, h[:, :inner], h[:, inner:]) for h in hidden]
    far_units = [jnp.where(core == 0, h[:, inner:], h[:, :inner]) for h in hidden]

    def down_sums(w_own):
        w_far = core_swap(w_own)
        came = []
        for d in range(1, n_tp):
            sent = (down(own_units[d], w_own) + down(far_units[d], w_far)).astype(
                jnp.bfloat16
            )
            came.append(turned(sent, "tp", -d))
        kept = down(own_units[0], w_own) + down(far_units[0], w_far)
        for t in came:
            kept = kept + t.astype(jnp.float32)
        return kept

    odd_sum = down_sums(down_odd)
    even_sum = down_sums(down_even)
    sums = (even_sum, odd_sum)
    return finish(mid, sums, depth)


def mult(x, m):
    return x if isinstance(x, int) else pl.multiple_of(x, m)


def ring_chip(place, chips):
    odd = lax.div(place, chips // 2)
    return (1 - odd) * (2 * place) + odd * (2 * (chips - 1 - place) + 1)


def layer_kernel(
    n_sp,
    n_tp,
    queries,
    keys,
    values,
    docs,
    sinks,
    residual,
    out_weight,
    norm_gain,
    w_gate,
    w_value,
    conv_gate,
    conv_value,
    w_down,
    mid,
    wg,
    wv,
    wd,
    nrm,
    hid,
    pre,
    q_v,
    k_v,
    v_v,
    doc_v,
    doc_col,
    same_one,
    same_two,
    att,
    heads,
    ow,
    sink_v,
    gain_v,
    cg_v,
    cv_v,
    send,
    came,
    own,
    local_sem,
    ring_send,
    ring_recv,
    sib_send,
    sib_recv,
    halo_send,
    halo_recv,
    ow_send,
    ow_recv,
    heads_send,
    heads_recv,
    nrm_send,
    nrm_recv,
    sum_send,
    sum_recv,
):
    sp = lax.axis_index("sp")
    tp = lax.axis_index("tp")
    chips = n_sp // 2
    core = lax.rem(sp, 2)
    chip = lax.div(sp, 2)
    odd = lax.rem(chip, 2)
    place = (1 - odd) * lax.div(chip, 2) + odd * (chips - 1 - lax.div(chip, 2))
    way = 1 - 2 * core
    down_sp = 2 * ring_chip(lax.rem(place + way + chips, chips), chips) + core
    up_sp = 2 * ring_chip(lax.rem(place - way + chips, chips), chips) + core
    sib_sp = sp + way
    next_sp = lax.rem(sp + 1, n_sp)
    prev_sp = lax.rem(sp + n_sp - 1, n_sp)

    rows, q_width = queries.shape
    part = rows // n_tp
    depth, units = w_gate.shape
    width = residual.shape[1]
    kv_heads = keys.shape[1] // HEAD_DIM
    group = q_width // keys.shape[1]
    blocks = rows // WINDOW
    part_blocks = part // WINDOW
    ow_half = q_width // 2
    unit_tiles = units // TILE
    events = (chips - 1) * SUB

    def peer(d):
        return lax.rem(tp + d, n_tp)

    def held(h):
        return 2 * ring_chip(lax.rem(place - way * h + chips, chips), chips) + core

    def sib_held(h):
        return 2 * ring_chip(lax.rem(place + way * h + chips, chips), chips) + 1 - core

    def piece(w, j, s):
        size = depth // SUB
        return (wg, wv, wd)[w].at[pl.ds(mult(j * depth + s * size, size), size), :]

    def remote(src, dst, send_sem, recv_sem, device):
        return pltpu.make_async_remote_copy(
            src_ref=src,
            dst_ref=dst,
            send_sem=send_sem,
            recv_sem=recv_sem,
            device_id=device,
            device_id_type=MESH,
        )

    def ring_copy(w, h, s):
        at = piece(w, held(h - 1), s)
        return remote(at, at, ring_send.at[w], ring_recv.at[w, h - 1, s], (down_sp, tp))

    def ring_wait(w, h, s):
        dst = piece(w, held(h), s)
        remote(
            dst, dst, ring_send.at[w], ring_recv.at[w, h - 1, s], (down_sp, tp)
        ).wait_recv()

    def sib_sem(w, h, s):
        if w < 2:
            return sib_recv.at[w]
        late = lax.div(h, chips - 1) * (s // (SUB // 2) if isinstance(s, int) else lax.div(s, SUB // 2))
        return sib_recv.at[2 + h + late]

    def sib_copy(w, h, s):
        at = piece(w, held(h), s)
        return remote(at, at, sib_send.at[w], sib_sem(w, h, s), (sib_sp, tp))

    def sib_wait(w, h, part_of=None):
        buf = (wg, wv, wd)[w]
        if w < 2:
            got = buf.at[pl.ds(0, chips * depth), :]
        elif part_of is None:
            got = buf.at[pl.ds(mult(sib_held(h) * depth, depth), depth), :]
        else:
            got = last_half(sib_held(h), part_of)
        sem = sib_sem(w, h, 0 if part_of is None else part_of * (SUB // 2))
        remote(got, got, sib_send.at[w], sem, (sib_sp, tp)).wait_recv()

    def last_half(j, part_of):
        return wd.at[pl.ds(mult(j * depth + part_of * (depth // 2), depth // 2), depth // 2), :]

    def sent_weights(w):
        buf = (wg, wv, wd)[w]
        ring = buf.at[pl.ds(0, (chips - 1) * depth), :]
        swapped = buf.at[pl.ds(0, chips * depth), :]
        remote(ring, ring, ring_send.at[w], ring_recv.at[w, 0, 0], (down_sp, tp)).wait_send()
        remote(swapped, swapped, sib_send.at[w], sib_recv.at[w], (sib_sp, tp)).wait_send()

    def start_own(w):
        for s in range(SUB):
            ring_copy(w, 1, s).start()
        for s in range(SUB):
            sib_copy(w, 0, s).start()

    def service(w, e):
        h = 1 + (e // SUB if isinstance(e, int) else lax.div(e, SUB))
        s = e % SUB if isinstance(e, int) else lax.rem(e, SUB)
        ring_wait(w, h, s)
        if isinstance(e, int):
            if h < chips - 1:
                ring_copy(w, h + 1, s).start()
        else:

            @pl.when(h < chips - 1)
            def _():
                ring_copy(w, h + 1, s).start()

        sib_copy(w, h, s).start()
        if w < 2:

            @pl.when(e == (chips - 2) * SUB - 1)
            def _():
                start_own(w + 1)

    def serve(w, first, last):
        if last > first:

            @pl.loop(first, last)
            def _(e):
                service(w, e)

    own_rows = pl.ds(mult(sp * depth, depth), depth)
    strips = [(c, min(rows, units - c * rows)) for c in range(-(-units // rows))]
    size = depth // SUB
    local = [(w_gate.at[pl.ds(s * size, size), :], piece(0, sp, s)) for s in range(SUB)]
    local += [
        (keys, k_v.at[pl.ds(WINDOW, rows), :]),
        (values, v_v.at[pl.ds(WINDOW, rows), :]),
        (docs, doc_v.at[pl.ds(8, blocks), :]),
        (queries, q_v),
        (sinks, sink_v),
        (residual, mid),
        (out_weight, ow.at[tp]),
        (norm_gain, gain_v),
        (conv_gate, cg_v),
        (conv_value, cv_v),
        (w_value, wv.at[own_rows, :]),
    ]
    local += [
        (
            w_down.at[pl.ds(c * rows, length), :],
            hid.at[pl.ds(0, length), pl.ds(c * depth, depth)],
        )
        for c, length in strips
    ]
    local = [
        pltpu.make_async_copy(src, dst, local_sem.at[i]) for i, (src, dst) in enumerate(local)
    ]
    early_end = SUB + 5
    for copy in local[:early_end]:
        copy.start()

    nrm[0:HALO, :] = jnp.zeros((HALO, width), jnp.bfloat16)
    barrier = pltpu.get_barrier_semaphore()
    greeted = [(down_sp, tp), (up_sp, tp), (sib_sp, tp), (next_sp, tp), (prev_sp, tp)]
    greeted += [(sp, peer(d)) for d in range(1, n_tp)]
    for device in greeted:
        pl.semaphore_signal(barrier, inc=1, device_id=device, device_id_type=MESH)
    pl.semaphore_wait(barrier, len(greeted))

    halos = [
        (keys.at[pl.ds(rows - WINDOW, WINDOW), :], k_v.at[pl.ds(0, WINDOW), :]),
        (values.at[pl.ds(rows - WINDOW, WINDOW), :], v_v.at[pl.ds(0, WINDOW), :]),
        (docs.at[pl.ds(blocks - 1, 1), :], doc_v.at[pl.ds(7, 1), :]),
    ]
    halos = [
        remote(src, dst, halo_send.at[i], halo_recv.at[i], (next_sp, tp))
        for i, (src, dst) in enumerate(halos)
    ]
    for copy in halos:
        copy.start()
    for s in range(SUB):
        local[s].wait()
        ring_copy(0, 1, s).start()
    for s in range(SUB):
        sib_copy(0, 0, s).start()

    def ow_rows(t, c):
        return ow.at[t, pl.ds(mult(c * ow_half, ow_half), ow_half), :]

    ow_src = out_weight.at[pl.ds(mult(core * ow_half, ow_half), ow_half), :]
    ow_out = [
        remote(ow_src, ow_rows(tp, core), ow_send.at[0, d - 1], ow_recv.at[0, d - 1], (sp, peer(n_tp - d)))
        for d in range(1, n_tp)
    ]
    for copy in ow_out:
        copy.start()
    for copy in local[early_end:]:
        copy.start()

    for copy in local[SUB:early_end]:
        copy.wait()
    for copy in halos:
        copy.wait_recv()

    lane = lax.broadcasted_iota(jnp.int32, (WINDOW, 2 * HEAD_DIM), 1)
    low_lane = lane < HEAD_DIM
    doc_v[7:8, :] = jnp.where(sp == 0, -1, doc_v[7:8, :])
    for b in range(-1, blocks):
        row = doc_v[8 + b : 9 + b, :]
        column = jnp.broadcast_to(row, (WINDOW, WINDOW)).T
        if b < 0:
            doc_col[0:8, :] = column[WINDOW - 8 :, :]
        else:
            doc_col[8 + b * WINDOW : 8 + (b + 1) * WINDOW, :] = column
    for b in range(blocks):
        at = 8 + b * WINDOW
        here = doc_col[at : at + WINDOW, :]
        back_one = doc_col[at - 1 : at - 1 + WINDOW, :]
        back_two = doc_col[at - 2 : at - 2 + WINDOW, :]
        to = slice(b * WINDOW, (b + 1) * WINDOW)
        same_one[to, :] = jnp.where(here == back_one, 1.0, 0.0)
        same_two[to, :] = jnp.where(here == back_two, 1.0, 0.0)

    q_index = lax.broadcasted_iota(jnp.int32, (WINDOW, 2 * WINDOW), 0)
    k_index = lax.broadcasted_iota(jnp.int32, (WINDOW, 2 * WINDOW), 1)
    first_rows = lax.broadcasted_iota(jnp.int32, (2 * WINDOW, 1), 0) < WINDOW

    def attend_block(b):
        base = mult(b * WINDOW, WINDOW)
        key_docs = jnp.concatenate([doc_v[pl.ds(7 + b, 1), :], doc_v[pl.ds(8 + b, 1), :]], axis=1)
        here = doc_col[pl.ds(mult(8 + base, 8), WINDOW), :]
        keep = (k_index > q_index) & (k_index <= q_index + WINDOW)
        keep = keep & (jnp.concatenate([here, here], axis=1) == key_docs)
        keep = jnp.concatenate([keep, keep], axis=0)
        k_band = k_v[pl.ds(base, 2 * WINDOW), :]
        v_band = v_v[pl.ds(base, 2 * WINDOW), :]
        for g in range(kv_heads):
            at = slice(g * HEAD_DIM, (g + 1) * HEAD_DIM)
            kk = jnp.concatenate([k_band[:, at], k_band[:, at]], axis=1)
            vv = jnp.concatenate([v_band[:, at], v_band[:, at]], axis=1)
            for pair in range(group // 2):
                head = g * group + 2 * pair
                lanes = slice(head * HEAD_DIM, (head + 2) * HEAD_DIM)
                both = q_v[pl.ds(base, WINDOW), lanes]
                zero = jnp.zeros_like(both)
                split = jnp.concatenate(
                    [jnp.where(low_lane, both, zero), jnp.where(low_lane, zero, both)], axis=0
                )
                scores = lax.dot_general(
                    split, kk, (((1,), (1,)), ((), ())), preferred_element_type=jnp.float32
                ) * HEAD_DIM ** (-0.5)
                scores = jnp.where(keep, scores, -1e30)
                sink = jnp.where(first_rows, sink_v[head], sink_v[head + 1])
                peak = jnp.maximum(jnp.max(scores, axis=1, keepdims=True), sink)
                expd = jnp.exp(scores - peak)
                total = jnp.sum(expd, axis=1, keepdims=True) + jnp.exp(sink - peak)
                probs = (expd * (1.0 / total)).astype(jnp.bfloat16)
                mixed = jnp.dot(probs, vv, preferred_element_type=jnp.float32)
                att[pl.ds(base, WINDOW), lanes] = jnp.where(
                    low_lane, mixed[:WINDOW], mixed[WINDOW:]
                ).astype(jnp.bfloat16)

    def due(share):
        return events * share // 28

    def attend_blocks(first, count, e, share):
        @pl.loop(0, count)
        def _(i):
            attend_block(lax.rem(first + i, blocks))
            before = lax.div(i * share, count)

            @pl.when(lax.div((i + 1) * share, count) > before)
            def _():
                service(0, e + before)

    far_share = min(due(2), blocks - part_blocks)
    own_share = min(due(3), part_blocks)
    attend_blocks((tp + 1) * part_blocks, blocks - part_blocks, 0, far_share)
    attend_blocks(tp * part_blocks, part_blocks, far_share, own_share)
    heads_out = [
        remote(
            att.at[pl.ds(mult(peer(n_tp - d) * part, part), part), :],
            heads.at[d - 1],
            heads_send.at[d - 1],
            heads_recv.at[d - 1],
            (sp, peer(n_tp - d)),
        )
        for d in range(1, n_tp)
    ]
    for copy in heads_out:
        copy.start()
    for copy in local[early_end:]:
        copy.wait()
    for c, length in strips:
        for at in range(0, length, TILE):
            turned_piece = hid[at : at + TILE, c * depth : (c + 1) * depth].astype(jnp.float32).T
            to = slice(c * rows + at, c * rows + at + TILE)
            wd[own_rows, to] = turned_piece.astype(jnp.bfloat16)
    before_proj = due(16)
    serve(0, far_share + own_share, before_proj)

    ow_on = []
    for d in range(1, n_tp):
        got = ow_rows(peer(d), core)
        remote(got, got, ow_send.at[0, d - 1], ow_recv.at[0, d - 1], (sp, peer(n_tp - d))).wait_recv()
        copy = remote(got, got, ow_send.at[1, d - 1], ow_recv.at[1, d - 1], (sib_sp, tp))
        copy.start()
        ow_on.append(copy)
    for d in range(1, n_tp):
        got = ow_rows(peer(d), 1 - core)
        remote(got, got, ow_send.at[1, d - 1], ow_recv.at[1, d - 1], (sib_sp, tp)).wait_recv()
        heads_out[d - 1].wait_recv()

    part_base = tp * part

    def nrm_rows(t, i):
        return nrm.at[pl.ds(mult(HALO + t * part + i * WINDOW, HALO), WINDOW), :]

    def nrm_copy(i, d):
        at = nrm_rows(tp, i)
        return remote(at, at, nrm_send.at[0], nrm_recv.at[i, d - 1], (sp, peer(n_tp - d)))

    def project(i):
        at = pl.ds(mult(i * WINDOW, WINDOW), WINDOW)
        mine = att[pl.ds(mult(part_base + i * WINDOW, WINDOW), WINDOW), :]
        proj = jnp.dot(mine, ow[tp], preferred_element_type=jnp.float32)
        for d in range(1, n_tp):
            proj = proj + jnp.dot(
                heads[d - 1, at, :], ow[peer(d)], preferred_element_type=jnp.float32
            )
        rounded = (mid[at, :].astype(jnp.float32) + proj).astype(jnp.bfloat16)
        mid[at, :] = rounded
        wide = rounded.astype(jnp.float32)
        scale = lax.rsqrt(jnp.mean(wide * wide, axis=1, keepdims=True) + 1e-06)
        normed = (wide * scale * gain_v[...]).astype(jnp.bfloat16)
        nrm[pl.ds(mult(HALO + part_base + i * WINDOW, HALO), WINDOW), :] = normed

    @pl.loop(0, part_blocks)
    def _(k):
        i = part_blocks - 1 - k
        project(i)
        for d in range(1, n_tp):

            @pl.when(k > 0)
            def _():
                nrm_copy(i + 1, d).start()

        @pl.when(before_proj + k < events)
        def _():
            service(0, before_proj + k)

    for d in range(1, n_tp):
        nrm_copy(0, d).start()

    after_proj = min(events, before_proj + part_blocks)
    serve(0, after_proj, events)
    early_value = due(14)

    def nrm_wait(i):
        for d in range(1, n_tp):
            got = nrm_rows(peer(d), i)
            remote(
                got, got, nrm_send.at[0], nrm_recv.at[i, d - 1], (sp, peer(n_tp - d))
            ).wait_recv()

    nrm_wait(part_blocks - 1)
    nrm_halo = remote(
        nrm.at[pl.ds(HALO + rows - REACH, REACH), :],
        nrm.at[pl.ds(HALO - REACH, REACH), :],
        halo_send.at[3],
        halo_recv.at[3],
        (next_sp, tp),
    )
    nrm_halo.start()
    serve(1, 0, early_value)
    pl.loop(0, part_blocks - 1)(nrm_wait)

    sib_wait(0, 0)
    for copy in halos + heads_out + ow_out + ow_on + [nrm_halo]:
        copy.wait_send()

    sent_rows = nrm.at[pl.ds(0, (n_tp - 1) * part), :]
    remote(sent_rows, sent_rows, nrm_send.at[0], nrm_recv.at[0, 0], (sp, peer(1))).wait_send()

    nrm_halo.wait_recv()

    def up_tile(w_ref, taps, n, base, lengths):
        cols = pl.ds(mult(n * TILE, TILE), TILE)
        at = 0
        for length in lengths:
            lhs = nrm[pl.ds(mult(base + at, HALO), length), :]
            pre[at : at + length, :] = (
                jnp.dot(lhs, w_ref[:, cols], preferred_element_type=jnp.float32)
                .astype(jnp.bfloat16)
                .astype(jnp.float32)
            )
            at += length
        tap = taps[:, cols]
        for b in range((at - HALO) // WINDOW):
            at = HALO + b * WINDOW
            to = pl.ds(mult(base + b * WINDOW, WINDOW), WINDOW)
            one = jnp.concatenate([same_one[to, :]] * (TILE // WINDOW), axis=1)
            two = jnp.concatenate([same_two[to, :]] * (TILE // WINDOW), axis=1)
            conv = tap[2:3] * pre[at : at + WINDOW, :]
            conv = conv + one * (tap[1:2] * pre[at - 1 : at - 1 + WINDOW, :])
            conv = conv + two * (tap[0:1] * pre[at - 2 : at - 2 + WINDOW, :])
            yield to, cols, conv

    def spread(w, first, count, i):
        before = lax.div(i * count, unit_tiles)
        after = lax.div((i + 1) * count, unit_tiles)

        @pl.when(after > before)
        def _():
            service(w, first + before)

    gate_count = min(unit_tiles, events - early_value)

    @pl.loop(0, unit_tiles)
    def _(n):
        lengths = (HALO + rows // 2, rows // 2)
        for to, cols, conv in up_tile(wg, cg_v, n, 0, lengths):
            hid[to, cols] = (conv / (1.0 + jnp.exp(-conv))).astype(jnp.bfloat16)
        spread(1, early_value, gate_count, n)

    serve(1, early_value + gate_count, events)
    sib_wait(1, 0)

    def value_part(t, first, count):
        @pl.loop(0, unit_tiles)
        def _(n):
            for to, cols, conv in up_tile(wv, cv_v, n, t * part, (HALO + part,)):
                hid[to, cols] = (hid[to, cols].astype(jnp.float32) * conv).astype(
                    jnp.bfloat16
                )
            spread(2, first, count, n)

    def sum_copy(h, d, strip=None):
        src, dst, sem = send.at[h, d - 1], came.at[h, d - 1], h
        if strip is not None:
            at, lanes = last_strips[strip]
            src, dst, sem = src.at[at, lanes], dst.at[at, lanes], h + strip
        return remote(src, dst, sum_send.at[0], sum_recv.at[sem, d - 1], (sp, peer(d)))

    low_cols, high_cols = slice(0, depth), slice(depth, 2 * depth)
    last_strips = [
        (slice(0, part), low_cols),
        (slice(0, part // 2), high_cols),
        (slice(part // 2, part), high_cols),
    ]

    def hop_cols(h, c):
        j = held(h) if c == 0 else sib_held(h)
        return pl.ds(mult(j * depth, depth), depth)

    def add_up(h, c, parts):
        cols = hop_cols(h, c)
        total = own[h, :, c * depth : (c + 1) * depth] + mid[:, cols].astype(jnp.float32)
        for t in parts:
            total = total + t.astype(jnp.float32)
        mid[:, cols] = total.astype(jnp.bfloat16)

    def finish_hop(h):
        for d in range(1, n_tp):
            sum_copy(h, d).wait_recv()
        for c in range(2):
            lanes = slice(c * depth, (c + 1) * depth)
            add_up(h, c, [came[h, d - 1, :, lanes] for d in range(1, n_tp)])

    def finish_last():
        h = chips - 1
        for strip in range(3):
            for d in range(1, n_tp):
                sum_copy(h, d, strip).wait_recv()
        for c in range(2):
            lo = c * (depth // 2)
            pairs = [
                [came[h, d - 1, :, at + lo : at + lo + depth // 2] for at in (0, depth)]
                for d in range(1, n_tp)
            ]
            add_up(h, c, [jnp.concatenate(pair, axis=1) for pair in pairs])

    def apart(step):
        pl.when(sp >= 0)(step)

    def down_rows(rhs, t, at=0, length=part):
        lhs = hid[pl.ds(mult(t * part + at, length), length), :]
        return lax.dot_general(
            lhs, rhs, (((1,), (1,)), ((), ())), preferred_element_type=jnp.float32
        )

    def hop_rows(h):
        return jnp.concatenate(
            [wd[pl.ds(mult(j * depth, depth), depth), :] for j in (held(h), sib_held(h))], axis=0
        )

    def down_far(h):
        sib_wait(2, h)
        for d in range(1, n_tp):

            @apart
            def _():
                send[h, d - 1] = down_rows(hop_rows(h), peer(d)).astype(jnp.bfloat16)

    def down_own(h):
        @apart
        def _():
            own[h] = down_rows(hop_rows(h), tp)

    def down_far_strip(strip):
        h = chips - 1
        at, lanes = last_strips[strip]
        half = min(strip, 1)

        def rhs():
            return jnp.concatenate(
                [last_half(j, half)[...] for j in (held(h), sib_held(h))], axis=0
            )

        for d in range(1, n_tp):

            @apart
            def _():
                send[h, d - 1, at, lanes] = down_rows(
                    rhs(), peer(d), at.start, at.stop - at.start
                ).astype(jnp.bfloat16)

    def send_sums(h, strip=None):
        for d in range(1, n_tp):
            sum_copy(h, d, strip).start()

    served = due(5)
    for d in range(1, n_tp):
        value_part(peer(d), 0, served if d == 1 else 0)

    @pl.loop(0, EARLY)
    def _(h):
        down_far(h)
        for i in range(due(1)):
            service(2, served + h * due(1) + i)
        send_sums(h)

    served += EARLY * due(1)
    more = due(6)
    value_part(tp, served, more)
    served += more

    @pl.loop(EARLY, chips - 1)
    def _(h):
        for s in range(SUB):

            @pl.when((h - 1) * SUB + s >= served)
            def _():
                service(2, (h - 1) * SUB + s)

        down_far(h)

        @pl.when(h > EARLY)
        def _():
            finish_hop(h - EARLY - 1)

        for w in range(2):

            @pl.when(h == EARLY + w)
            def _():
                sent_weights(w)

        send_sums(h)
        down_own(h - EARLY)

    last = chips - 1

    def serve_last(half):
        for s in range(SUB // 2):
            service(2, (last - 1) * SUB + half * (SUB // 2) + s)
        sib_wait(2, last, half)

    def finish_range(first, stop):
        for h in range(first, stop):
            finish_hop(h)

    serve_last(0)
    down_far_strip(0)
    finish_range(last - EARLY - 1, last - EARLY)
    send_sums(last, 0)
    pl.loop(last - EARLY, last)(down_own)
    serve_last(1)
    down_far_strip(1)
    finish_range(last - EARLY, last - 1)
    send_sums(last, 1)
    down_far_strip(2)
    finish_range(last - 1, last)
    send_sums(last, 2)
    down_own(last)
    finish_last()

    sent_weights(2)

    remote(send, send, sum_send.at[0], sum_recv.at[0, 0], (sp, peer(1))).wait_send()


def whole_layer(n_sp, n_tp, queries, keys, values, doc_ids, sinks, residual, out_weight,
                norm_gain, w_gate, w_value, conv_gate, conv_value, w_down):
    rows, q_width = queries.shape
    kv_width = keys.shape[1]
    part, width = residual.shape
    depth, units = w_gate.shape
    chips = n_sp // 2
    bf16, f32 = jnp.bfloat16, jnp.float32
    dma = pltpu.SemaphoreType.DMA
    part_blocks = part // WINDOW
    scratch = [
        pltpu.VMEM((width, units), bf16),
        pltpu.VMEM((width, units), bf16),
        pltpu.VMEM((width, units), bf16),
        pltpu.VMEM((HALO + rows, width), bf16),
        pltpu.VMEM((rows, units), bf16),
        pltpu.VMEM((HALO + rows, TILE), f32),
        pltpu.VMEM((rows, q_width), bf16),
        pltpu.VMEM((WINDOW + rows, kv_width), bf16),
        pltpu.VMEM((WINDOW + rows, kv_width), bf16),
        pltpu.VMEM((8 + rows // WINDOW, WINDOW), jnp.int32),
        pltpu.VMEM((8 + rows, WINDOW), jnp.int32),
        pltpu.VMEM((rows, WINDOW), f32),
        pltpu.VMEM((rows, WINDOW), f32),
        pltpu.VMEM((rows, q_width), bf16),
        pltpu.VMEM((n_tp - 1, part, q_width), bf16),
        pltpu.VMEM((n_tp, q_width, width), bf16),
        pltpu.SMEM((q_width // HEAD_DIM,), f32),
        pltpu.VMEM((1, width), f32),
        pltpu.VMEM((3, units), f32),
        pltpu.VMEM((3, units), f32),
        pltpu.VMEM((chips, n_tp - 1, part, 2 * depth), bf16),
        pltpu.VMEM((chips, n_tp - 1, part, 2 * depth), bf16),
        pltpu.VMEM((chips, part, 2 * depth), f32),
        dma((11 + SUB - (-units // rows),)),
        dma((3,)),
        dma((3, chips - 1, SUB)),
        dma((3,)),
        dma((chips + 3,)),
        dma((4,)),
        dma((4,)),
        dma((2, n_tp - 1)),
        dma((2, n_tp - 1)),
        dma((n_tp - 1,)),
        dma((n_tp - 1,)),
        dma((1,)),
        dma((part_blocks, n_tp - 1)),
        dma((1,)),
        dma((chips + 2, n_tp - 1)),
    ]
    any_spec = pl.BlockSpec(memory_space=pl.ANY)
    return pl.pallas_call(
        functools.partial(layer_kernel, n_sp, n_tp),
        out_shape=pltpu.VMEM(residual.shape, residual.dtype),
        in_specs=[any_spec] * 13,
        out_specs=pl.BlockSpec(memory_space=pltpu.VMEM),
        scratch_shapes=scratch,
        compiler_params=pltpu.CompilerParams(
            collective_id=0, has_side_effects=True, vmem_limit_bytes=VMEM_BYTES - 2 * residual.size
        ),
    )(
        queries,
        keys,
        values,
        doc_ids.reshape(rows // WINDOW, WINDOW),
        sinks,
        residual,
        out_weight,
        norm_gain.reshape(1, width),
        w_gate,
        w_value,
        conv_gate,
        conv_value,
        w_down,
    )


def in_one_kernel(n_sp, n_tp, queries, keys, values, doc_ids, *weights):
    w_gate = weights[4]
    depth, units = w_gate.shape
    aligned = depth % 128 == 0 and keys.shape[1] % 128 == 0 and units % TILE == 0
    return aligned and n_sp % 4 == 0 and n_tp > 1 and doc_ids.shape[0] % (n_tp * WINDOW) == 0


def solution(mesh):
    n_sp, n_tp = mesh.shape["sp"], mesh.shape["tp"]

    def body(*args):
        if in_one_kernel(n_sp, n_tp, *args):
            return whole_layer(n_sp, n_tp, *args)
        return per_device(*args)

    return jax.shard_map(
        body,
        mesh=mesh,
        in_specs=(
            P("sp", "tp"),
            P("sp", "tp"),
            P("sp", "tp"),
            P("sp"),
            P("tp"),
            P(("sp", "tp"), None),
            P("tp", None),
            P(),
            P("sp", "tp"),
            P("sp", "tp"),
            P(None, "tp"),
            P(None, "tp"),
            P("tp", "sp"),
        ),
        out_specs=P(("sp", "tp"), None),
        check_vma=False,
    )
```
